256 devices in a mesh: st: 64 (over z, y, core), tp: 4 (over x).
Axes of the slice: x: 4, y: 4, z: 8, core: 2. Of those that a mesh axis runs over, the one named last changes fastest.
Arguments:
- queries: bfloat16 [65536, 1024], P('st', 'tp'), may hold values from -540 to 540
- gate_pre: bfloat16 [65536, 1024], P('st', 'tp'), may hold values from -6 to 6
- cotangent: bfloat16 [65536, 1024], P('st', 'tp'), may hold values from -6 to 6
- store: bfloat16 [81920, 2048], P('st'), may hold values from -6 to 6
- store_gain: float32 [2048], replicated, may hold values from 0.1 to 1.9
- w_key: bfloat16 [2048, 1024], P(None, 'tp'), may hold values from -0.125 to 0.125
- w_value: bfloat16 [2048, 1024], P(None, 'tp'), may hold values from -0.125 to 0.125
- owners: int32 [512, 4], P('st'), may hold values from 0 to 63, all different within a row; in each aligned block of 8 rows (0 to 7, 8 to 15, ...) at most 1 rows name the same one
- slots: int32 [512, 4], P('st'), may hold values from 0 to 19
Outputs:
- grad_queries: float32 [65536, 1024], P('st', 'tp')
- grad_store: float32 [81920, 2048], P(('st', 'tp'))
- grad_w_value: float32 [2048, 1024], P('st', 'tp')
The draws below stay inside these ranges and needn't reach their ends.
Inputs may be any that keep to these rules, and one draw needn't show every extreme that they name: Each block names 4 different owners. Among the blocks of one device no owner is named twice.
All inputs are finite; a program needn't handle non-finite values.
Results may differ from the reference program's by a relative error of at most 0.014.
Values may be sent and summed in bfloat16 or wider, within the bound.
No kernel may reach another device: no remote copies, remote signals or barrier semaphores. Data moves between devices by JAX's collectives and lax.ppermute only.
A program may use at most 192 MiB of HBM per device.

```python
import math
import jax
import jax.numpy as jnp
import numpy as np
from jax import lax

D = 2048
HEADS = 8
HD = 128
PLEN = 64
BLK = 128
NPB = 4
PASS_DEV = 20
XW = 1024
BLK_DEV = 8
CAP = 1
TOKENS = 65536
BLOCKS = 512
PASSAGES = 1280
ROWS = 81920
N_ST = 64


def draw_queries(key, part):
    first_key = jax.random.fold_in(key, 11)
    drawn = jnp.clip(jax.random.normal(first_key, (TOKENS, XW), jnp.float32), -6.0, 6.0)
    return drawn.astype(jnp.bfloat16)


def draw_cotangent(key, part):
    first_key = jax.random.fold_in(key, 13)
    drawn = jnp.clip(jax.random.normal(first_key, (TOKENS, XW), jnp.float32), -6.0, 6.0)
    return drawn.astype(jnp.bfloat16)


def set_ends(array, stream_key, least, high):
    place = [jax.random.randint(jax.random.fold_in(stream_key, axis), (), 0, length) for axis, length in enumerate(array.shape)]
    widest = array.shape.index(max(array.shape))
    neighbour = place[:widest] + [(place[widest] + 1) % array.shape[widest]] + place[widest + 1:]
    return array.at[tuple(place)].set(least).at[tuple(neighbour)].set(high)


def shard_levels(key, extent, shards, low, largest):
    gain = 1.0
    for position, shards_of in shards:
        heights = jax.random.uniform(jax.random.fold_in(jax.random.fold_in(key, 6), position), (shards_of,), jnp.float32, low / len(shards), largest / len(shards))
        gain = gain * jnp.repeat(jnp.exp(heights), extent[position] // shards_of).reshape((-1,) + (1,) * (len(extent) - 1 - position))
    return gain


def rank_bounds(number_of, skew):
    portions = [(1 << 20) // math.isqrt(grade ** skew) + 1 for grade in range(1, number_of + 1)]
    width = 1 + sum(portions) // (1 << 30)
    return np.cumsum(np.array([max(1, weight // width) for weight in portions]))


def ranked_ids(rng, dims, count, skew):
    table = rank_bounds(count, skew)
    lot = jax.random.randint(jax.random.fold_in(rng, 1), dims, 0, int(table[count - 1]))
    standing = jnp.searchsorted(jnp.asarray(table, jnp.int32), lot, side="right")
    return jax.random.permutation(jax.random.fold_in(rng, 2), count)[standing].astype(jnp.int32)


def routed_block(own_key, own, number, rows, count, top, bound, lean):
    sequence = jax.random.permutation(own_key, count)
    heavy_load, common = portions_of(count, rows * top, bound, lean, True), portions_of(count, rows * top, bound, lean, False)
    places = jnp.arange(count)

    def named(lengths, rotation):
        used = int((lengths > 0).sum())
        fixed = max(1, used // 4)
        moved = fixed + (places - fixed + rotation * (used - fixed)) % max(1, count - fixed)
        return jnp.zeros((count,), jnp.int32).at[sequence[jnp.where(places < fixed, places, moved)]].set(jnp.asarray(lengths, jnp.int32))

    lengths = jnp.where(number % 4 == 0, named(heavy_load, number // 4), named(common, number - number // 4 - 1))
    mixed = jax.random.permutation(jax.random.fold_in(own, 3), count)
    giver, sink = mixed[0:count // 2 * 2:2], mixed[1:count // 2 * 2:2]
    room = jnp.minimum(lengths[giver] - 1, bound - lengths[sink]) // 2
    room = jnp.where((giver == sequence[0]) | (sink == sequence[0]) | (lengths[sink] == 0), 0, jnp.maximum(room, 0))
    moved = jax.random.randint(jax.random.fold_in(own, 4), (count // 2,), 0, 1 << 20) % (room + 1)
    lengths = lengths.at[giver].add(-moved).at[sink].add(moved)
    labels = jnp.searchsorted(jnp.cumsum(lengths), jnp.arange(rows * top), side="right").astype(jnp.int32)
    listing = labels.reshape(top, rows).T
    listing = listing[jax.random.permutation(jax.random.fold_in(own, 1), rows)]
    rotation = jax.random.randint(jax.random.fold_in(own, 2), (rows, 1), 0, top)
    return jnp.take_along_axis(listing, (jnp.arange(top)[None, :] + rotation) % top, axis=1)


def portions_of(amount, total, bound, slope, full):
    weights = [(1 << 20) // math.isqrt(rank ** slope) + 1 for rank in range(1, amount + 1)]
    largest = bound if full else min(bound, max(-(-total // amount), total * weights[0] // sum(weights)))
    least = 1 if total - largest >= amount - 1 else 0
    counts, surplus = [largest] + [least] * (amount - 1), total - largest - least * (amount - 1)
    while surplus > 0:
        movable = [i for i in range(1, amount) if counts[i] < largest] or [i for i in range(1, amount) if counts[i] < bound]
        whole, budget = sum([weights[i] for i in movable]), surplus
        for i in movable:
            addition = min(bound - counts[i], max(1, budget * weights[i] // whole), surplus)
            counts[i] = counts[i] + addition
            surplus = surplus - addition
    return np.array(counts)


def normal_values(own_key, dims, scale, bound, split=(), kind=jnp.bfloat16):
    factor_of = shard_levels(own_key, dims, split, -0.22, 0.18) if split else 1.0
    values = jax.random.normal(own_key, dims, jnp.float32) * scale * factor_of
    return jnp.minimum(jnp.maximum(values, -bound), bound).astype(kind)


def setup_inputs(seed: int = 0) -> dict:
    key_of = jax.random.split(jax.random.key(seed), 10)
    queries = draw_queries(jax.random.fold_in(key_of[9], 71), 0)
    gate_pre = normal_values(key_of[1], (TOKENS, XW), 1.5, 6.0, ((0, 64), (1, 4)))
    cotangent = draw_cotangent(jax.random.fold_in(key_of[9], 71), 0)
    store = normal_values(key_of[3], (ROWS, D), 1.0, 6.0, ((0, 64),))
    store_gain = jnp.clip(1.0 + 0.18 * jax.random.normal(key_of[4], (D,), jnp.float32), 0.1, 1.9)
    w_key = normal_values(key_of[5], (D, XW), D ** -0.5, 0.125, ((1, 4),))
    w_value = normal_values(key_of[6], (D, XW), D ** -0.5, 0.125, ((1, 4),))
    owners_keys = jax.random.split(jax.random.fold_in(key_of[7], 1), BLOCKS // BLK_DEV)
    owners_turns = jax.random.permutation(jax.random.fold_in(key_of[7], 3), BLOCKS // BLK_DEV)
    owners = jax.vmap(lambda own, number: routed_block(jax.random.fold_in(key_of[7], 2), own, number, BLK_DEV, N_ST, NPB, CAP, 2))(owners_keys, owners_turns).reshape((BLOCKS, NPB))
    slots = set_ends(ranked_ids(key_of[8], (BLOCKS, NPB), PASS_DEV, 2), jax.random.fold_in(key_of[8], 3), 0, PASS_DEV - 1).astype(jnp.int32)
    return {"queries": queries, "gate_pre": gate_pre, "cotangent": cotangent, "store": store, "store_gain": store_gain, "w_key": w_key, "w_value": w_value, "owners": owners, "slots": slots}


EPS = 1e-06

def reference(queries, gate_pre, cotangent, store, store_gain, w_key, w_value, owners, slots):
    store_rows = store.astype(jnp.float32)
    row_inverse = lax.rsqrt(lax.optimization_barrier(jnp.mean(store_rows * store_rows, axis=-1, keepdims=True)) + EPS)
    normed = (store_rows * row_inverse * store_gain).astype(jnp.bfloat16)
    key_table = jnp.dot(normed, w_key, preferred_element_type=jnp.float32).astype(jnp.bfloat16).reshape(PASSAGES, PLEN, XW)
    value_table = jnp.dot(normed, w_value, preferred_element_type=jnp.float32).astype(jnp.bfloat16).reshape(PASSAGES, PLEN, XW)
    passage_ids = (owners * PASS_DEV + slots).astype(jnp.int32)
    score_scale = HD ** (-0.5)

    def one_group(group):
        query_part, gate_part, cot_part, id_part = group
        flat_ids = id_part.reshape(-1).astype(jnp.int32)
        group_keys = key_table[flat_ids].reshape(BLK_DEV, NPB * PLEN, HEADS, HD).astype(jnp.float32)
        group_values = value_table[flat_ids].reshape(BLK_DEV, NPB * PLEN, HEADS, HD).astype(jnp.float32)
        query_wide = query_part.astype(jnp.float32)
        scores = jnp.einsum('bqhd,bkhd->bhqk', query_wide, group_keys) * score_scale
        shifted = scores - lax.optimization_barrier(jnp.max(scores, axis=-1, keepdims=True))
        weights = jnp.exp(shifted)
        weights = weights / lax.optimization_barrier(jnp.sum(weights, axis=-1, keepdims=True))
        weights_half = lax.optimization_barrier(weights.astype(jnp.bfloat16)).astype(jnp.float32)
        grad_in = jax.nn.sigmoid(gate_part.astype(jnp.float32)) * cot_part.astype(jnp.float32)
        grad_in = lax.optimization_barrier(grad_in.astype(jnp.bfloat16)).astype(jnp.float32)
        attended = jnp.einsum('bhqk,bkhd->bqhd', weights_half, group_values)
        row_delta = lax.optimization_barrier(jnp.sum(grad_in * attended, axis=-1))
        grad_weights = jnp.einsum('bqhd,bkhd->bhqk', grad_in, group_values)
        grad_scores = weights * (grad_weights - jnp.transpose(row_delta, (0, 2, 1))[..., None])
        grad_half = lax.optimization_barrier(grad_scores.astype(jnp.bfloat16)).astype(jnp.float32)
        grad_query = jnp.einsum('bhqk,bkhd->bqhd', grad_half, group_keys) * score_scale
        grad_key = jnp.einsum('bhqk,bqhd->bkhd', grad_half, query_wide) * score_scale
        grad_value = jnp.einsum('bhqk,bqhd->bkhd', weights_half, grad_in)
        return (grad_query.reshape(BLK_DEV * BLK, XW), grad_key.reshape(BLK_DEV * NPB, PLEN, XW), grad_value.reshape(BLK_DEV * NPB, PLEN, XW))
    groups = (queries.reshape(N_ST, BLK_DEV, BLK, HEADS, HD), gate_pre.reshape(N_ST, BLK_DEV, BLK, HEADS, HD), cotangent.reshape(N_ST, BLK_DEV, BLK, HEADS, HD), passage_ids.reshape(N_ST, BLK_DEV, NPB))
    grad_queries, slot_keys, slot_values = lax.map(one_group, groups)
    grad_queries = grad_queries.reshape(TOKENS, XW)
    every_id = passage_ids.reshape(-1)
    passage_keys = jnp.zeros((PASSAGES, PLEN, XW), jnp.float32).at[every_id].add(slot_keys.reshape(BLOCKS * NPB, PLEN, XW))
    passage_values = jnp.zeros((PASSAGES, PLEN, XW), jnp.float32).at[every_id].add(slot_values.reshape(BLOCKS * NPB, PLEN, XW))
    passage_keys = passage_keys.astype(jnp.bfloat16).reshape(ROWS, XW)
    passage_values = passage_values.astype(jnp.bfloat16).reshape(ROWS, XW)
    grad_normed = jnp.dot(passage_keys, w_key.T, preferred_element_type=jnp.float32) + jnp.dot(passage_values, w_value.T, preferred_element_type=jnp.float32)
    grad_w_value = jnp.dot(normed.T, passage_values, preferred_element_type=jnp.float32)
    unit_rows = store_rows * row_inverse
    grad_unit = grad_normed * store_gain
    grad_store = row_inverse * (grad_unit - unit_rows * lax.optimization_barrier(jnp.mean(grad_unit * unit_rows, axis=-1, keepdims=True)))
    return (grad_queries, grad_store, grad_w_value)
```

```python
import jax
import jax.numpy as jnp
from jax import lax
from jax.experimental import pallas as pl
from jax.experimental.pallas import tpu as pltpu
from jax.sharding import Mesh
from jax.sharding import PartitionSpec as P

HD = 128
PLEN = 64
EPS = 1e-06
ST = ("st_0", "st_1", "st_2")
CHIPS = ("st_0", "st_1")
ST_TP = ("st_0", "st_1", "st_2", "tp")
VMEM_LIMIT = 48 * 1024 * 1024


def params(grid_dims=1):
    return pltpu.CompilerParams(
        dimension_semantics=("arbitrary",) * grid_dims, vmem_limit_bytes=VMEM_LIMIT
    )


def dot_nn(a, b):
    return lax.dot_general(a, b, (((1,), (0,)), ((), ())), preferred_element_type=jnp.float32)


def dot_nt(a, b):
    return lax.dot_general(a, b, (((1,), (1,)), ((), ())), preferred_element_type=jnp.float32)


def dot_tn(a, b):
    return lax.dot_general(a, b, (((0,), (0,)), ((), ())), preferred_element_type=jnp.float32)


def normed_rows(x, gain):
    inverse = lax.rsqrt(jnp.mean(x * x, axis=-1, keepdims=True) + EPS)
    return (x * inverse * gain).astype(jnp.bfloat16)


def tables_kernel(store_ref, gain_ref, wk_ref, wv_ref, table_ref):
    width = wk_ref.shape[1]
    normed = normed_rows(store_ref[...].astype(jnp.float32), gain_ref[...])
    table_ref[:, :width] = dot_nn(normed, wk_ref[...]).astype(jnp.bfloat16)
    table_ref[:, width:] = dot_nn(normed, wv_ref[...]).astype(jnp.bfloat16)


def key_value_tables(store, gain, w_key, w_value):
    rows, model = store.shape
    width = w_key.shape[1]
    step = 256
    return pl.pallas_call(
        tables_kernel,
        grid=(rows // step,),
        in_specs=[
            pl.BlockSpec((step, model), lambda i: (i, 0)),
            pl.BlockSpec((1, model), lambda i: (0, 0)),
            pl.BlockSpec((model, width), lambda i: (0, 0)),
            pl.BlockSpec((model, width), lambda i: (0, 0)),
        ],
        out_specs=pl.BlockSpec((step, 2 * width), lambda i: (i, 0)),
        out_shape=jax.ShapeDtypeStruct((rows, 2 * width), jnp.bfloat16),
        compiler_params=params(),
        cost_estimate=pl.CostEstimate(
            flops=4 * rows * model * width, bytes_accessed=2 * rows * model, transcendentals=rows
        ),
        name="tables",
    )(store, gain, w_key, w_value)


def turned_kernel(store_ref, gain_ref, out_ref):
    normed = normed_rows(store_ref[...].astype(jnp.float32), gain_ref[...])
    out_ref[...] = normed.T


def turned_normed(store, gain):
    rows, model = store.shape
    step = 256
    return pl.pallas_call(
        turned_kernel,
        grid=(rows // step,),
        in_specs=[
            pl.BlockSpec((step, model), lambda i: (i, 0)),
            pl.BlockSpec((1, model), lambda i: (0, 0)),
        ],
        out_specs=pl.BlockSpec((model, step), lambda i: (0, i)),
        out_shape=jax.ShapeDtypeStruct((model, rows), jnp.bfloat16),
        compiler_params=params(),
        cost_estimate=pl.CostEstimate(
            flops=16 * rows * model, bytes_accessed=4 * rows * model, transcendentals=rows
        ),
        name="turned_normed",
    )(store, gain)


def gather_kernel(asked_ref, table_ref, out_ref):
    base = pl.program_id(0) * out_ref.shape[0]
    for i in range(out_ref.shape[0]):
        out_ref[i] = table_ref[jnp.maximum(asked_ref[base + i], 0)]


def picked_passages(asked, table):
    passages, length, width = table.shape
    slots = asked.shape[0]
    step = 16
    return pl.pallas_call(
        gather_kernel,
        grid_spec=pltpu.PrefetchScalarGridSpec(
            num_scalar_prefetch=1,
            grid=(slots // step,),
            in_specs=[pl.BlockSpec((passages, length, width), lambda i, a: (0, 0, 0))],
            out_specs=pl.BlockSpec((step, length, width), lambda i, a: (i, 0, 0)),
        ),
        out_shape=jax.ShapeDtypeStruct((slots, length, width), jnp.bfloat16),
        compiler_params=params(),
        name="picked",
    )(asked, table)


def attention_kernel(owner_ref, q_ref, g_ref, c_ref, got_ref, gq_ref, out_ref):
    block = pl.program_id(0)
    width = q_ref.shape[1]
    per_block = owner_ref.shape[0] // pl.num_programs(0)
    scale = HD ** (-0.5)
    owners = [owner_ref[block * per_block + j] for j in range(per_block)]
    gate = jax.nn.sigmoid(g_ref[...].astype(jnp.float32))
    grad_in = (gate * c_ref[...].astype(jnp.float32)).astype(jnp.bfloat16)
    for h in range(width // HD):
        cols = slice(h * HD, (h + 1) * HD)
        vcols = slice(width + h * HD, width + (h + 1) * HD)
        q = q_ref[:, cols]
        gin = grad_in[:, cols]
        keys = jnp.concatenate([got_ref[o, :, cols] for o in owners], axis=0)
        values = jnp.concatenate([got_ref[o, :, vcols] for o in owners], axis=0)
        scores = dot_nt(q, keys) * scale
        weights = jnp.exp(scores - jnp.max(scores, axis=-1, keepdims=True))
        weights = weights / jnp.sum(weights, axis=-1, keepdims=True)
        half = weights.astype(jnp.bfloat16)
        grad_weights = dot_nt(gin, values)
        delta = jnp.sum(half.astype(jnp.float32) * grad_weights, axis=-1, keepdims=True)
        grad_half = (weights * (grad_weights - delta)).astype(jnp.bfloat16)
        gq_ref[:, cols] = dot_nn(grad_half, keys) * scale
        grad_keys = (dot_tn(grad_half, q) * scale).astype(jnp.bfloat16)
        grad_values = dot_tn(half, gin).astype(jnp.bfloat16)
        for j, o in enumerate(owners):
            rows = slice(j * PLEN, (j + 1) * PLEN)
            out_ref[o, :, cols] = grad_keys[rows]
            out_ref[o, :, vcols] = grad_values[rows]


def attention(owner_flat, queries, gate_pre, cotangent, got, blocks):
    rows, width = queries.shape
    length = rows // blocks
    tokens = pl.BlockSpec((length, width), lambda b, o: (b, 0))
    whole = pl.BlockSpec(got.shape, lambda b, o: (0, 0, 0))
    keys = PLEN * owner_flat.shape[0] // blocks
    return pl.pallas_call(
        attention_kernel,
        grid_spec=pltpu.PrefetchScalarGridSpec(
            num_scalar_prefetch=1,
            grid=(blocks,),
            in_specs=[tokens, tokens, tokens, whole],
            out_specs=[tokens, whole],
        ),
        out_shape=[
            jax.ShapeDtypeStruct((rows, width), jnp.float32),
            jax.ShapeDtypeStruct(got.shape, jnp.bfloat16),
        ],
        compiler_params=params(),
        cost_estimate=pl.CostEstimate(
            flops=10 * rows * width * keys,
            bytes_accessed=10 * rows * width + 4 * got.size,
            transcendentals=rows * width * keys // HD,
        ),
        name="attention",
    )(owner_flat, queries, gate_pre, cotangent, got)


def sums_kernel(asked_ref, place_ref, back_ref, own_ref, a_ref, b_ref, c_ref, values_ref, total):
    slots, length, both = back_ref.shape
    width = both // 2
    passages = total.shape[0]
    part = passages // 4
    total[...] = jnp.zeros_like(total)

    def add(r, carry):
        asked = asked_ref[r]

        @pl.when(asked >= 0)
        def _():
            total[asked] += back_ref[r].astype(jnp.float32)

        return carry

    lax.fori_loop(0, slots, add, 0)
    for p in range(passages):
        values_ref[p * length : (p + 1) * length, :] = total[p, :, width:].astype(jnp.bfloat16)
    for turn, out in enumerate((own_ref, a_ref, b_ref, c_ref)):
        first = lax.rem(place_ref[0] + turn, 4) * part
        for p in range(part):
            out[p * length : (p + 1) * length, :] = total[first + p].astype(jnp.bfloat16)


def passage_sums(asked, place, back, passages):
    slots, length, both = back.shape
    quarter = jax.ShapeDtypeStruct((passages * length // 4, both), jnp.bfloat16)
    return pl.pallas_call(
        sums_kernel,
        in_specs=[
            pl.BlockSpec(memory_space=pltpu.SMEM),
            pl.BlockSpec(memory_space=pltpu.SMEM),
            pl.BlockSpec(memory_space=pltpu.VMEM),
        ],
        out_specs=[pl.BlockSpec(memory_space=pltpu.VMEM)] * 5,
        out_shape=[
            quarter,
            quarter,
            quarter,
            quarter,
            jax.ShapeDtypeStruct((passages * length, both // 2), jnp.bfloat16),
        ],
        scratch_shapes=[pltpu.VMEM((passages, length, both), jnp.float32)],
        compiler_params=pltpu.CompilerParams(vmem_limit_bytes=VMEM_LIMIT),
        name="sums",
    )(asked, place, back)


def weight_kernel(turned_ref, values_ref, out_ref):
    terms = dot_nn(turned_ref[...], values_ref[...]).astype(jnp.bfloat16)
    cores, chips, share, _ = out_ref.shape
    for i in range(cores * chips):
        out_ref[i % cores, i // cores] = terms[i * share : (i + 1) * share]


def weight_terms(turned, values, chips, cores):
    model, rows = turned.shape
    width = values.shape[1]
    share = model // (chips * cores)
    steps = 4
    return pl.pallas_call(
        weight_kernel,
        grid=(steps,),
        in_specs=[
            pl.BlockSpec((model // steps, rows), lambda i: (i, 0)),
            pl.BlockSpec((rows, width), lambda i: (0, 0)),
        ],
        out_specs=pl.BlockSpec((cores, chips // steps, share, width), lambda i: (0, i, 0, 0)),
        out_shape=jax.ShapeDtypeStruct((cores, chips, share, width), jnp.bfloat16),
        compiler_params=params(),
        cost_estimate=pl.CostEstimate(
            flops=2 * model * rows * width, bytes_accessed=2 * model * rows, transcendentals=0
        ),
        name="weight_terms",
    )(turned, values)


def final_kernel(place_ref, store_ref, gain_ref, *refs):
    parts, weights, out_ref = refs[:4], refs[4:8], refs[8]
    grad_normed = dot_nt(parts[0][...], weights[0][...])
    for p, w in zip(parts[1:], weights[1:]):
        grad_normed += dot_nt(p[...], w[...])
    rows = store_ref[...].astype(jnp.float32)
    inverse = lax.rsqrt(jnp.mean(rows * rows, axis=-1, keepdims=True) + EPS)
    unit = rows * inverse
    grad_unit = grad_normed * gain_ref[...]
    mean = jnp.mean(grad_unit * unit, axis=-1, keepdims=True)
    out_ref[...] = inverse * (grad_unit - unit * mean)


def store_gradient(place, store, gain, parts, weights):
    quarter, both = parts[0].shape
    model = store.shape[1]
    steps = 4
    step = quarter // steps
    return pl.pallas_call(
        final_kernel,
        grid_spec=pltpu.PrefetchScalarGridSpec(
            num_scalar_prefetch=1,
            grid=(steps,),
            in_specs=[
                pl.BlockSpec((step, model), lambda i, t: (t[0] * steps + i, 0)),
                pl.BlockSpec((1, model), lambda i, t: (0, 0)),
            ]
            + [pl.BlockSpec((step, both), lambda i, t: (i, 0))] * 4
            + [pl.BlockSpec((model, both), lambda i, t: (0, 0))] * 4,
            out_specs=pl.BlockSpec((step, model), lambda i, t: (i, 0)),
        ),
        out_shape=jax.ShapeDtypeStruct((quarter, model), jnp.float32),
        compiler_params=params(),
        cost_estimate=pl.CostEstimate(
            flops=8 * quarter * model * both,
            bytes_accessed=8 * model * both + 6 * quarter * model,
            transcendentals=quarter,
        ),
        name="store_gradient",
    )(place, store, gain, *parts, *weights)


def shifted(value, turn):
    return lax.ppermute(value, "tp", [(i, (i + turn) % 4) for i in range(4)])


def local(queries, gate_pre, cotangent, store, store_gain, w_key, w_value, owners, slots):
    st_size = lax.axis_size(ST)
    chips = lax.axis_size(CHIPS)
    cores = lax.axis_size("st_2")
    blocks, per_block = owners.shape
    width = queries.shape[1]
    rows_dev, model = store.shape
    passages = rows_dev // PLEN
    place = lax.axis_index("tp").reshape(1).astype(jnp.int32)
    gain = store_gain.reshape(1, model)

    owner_flat = owners.reshape(blocks * per_block)
    slot_flat = slots.reshape(blocks * per_block)
    hits = owner_flat[:, None] == jnp.arange(st_size, dtype=jnp.int32)[None, :]
    requests = jnp.max(jnp.where(hits, slot_flat[:, None], -1), axis=0)
    asked = requests.reshape(chips, cores, 1)
    asked = lax.all_to_all(asked, "st_2", split_axis=1, concat_axis=1, tiled=True)
    asked = lax.all_to_all(asked, CHIPS, split_axis=0, concat_axis=0, tiled=True)
    asked = asked.reshape(st_size)

    table = key_value_tables(store, gain, w_key, w_value)
    picked = picked_passages(asked, table.reshape(passages, PLEN, 2 * width))
    got = lax.all_to_all(picked, ST, split_axis=0, concat_axis=0, tiled=True)

    both = jnp.concatenate([w_key, w_value], axis=1)
    weights = [both] + [shifted(both, turn) for turn in (1, 2, 3)]
    turned = turned_normed(store, gain)
    got, turned = lax.optimization_barrier((got, turned))

    grad_queries, outgoing = attention(owner_flat, queries, gate_pre, cotangent, got, blocks)
    back = lax.all_to_all(outgoing, ST, split_axis=0, concat_axis=0, tiled=True)

    own, first, second, third, values = passage_sums(asked, place, back, passages)
    parts = [own, shifted(first, 1), shifted(second, 2), shifted(third, 3)]

    terms = weight_terms(turned, values, chips, cores)
    terms = lax.all_to_all(terms, "st_2", split_axis=0, concat_axis=0, tiled=True)
    terms = jnp.sum(terms.astype(jnp.float32), axis=0).astype(jnp.bfloat16)
    terms = lax.all_to_all(terms, CHIPS, split_axis=0, concat_axis=0, tiled=True)
    grad_w_value = jnp.sum(terms.astype(jnp.float32), axis=0)

    grad_store = store_gradient(place, store, gain, parts, weights)
    return (grad_queries, grad_store, grad_w_value)


def solution(mesh):
    torus = Mesh(mesh.devices.reshape(8, 4, 2, mesh.shape["tp"]), ("st_0", "st_1", "st_2", "tp"))
    return jax.shard_map(
        local,
        mesh=torus,
        in_specs=(
            P(ST, "tp"),
            P(ST, "tp"),
            P(ST, "tp"),
            P(ST, None),
            P(),
            P(None, "tp"),
            P(None, "tp"),
            P(ST, None),
            P(ST, None),
        ),
        out_specs=(P(ST, "tp"), P(ST_TP, None), P(ST, "tp")),
        check_vma=False,
    )
```

```python
import jax
import jax.numpy as jnp
from jax import lax
from jax.experimental import pallas as pl
from jax.experimental.pallas import tpu as pltpu
from jax.sharding import Mesh
from jax.sharding import PartitionSpec as P

HD = 128
PLEN = 64
EPS = 1e-06
ST = ("st_0", "st_1", "st_2")
CHIPS = ("st_0", "st_1")
ST_TP = ("st_0", "st_1", "st_2", "tp")
MIB = 1024 * 1024


def params(mib):
    return pltpu.CompilerParams(
        dimension_semantics=("arbitrary",), vmem_limit_bytes=mib * MIB
    )


def in_hbm(value):
    return pltpu.with_memory_space_constraint(value, pltpu.HBM)


def dot_nn(a, b):
    return lax.dot_general(a, b, (((1,), (0,)), ((), ())), preferred_element_type=jnp.float32)


def dot_nt(a, b):
    return lax.dot_general(a, b, (((1,), (1,)), ((), ())), preferred_element_type=jnp.float32)


def dot_tn(a, b):
    return lax.dot_general(a, b, (((0,), (0,)), ((), ())), preferred_element_type=jnp.float32)


def normed_rows(x, gain):
    inverse = lax.rsqrt(jnp.mean(x * x, axis=-1, keepdims=True) + EPS)
    return (x * inverse * gain).astype(jnp.bfloat16)


def tables_kernel(store_ref, gain_ref, wk_hbm, wv_hbm, table_ref, wk_ref, wv_ref, sems):
    first = pl.program_id(0) == 0
    width = wk_ref.shape[1]
    keys_in = pltpu.make_async_copy(wk_hbm, wk_ref, sems.at[0])
    values_in = pltpu.make_async_copy(wv_hbm, wv_ref, sems.at[1])

    @pl.when(first)
    def _():
        keys_in.start()
        values_in.start()

    normed = normed_rows(store_ref[...].astype(jnp.float32), gain_ref[...])

    @pl.when(first)
    def _():
        keys_in.wait()
        values_in.wait()

    table_ref[:, :width] = dot_nn(normed, wk_ref[...]).astype(jnp.bfloat16)
    table_ref[:, width:] = dot_nn(normed, wv_ref[...]).astype(jnp.bfloat16)


def key_value_tables(store, gain, w_key, w_value):
    rows, model = store.shape
    width = w_key.shape[1]
    step = 256
    return pl.pallas_call(
        tables_kernel,
        grid=(rows // step,),
        in_specs=[
            pl.BlockSpec((step, model), lambda i: (i, 0)),
            pl.BlockSpec((1, model), lambda i: (0, 0)),
            pl.BlockSpec(memory_space=pltpu.HBM),
            pl.BlockSpec(memory_space=pltpu.HBM),
        ],
        out_specs=pl.BlockSpec((step, 2 * width), lambda i: (i, 0)),
        out_shape=jax.ShapeDtypeStruct((rows, 2 * width), jnp.bfloat16),
        scratch_shapes=[
            pltpu.VMEM((model, width), jnp.bfloat16),
            pltpu.VMEM((model, width), jnp.bfloat16),
            pltpu.SemaphoreType.DMA((2,)),
        ],
        compiler_params=params(16),
        cost_estimate=pl.CostEstimate(
            flops=4 * rows * model * width, bytes_accessed=2 * rows * model, transcendentals=rows
        ),
        name="tables",
    )(in_hbm(store), in_hbm(gain), in_hbm(w_key), in_hbm(w_value))


def turned_kernel(store_ref, gain_ref, out_ref):
    normed = normed_rows(store_ref[...].astype(jnp.float32), gain_ref[...])
    out_ref[...] = normed.T


def turned_normed(store, gain):
    rows, model = store.shape
    step = 256
    return pl.pallas_call(
        turned_kernel,
        grid=(rows // step,),
        in_specs=[
            pl.BlockSpec((step, model), lambda i: (i, 0)),
            pl.BlockSpec((1, model), lambda i: (0, 0)),
        ],
        out_specs=pl.BlockSpec((model, step), lambda i: (0, i)),
        out_shape=pltpu.HBM((model, rows), jnp.bfloat16),
        compiler_params=params(16),
        cost_estimate=pl.CostEstimate(
            flops=16 * rows * model, bytes_accessed=4 * rows * model, transcendentals=rows
        ),
        name="turned_normed",
    )(in_hbm(store), in_hbm(gain))


def gather_kernel(asked_ref, table_ref, out_hbm, sems):
    copies = []
    for i in range(out_hbm.shape[0]):
        asked = jnp.maximum(asked_ref[i], 0)
        copies.append(pltpu.make_async_copy(table_ref.at[asked], out_hbm.at[i], sems.at[i]))
        copies[-1].start()
    for copy in copies:
        copy.wait()


def picked_passages(asked, table):
    _, length, width = table.shape
    slots = asked.shape[0]
    return pl.pallas_call(
        gather_kernel,
        in_specs=[
            pl.BlockSpec(memory_space=pltpu.SMEM),
            pl.BlockSpec(memory_space=pltpu.VMEM),
        ],
        out_specs=pl.BlockSpec(memory_space=pltpu.HBM),
        out_shape=pltpu.HBM((slots, length, width), jnp.bfloat16),
        scratch_shapes=[pltpu.SemaphoreType.DMA((slots,))],
        compiler_params=pltpu.CompilerParams(vmem_limit_bytes=8 * MIB),
        name="picked",
    )(asked, table)


def attention_kernel(owner_ref, q_ref, g_ref, c_ref, *refs):
    pieces, (gq_ref, out_hbm, scratch, sems) = refs[:-4], refs[-4:]
    step, steps = pl.program_id(0), pl.num_programs(0)
    width = q_ref.shape[1]
    per_block = owner_ref.shape[0]
    each = len(pieces) // per_block
    length = q_ref.shape[0] // each
    scale = HD ** (-0.5)
    slot = lax.rem(step, 2)

    def copies(at, parity):
        return [
            pltpu.make_async_copy(
                scratch.at[parity, b * per_block + j],
                out_hbm.at[owner_ref[j, at * each + b]],
                sems.at[parity, b * per_block + j],
            )
            for b in range(each)
            for j in range(per_block)
        ]

    gate = jax.nn.sigmoid(g_ref[...].astype(jnp.float32))
    grad_in = (gate * c_ref[...].astype(jnp.float32)).astype(jnp.bfloat16)
    units = [(b, h) for b in range(each) for h in range(width // HD)]
    rows = [slice(b * length, (b + 1) * length) for b, _ in units]
    cols = [slice(h * HD, (h + 1) * HD) for _, h in units]
    vcols = [slice(width + h * HD, width + (h + 1) * HD) for _, h in units]
    own = [pieces[b * per_block : (b + 1) * per_block] for b, _ in units]
    count = range(len(units))
    q = [q_ref[rows[u], cols[u]] for u in count]
    gin = [grad_in[rows[u], cols[u]] for u in count]
    keys = [jnp.concatenate([p[0, :, cols[u]] for p in own[u]], axis=0) for u in count]
    values = [jnp.concatenate([p[0, :, vcols[u]] for p in own[u]], axis=0) for u in count]
    scores = [dot_nt(q[u], keys[u]) * scale for u in count]
    grad_weights = [dot_nt(gin[u], values[u]) for u in count]
    weights = [jnp.exp(x - jnp.max(x, axis=-1, keepdims=True)) for x in scores]
    weights = [x / jnp.sum(x, axis=-1, keepdims=True) for x in weights]
    half = [x.astype(jnp.bfloat16) for x in weights]
    delta = [
        jnp.sum(half[u].astype(jnp.float32) * grad_weights[u], axis=-1, keepdims=True)
        for u in count
    ]
    grad_half = [
        (weights[u] * (grad_weights[u] - delta[u])).astype(jnp.bfloat16) for u in count
    ]

    @pl.when(step >= 2)
    def _():
        for copy in copies(step - 2, slot):
            copy.wait()

    for u, (b, _) in enumerate(units):
        gq_ref[rows[u], cols[u]] = dot_nn(grad_half[u], keys[u]) * scale
        grad_keys = (dot_tn(grad_half[u], q[u]) * scale).astype(jnp.bfloat16)
        grad_values = dot_tn(half[u], gin[u]).astype(jnp.bfloat16)
        for j in range(per_block):
            part = slice(j * PLEN, (j + 1) * PLEN)
            scratch[slot, b * per_block + j, :, cols[u]] = grad_keys[part]
            scratch[slot, b * per_block + j, :, vcols[u]] = grad_values[part]

    for copy in copies(step, slot):
        copy.start()

    @pl.when(step == steps - 1)
    def _():
        for copy in copies(step - 1, 1 - slot):
            copy.wait()
        for copy in copies(step, slot):
            copy.wait()


def attention(owner_turned, queries, gate_pre, cotangent, got):
    rows, width = queries.shape
    per_block, blocks = owner_turned.shape
    each = 2
    steps = blocks // each
    tokens = pl.BlockSpec((rows // steps, width), lambda i, o: (i, 0))

    def piece(b, j):
        return pl.BlockSpec((1,) + got.shape[1:], lambda i, o: (o[j, i * each + b], 0, 0))

    pieces = [piece(b, j) for b in range(each) for j in range(per_block)]
    keys = PLEN * per_block
    return pl.pallas_call(
        attention_kernel,
        grid_spec=pltpu.PrefetchScalarGridSpec(
            num_scalar_prefetch=1,
            grid=(steps,),
            in_specs=[tokens, tokens, tokens] + pieces,
            out_specs=[tokens, pl.BlockSpec(memory_space=pltpu.HBM)],
            scratch_shapes=[
                pltpu.VMEM((2, len(pieces)) + got.shape[1:], jnp.bfloat16),
                pltpu.SemaphoreType.DMA((2, len(pieces))),
            ],
        ),
        out_shape=[
            jax.ShapeDtypeStruct((rows, width), jnp.float32),
            pltpu.HBM(got.shape, jnp.bfloat16),
        ],
        compiler_params=params(20),
        cost_estimate=pl.CostEstimate(
            flops=10 * rows * width * keys,
            bytes_accessed=10 * rows * width + 2 * got.size,
            transcendentals=rows * width * keys // HD,
        ),
        name="attention",
    )(
        owner_turned,
        in_hbm(queries),
        in_hbm(gate_pre),
        in_hbm(cotangent),
        *([in_hbm(got)] * len(pieces)),
    )


def sums_kernel(asked_ref, place_ref, back_ref, turned_hbm, *refs):
    parts, (mine_ref, other_ref, total, turned_ref, terms, sem) = refs[:4], refs[4:]
    step, steps = pl.program_id(0), pl.num_programs(0)
    each, length, both = back_ref.shape
    width = both // 2
    passages = total.shape[0]
    share = passages // 4
    turned_in = pltpu.make_async_copy(turned_hbm, turned_ref, sem)

    @pl.when(step == 0)
    def _():
        turned_in.start()
        total[...] = jnp.zeros_like(total)

    for i in range(each):
        asked = asked_ref[step * each + i]

        @pl.when(asked >= 0)
        def _():
            total[asked] += back_ref[i].astype(jnp.float32)

    @pl.when(step == steps - 1)
    def _():
        values = total[:, :, width:].astype(jnp.bfloat16).reshape(passages * length, width)
        for turn, out in enumerate(parts):
            first = lax.rem(place_ref[0] + turn, 4) * share
            for p in range(share):
                out[p * length : (p + 1) * length, :] = total[first + p].astype(jnp.bfloat16)
        turned_in.wait()
        pieces, piece, _ = terms.shape
        made = dot_nn(turned_ref[...], values).astype(jnp.bfloat16)
        for p in range(pieces):
            terms[p] = made[p * piece : (p + 1) * piece]
        for p in range(pieces // 2):
            mine_ref[p] = terms[2 * p + place_ref[1]]
            other_ref[p] = terms[2 * p + 1 - place_ref[1]]


def passage_sums(asked, place, back, turned, passages, devices):
    slots, length, both = back.shape
    model, rows = turned.shape
    each = 8
    quarter = jax.ShapeDtypeStruct((rows // 4, both), jnp.bfloat16)
    half = jax.ShapeDtypeStruct((devices // 2, model // devices, both // 2), jnp.bfloat16)
    return pl.pallas_call(
        sums_kernel,
        grid_spec=pltpu.PrefetchScalarGridSpec(
            num_scalar_prefetch=2,
            grid=(slots // each,),
            in_specs=[
                pl.BlockSpec((each, length, both), lambda i, a, t: (i, 0, 0)),
                pl.BlockSpec(memory_space=pltpu.HBM),
            ],
            out_specs=[pl.BlockSpec(quarter.shape, lambda i, a, t: (0, 0))] * 4
            + [pl.BlockSpec(half.shape, lambda i, a, t: (0, 0, 0))] * 2,
            scratch_shapes=[
                pltpu.VMEM((passages, length, both), jnp.float32),
                pltpu.VMEM((model, rows), jnp.bfloat16),
                pltpu.VMEM((devices, model // devices, both // 2), jnp.bfloat16),
                pltpu.SemaphoreType.DMA,
            ],
        ),
        out_shape=[quarter] * 4 + [half] * 2,
        compiler_params=params(24),
        cost_estimate=pl.CostEstimate(
            flops=model * rows * both, bytes_accessed=2 * model * rows, transcendentals=0
        ),
        name="sums",
    )(asked, place, in_hbm(back), in_hbm(turned))


def final_kernel(store_ref, gain_ref, *refs):
    parts, weights = refs[:4], refs[4:8]
    out_hbm, grads, out_ref, *held, sems = refs[8:]
    arrivals = [pltpu.make_async_copy(w, h, sems.at[i]) for i, (w, h) in enumerate(zip(weights, held))]
    for arrival in arrivals:
        arrival.start()
    for i, arrival in enumerate(arrivals):
        arrival.wait()
        made = dot_nt(parts[i][...], held[i][...])
        grads[...] = made if i == 0 else grads[...] + made
    step = 64
    sent = []
    for i in range(grads.shape[0] // step):
        at = slice(i * step, (i + 1) * step)
        rows = store_ref[at].astype(jnp.float32)
        inverse = lax.rsqrt(jnp.mean(rows * rows, axis=-1, keepdims=True) + EPS)
        unit = rows * inverse
        grad_unit = grads[at] * gain_ref[...]
        mean = jnp.mean(grad_unit * unit, axis=-1, keepdims=True)
        out_ref[at] = inverse * (grad_unit - unit * mean)
        sent.append(pltpu.make_async_copy(out_ref.at[at], out_hbm.at[at], sems.at[4 + i]))
        sent[-1].start()
    for copy in sent:
        copy.wait()


def store_gradient(place, store, gain, parts, weights):
    quarter, both = parts[0].shape
    model = store.shape[1]

    def kernel(place_ref, *refs):
        final_kernel(*refs)

    return pl.pallas_call(
        kernel,
        grid_spec=pltpu.PrefetchScalarGridSpec(
            num_scalar_prefetch=1,
            grid=(1,),
            in_specs=[
                pl.BlockSpec((quarter, model), lambda i, t: (t[0], 0)),
                pl.BlockSpec((1, model), lambda i, t: (0, 0)),
            ]
            + [pl.BlockSpec((quarter, both), lambda i, t: (0, 0))] * 4
            + [pl.BlockSpec(memory_space=pltpu.HBM)] * 4,
            out_specs=pl.BlockSpec(memory_space=pltpu.HBM),
            scratch_shapes=[
                pltpu.VMEM((quarter, model), jnp.float32),
                pltpu.VMEM((quarter, model), jnp.float32),
            ]
            + [pltpu.VMEM((model, both), jnp.bfloat16)] * 4
            + [pltpu.SemaphoreType.DMA((4 + quarter // 64,))],
        ),
        out_shape=jax.ShapeDtypeStruct((quarter, model), jnp.float32),
        compiler_params=params(28),
        cost_estimate=pl.CostEstimate(
            flops=8 * quarter * model * both,
            bytes_accessed=8 * model * both + 6 * quarter * model,
            transcendentals=quarter,
        ),
        name="store_gradient",
    )(place, in_hbm(store), in_hbm(gain), *parts, *[in_hbm(w) for w in weights])


def shifted(value, turn):
    return lax.ppermute(value, "tp", [(i, (i + turn) % 4) for i in range(4)])


def local(queries, gate_pre, cotangent, store, store_gain, w_key, w_value, owners, slots):
    st_size = lax.axis_size(ST)
    width = queries.shape[1]
    rows_dev, model = store.shape
    passages = rows_dev // PLEN
    place = jnp.stack([lax.axis_index("tp"), lax.axis_index("st_2")]).astype(jnp.int32)
    gain = store_gain.reshape(1, model)

    owner_turned = owners.T
    hits = owner_turned[:, :, None] == jnp.arange(st_size, dtype=jnp.int32)[None, None, :]
    requests = jnp.max(jnp.where(hits, slots.T[:, :, None], -1), axis=(0, 1))
    asked = requests.reshape(st_size, 1)
    asked = lax.all_to_all(asked, ST, split_axis=0, concat_axis=0, tiled=True).reshape(st_size)

    table = key_value_tables(store, gain, w_key, w_value)
    picked = picked_passages(asked, table.reshape(passages, PLEN, 2 * width))
    got = lax.all_to_all(picked, ST, split_axis=0, concat_axis=0, tiled=True)

    both = jnp.concatenate([w_key, w_value], axis=1)
    weights = [both] + [shifted(both, turn) for turn in (1, 3, 2)]
    turned = turned_normed(store, gain)
    got, turned = lax.optimization_barrier((got, turned))

    grad_queries, outgoing = attention(owner_turned, queries, gate_pre, cotangent, got)
    back = lax.all_to_all(outgoing, ST, split_axis=0, concat_axis=0, tiled=True)

    own, first, second, third, mine, other = passage_sums(
        asked, place, back, turned, passages, st_size
    )
    terms = mine + lax.ppermute(other, "st_2", [(0, 1), (1, 0)])
    terms = lax.all_to_all(terms, CHIPS, split_axis=0, concat_axis=0, tiled=True)
    grad_w_value = jnp.sum(terms.astype(jnp.float32), axis=0)

    parts = [own, shifted(first, 1), shifted(third, 3), shifted(second, 2)]
    grad_store = store_gradient(place, store, gain, parts, weights)
    return (grad_queries, grad_store, grad_w_value)


def solution(mesh):
    torus = Mesh(mesh.devices.reshape(8, 4, 2, mesh.shape["tp"]), ("st_0", "st_1", "st_2", "tp"))
    return jax.shard_map(
        local,
        mesh=torus,
        in_specs=(
            P(ST, "tp"),
            P(ST, "tp"),
            P(ST, "tp"),
            P(ST, None),
            P(),
            P(None, "tp"),
            P(None, "tp"),
            P(ST, None),
            P(ST, None),
        ),
        out_specs=(P(ST, "tp"), P(ST_TP, None), P(ST, "tp")),
        check_vma=False,
    )
```

```python
import jax
import jax.numpy as jnp
from jax import lax
from jax.experimental import pallas as pl
from jax.experimental.pallas import tpu as pltpu
from jax.sharding import Mesh
from jax.sharding import PartitionSpec as P

HD = 128
PLEN = 64
EPS = 1e-06
ST = ("st_0", "st_1", "st_2")
CHIPS = ("st_0", "st_1")
ST_TP = ("st_0", "st_1", "st_2", "tp")
MIB = 1024 * 1024


def params(mib):
    return pltpu.CompilerParams(
        dimension_semantics=("arbitrary",), vmem_limit_bytes=mib * MIB
    )


def in_hbm(value):
    return pltpu.with_memory_space_constraint(value, pltpu.HBM)


def dot_nn(a, b):
    return lax.dot_general(a, b, (((1,), (0,)), ((), ())), preferred_element_type=jnp.float32)


def dot_nt(a, b):
    return lax.dot_general(a, b, (((1,), (1,)), ((), ())), preferred_element_type=jnp.float32)


def dot_tn(a, b):
    return lax.dot_general(a, b, (((0,), (0,)), ((), ())), preferred_element_type=jnp.float32)


def normed_rows(x, gain):
    inverse = lax.rsqrt(jnp.mean(x * x, axis=-1, keepdims=True) + EPS)
    return (x * inverse * gain).astype(jnp.bfloat16)


def tables_kernel(store_ref, gain_ref, wk_hbm, wv_hbm, table_ref, wk_ref, wv_ref, sems):
    first = pl.program_id(0) == 0
    width = wk_ref.shape[1]
    keys_in = pltpu.make_async_copy(wk_hbm, wk_ref, sems.at[0])
    values_in = pltpu.make_async_copy(wv_hbm, wv_ref, sems.at[1])

    @pl.when(first)
    def _():
        keys_in.start()
        values_in.start()

    normed = normed_rows(store_ref[...].astype(jnp.float32), gain_ref[...])

    @pl.when(first)
    def _():
        keys_in.wait()
        values_in.wait()

    table_ref[:, :width] = dot_nn(normed, wk_ref[...]).astype(jnp.bfloat16)
    table_ref[:, width:] = dot_nn(normed, wv_ref[...]).astype(jnp.bfloat16)


def key_value_tables(store, gain, w_key, w_value):
    rows, model = store.shape
    width = w_key.shape[1]
    step = 256
    return pl.pallas_call(
        tables_kernel,
        grid=(rows // step,),
        in_specs=[
            pl.BlockSpec((step, model), lambda i: (i, 0)),
            pl.BlockSpec((1, model), lambda i: (0, 0)),
            pl.BlockSpec(memory_space=pltpu.HBM),
            pl.BlockSpec(memory_space=pltpu.HBM),
        ],
        out_specs=pl.BlockSpec((step, 2 * width), lambda i: (i, 0)),
        out_shape=jax.ShapeDtypeStruct((rows, 2 * width), jnp.bfloat16),
        scratch_shapes=[
            pltpu.VMEM((model, width), jnp.bfloat16),
            pltpu.VMEM((model, width), jnp.bfloat16),
            pltpu.SemaphoreType.DMA((2,)),
        ],
        compiler_params=params(16),
        cost_estimate=pl.CostEstimate(
            flops=4 * rows * model * width, bytes_accessed=2 * rows * model, transcendentals=rows
        ),
        name="tables",
    )(in_hbm(store), in_hbm(gain), in_hbm(w_key), in_hbm(w_value))


def turned_kernel(store_ref, gain_ref, out_ref):
    normed = normed_rows(store_ref[...].astype(jnp.float32), gain_ref[...])
    out_ref[...] = normed.T


def turned_normed(store, gain):
    rows, model = store.shape
    step = 256
    return pl.pallas_call(
        turned_kernel,
        grid=(rows // step,),
        in_specs=[
            pl.BlockSpec((step, model), lambda i: (i, 0)),
            pl.BlockSpec((1, model), lambda i: (0, 0)),
        ],
        out_specs=pl.BlockSpec((model, step), lambda i: (0, i)),
        out_shape=pltpu.HBM((model, rows), jnp.bfloat16),
        compiler_params=params(16),
        cost_estimate=pl.CostEstimate(
            flops=16 * rows * model, bytes_accessed=4 * rows * model, transcendentals=rows
        ),
        name="turned_normed",
    )(in_hbm(store), in_hbm(gain))


def gather_kernel(asked_ref, table_ref, out_hbm, sems):
    copies = []
    for i in range(out_hbm.shape[0]):
        asked = jnp.maximum(asked_ref[i], 0)
        copies.append(pltpu.make_async_copy(table_ref.at[asked], out_hbm.at[i], sems.at[i]))
        copies[-1].start()
    for copy in copies:
        copy.wait()


def picked_passages(asked, table):
    _, length, width = table.shape
    slots = asked.shape[0]
    return pl.pallas_call(
        gather_kernel,
        in_specs=[
            pl.BlockSpec(memory_space=pltpu.SMEM),
            pl.BlockSpec(memory_space=pltpu.VMEM),
        ],
        out_specs=pl.BlockSpec(memory_space=pltpu.HBM),
        out_shape=pltpu.HBM((slots, length, width), jnp.bfloat16),
        scratch_shapes=[pltpu.SemaphoreType.DMA((slots,))],
        compiler_params=pltpu.CompilerParams(vmem_limit_bytes=8 * MIB),
        name="picked",
    )(asked, table)


def attention_kernel(owner_ref, q_ref, g_ref, c_ref, *refs):
    pieces, (gq_ref, out_hbm, scratch, sems) = refs[:-4], refs[-4:]
    step, steps = pl.program_id(0), pl.num_programs(0)
    width = q_ref.shape[1]
    per_block = owner_ref.shape[0]
    each = len(pieces) // per_block
    length = q_ref.shape[0] // each
    scale = HD ** (-0.5)
    slot = lax.rem(step, 2)

    def copies(at, parity):
        return [
            pltpu.make_async_copy(
                scratch.at[parity, b * per_block + j],
                out_hbm.at[owner_ref[j, at * each + b]],
                sems.at[parity, b * per_block + j],
            )
            for b in range(each)
            for j in range(per_block)
        ]

    gate = jax.nn.sigmoid(g_ref[...].astype(jnp.float32))
    grad_in = (gate * c_ref[...].astype(jnp.float32)).astype(jnp.bfloat16)
    units = [(b, h) for b in range(each) for h in range(width // HD)]
    rows = [slice(b * length, (b + 1) * length) for b, _ in units]
    cols = [slice(h * HD, (h + 1) * HD) for _, h in units]
    vcols = [slice(width + h * HD, width + (h + 1) * HD) for _, h in units]
    own = [pieces[b * per_block : (b + 1) * per_block] for b, _ in units]
    count = range(len(units))
    q = [q_ref[rows[u], cols[u]] for u in count]
    gin = [grad_in[rows[u], cols[u]] for u in count]
    keys = [jnp.concatenate([p[0, :, cols[u]] for p in own[u]], axis=0) for u in count]
    values = [jnp.concatenate([p[0, :, vcols[u]] for p in own[u]], axis=0) for u in count]
    scores = [dot_nt(q[u], keys[u]) * scale for u in count]
    grad_weights = [dot_nt(gin[u], values[u]) for u in count]
    weights = [jnp.exp(x - jnp.max(x, axis=-1, keepdims=True)) for x in scores]
    weights = [x / jnp.sum(x, axis=-1, keepdims=True) for x in weights]
    half = [x.astype(jnp.bfloat16) for x in weights]
    delta = [
        jnp.sum(half[u].astype(jnp.float32) * grad_weights[u], axis=-1, keepdims=True)
        for u in count
    ]
    grad_half = [
        (weights[u] * (grad_weights[u] - delta[u])).astype(jnp.bfloat16) for u in count
    ]

    @pl.when(step >= 2)
    def _():
        for copy in copies(step - 2, slot):
            copy.wait()

    for u, (b, _) in enumerate(units):
        gq_ref[rows[u], cols[u]] = dot_nn(grad_half[u], keys[u]) * scale
        grad_keys = (dot_tn(grad_half[u], q[u]) * scale).astype(jnp.bfloat16)
        grad_values = dot_tn(half[u], gin[u]).astype(jnp.bfloat16)
        for j in range(per_block):
            part = slice(j * PLEN, (j + 1) * PLEN)
            scratch[slot, b * per_block + j, :, cols[u]] = grad_keys[part]
            scratch[slot, b * per_block + j, :, vcols[u]] = grad_values[part]

    for copy in copies(step, slot):
        copy.start()

    @pl.when(step == steps - 1)
    def _():
        for copy in copies(step - 1, 1 - slot):
            copy.wait()
        for copy in copies(step, slot):
            copy.wait()


def attention(owner_turned, queries, gate_pre, cotangent, got):
    rows, width = queries.shape
    per_block, blocks = owner_turned.shape
    each = 2
    steps = blocks // each
    tokens = pl.BlockSpec((rows // steps, width), lambda i, o: (i, 0))

    def piece(b, j):
        return pl.BlockSpec((1,) + got.shape[1:], lambda i, o: (o[j, i * each + b], 0, 0))

    pieces = [piece(b, j) for b in range(each) for j in range(per_block)]
    keys = PLEN * per_block
    return pl.pallas_call(
        attention_kernel,
        grid_spec=pltpu.PrefetchScalarGridSpec(
            num_scalar_prefetch=1,
            grid=(steps,),
            in_specs=[tokens, tokens, tokens] + pieces,
            out_specs=[tokens, pl.BlockSpec(memory_space=pltpu.HBM)],
            scratch_shapes=[
                pltpu.VMEM((2, len(pieces)) + got.shape[1:], jnp.bfloat16),
                pltpu.SemaphoreType.DMA((2, len(pieces))),
            ],
        ),
        out_shape=[
            jax.ShapeDtypeStruct((rows, width), jnp.float32),
            pltpu.HBM(got.shape, jnp.bfloat16),
        ],
        compiler_params=params(20),
        cost_estimate=pl.CostEstimate(
            flops=10 * rows * width * keys,
            bytes_accessed=10 * rows * width + 2 * got.size,
            transcendentals=rows * width * keys // HD,
        ),
        name="attention",
    )(
        owner_turned,
        in_hbm(queries),
        in_hbm(gate_pre),
        in_hbm(cotangent),
        *([in_hbm(got)] * len(pieces)),
    )


def add_asked(asked_ref, back_ref, total):
    step = pl.program_id(0)
    each = back_ref.shape[0]

    @pl.when(step == 0)
    def _():
        total[...] = jnp.zeros_like(total)

    for i in range(each):
        asked = asked_ref[step * each + i]

        @pl.when(asked >= 0)
        def _():
            total[asked] += back_ref[i].astype(jnp.float32)


def value_kernel(asked_ref, place_ref, back_ref, turned_hbm, *refs):
    values_ref, mine_ref, other_ref, total, terms, turned_ref, sem = refs
    turned_in = pltpu.make_async_copy(turned_hbm, turned_ref, sem)

    @pl.when(pl.program_id(0) == 0)
    def _():
        turned_in.start()

    add_asked(asked_ref, back_ref, total)

    @pl.when(pl.program_id(0) == pl.num_programs(0) - 1)
    def _():
        values = total[...].astype(jnp.bfloat16).reshape(values_ref.shape)
        values_ref[...] = values
        pieces, piece, _ = terms.shape
        turned_in.wait()
        made = dot_nn(turned_ref[...], values).astype(jnp.bfloat16)
        for p in range(pieces):
            terms[p] = made[p * piece : (p + 1) * piece]
        for p in range(pieces // 2):
            mine_ref[p] = terms[2 * p + place_ref[1]]
            other_ref[p] = terms[2 * p + 1 - place_ref[1]]


def value_sums(asked, place, back, turned, passages, devices):
    slots, length, both = back.shape
    model, rows = turned.shape
    width = both // 2
    each = 16
    values = jax.ShapeDtypeStruct((rows, width), jnp.bfloat16)
    half = jax.ShapeDtypeStruct((devices // 2, model // devices, width), jnp.bfloat16)
    return pl.pallas_call(
        value_kernel,
        grid_spec=pltpu.PrefetchScalarGridSpec(
            num_scalar_prefetch=2,
            grid=(slots // each,),
            in_specs=[
                pl.BlockSpec((each, length, width), lambda i, a, t: (i, 0, 1)),
                pl.BlockSpec(memory_space=pltpu.HBM),
            ],
            out_specs=[pl.BlockSpec(values.shape, lambda i, a, t: (0, 0))]
            + [pl.BlockSpec(half.shape, lambda i, a, t: (0, 0, 0))] * 2,
            scratch_shapes=[
                pltpu.VMEM((passages, length, width), jnp.float32),
                pltpu.VMEM((devices, model // devices, width), jnp.bfloat16),
                pltpu.VMEM((model, rows), jnp.bfloat16),
                pltpu.SemaphoreType.DMA,
            ],
        ),
        out_shape=[values, half, half],
        compiler_params=params(24),
        cost_estimate=pl.CostEstimate(
            flops=2 * model * rows * width, bytes_accessed=2 * model * rows, transcendentals=0
        ),
        name="value_sums",
    )(asked, place, in_hbm(back), in_hbm(turned))


def key_kernel(asked_ref, place_ref, back_ref, values_ref, *refs):
    parts, total = refs[:4], refs[4]
    add_asked(asked_ref, back_ref, total)
    passages, length, width = total.shape
    share = passages // 4

    @pl.when(pl.program_id(0) == pl.num_programs(0) - 1)
    def _():
        for turn, out in enumerate(parts):
            first = lax.rem(place_ref[0] + turn, 4) * share
            for p in range(share):
                rows = slice(p * length, (p + 1) * length)
                out[rows, :width] = total[first + p].astype(jnp.bfloat16)
            taken = pl.ds(pl.multiple_of(first * length, length), share * length)
            out[:, width:] = values_ref[taken, :]


def key_sums(asked, place, back, values, passages):
    slots, length, both = back.shape
    rows, width = values.shape
    each = 16
    quarter = jax.ShapeDtypeStruct((rows // 4, both), jnp.bfloat16)
    return pl.pallas_call(
        key_kernel,
        grid_spec=pltpu.PrefetchScalarGridSpec(
            num_scalar_prefetch=2,
            grid=(slots // each,),
            in_specs=[
                pl.BlockSpec((each, length, width), lambda i, a, t: (i, 0, 0)),
                pl.BlockSpec(memory_space=pltpu.VMEM),
            ],
            out_specs=[pl.BlockSpec(quarter.shape, lambda i, a, t: (0, 0))] * 4,
            scratch_shapes=[pltpu.VMEM((passages, length, width), jnp.float32)],
        ),
        out_shape=[quarter] * 4,
        compiler_params=params(16),
        cost_estimate=pl.CostEstimate(
            flops=4 * back.size, bytes_accessed=2 * back.size, transcendentals=0
        ),
        name="key_sums",
    )(asked, place, in_hbm(back), values)


def products(parts, weights, held, sems):
    arrivals = [
        pltpu.make_async_copy(w, h, sems.at[i]) for i, (w, h) in enumerate(zip(weights, held))
    ]
    for arrival in arrivals:
        arrival.start()
    made = []
    for part, arrival, h in zip(parts, arrivals, held):
        arrival.wait()
        made.append(dot_nt(part[...], h[...]))
    return made


def near_kernel(*refs):
    count = 3
    parts, weights, out_ref = refs[:count], refs[count : 2 * count], refs[2 * count]
    held, sems = refs[2 * count + 1 : -1], refs[-1]
    out_ref[...] = sum(products(parts, weights, held, sems))


def near_products(parts, weights):
    quarter, both = parts[0].shape
    model = weights[0].shape[0]
    count = len(parts)
    return pl.pallas_call(
        near_kernel,
        in_specs=[pl.BlockSpec(memory_space=pltpu.VMEM)] * count
        + [pl.BlockSpec(memory_space=pltpu.HBM)] * count,
        out_specs=pl.BlockSpec(memory_space=pltpu.VMEM),
        out_shape=jax.ShapeDtypeStruct((quarter, model), jnp.float32),
        scratch_shapes=[pltpu.VMEM((model, both), jnp.bfloat16)] * count
        + [pltpu.SemaphoreType.DMA((count,))],
        compiler_params=pltpu.CompilerParams(vmem_limit_bytes=24 * MIB),
        cost_estimate=pl.CostEstimate(
            flops=2 * count * quarter * model * both,
            bytes_accessed=2 * count * model * both,
            transcendentals=0,
        ),
        name="near_products",
    )(*parts, *[in_hbm(w) for w in weights])


def final_kernel(place_ref, store_ref, gain_ref, near_ref, part_ref, weight_hbm, out_hbm, out_ref, held, sems):
    (made,) = products([part_ref], [weight_hbm], [held], sems)
    step = 64
    sent = []
    for i in range(out_ref.shape[0] // step):
        at = slice(i * step, (i + 1) * step)
        rows = store_ref[at].astype(jnp.float32)
        inverse = lax.rsqrt(jnp.mean(rows * rows, axis=-1, keepdims=True) + EPS)
        unit = rows * inverse
        grad_unit = (near_ref[at] + made[at]) * gain_ref[...]
        mean = jnp.mean(grad_unit * unit, axis=-1, keepdims=True)
        out_ref[at] = inverse * (grad_unit - unit * mean)
        sent.append(pltpu.make_async_copy(out_ref.at[at], out_hbm.at[at], sems.at[1 + i]))
        sent[-1].start()
    for copy in sent:
        copy.wait()


def store_gradient(place, store, gain, near, part, weight):
    quarter, both = part.shape
    model = store.shape[1]
    return pl.pallas_call(
        final_kernel,
        grid_spec=pltpu.PrefetchScalarGridSpec(
            num_scalar_prefetch=1,
            grid=(1,),
            in_specs=[
                pl.BlockSpec((quarter, model), lambda i, t: (t[0], 0)),
                pl.BlockSpec((1, model), lambda i, t: (0, 0)),
                pl.BlockSpec(memory_space=pltpu.VMEM),
                pl.BlockSpec(memory_space=pltpu.VMEM),
                pl.BlockSpec(memory_space=pltpu.HBM),
            ],
            out_specs=pl.BlockSpec(memory_space=pltpu.HBM),
            scratch_shapes=[
                pltpu.VMEM((quarter, model), jnp.float32),
                pltpu.VMEM((model, both), jnp.bfloat16),
                pltpu.SemaphoreType.DMA((1 + quarter // 64,)),
            ],
        ),
        out_shape=jax.ShapeDtypeStruct((quarter, model), jnp.float32),
        compiler_params=params(20),
        cost_estimate=pl.CostEstimate(
            flops=2 * quarter * model * both,
            bytes_accessed=2 * model * both + 10 * quarter * model,
            transcendentals=quarter,
        ),
        name="store_gradient",
    )(place, in_hbm(store), in_hbm(gain), near, part, in_hbm(weight))


def shifted(value, turn):
    return lax.ppermute(value, "tp", [(i, (i + turn) % 4) for i in range(4)])


def local(queries, gate_pre, cotangent, store, store_gain, w_key, w_value, owners, slots):
    st_size = lax.axis_size(ST)
    width = queries.shape[1]
    rows_dev, model = store.shape
    passages = rows_dev // PLEN
    place = jnp.stack([lax.axis_index("tp"), lax.axis_index("st_2")]).astype(jnp.int32)
    gain = store_gain.reshape(1, model)

    owner_turned = owners.T
    hits = owner_turned[None] == jnp.arange(st_size, dtype=jnp.int32)[:, None, None]
    requests = jnp.where(hits, slots.T[None], -1)
    asked = lax.all_to_all(requests, ST, split_axis=0, concat_axis=0, tiled=True)
    asked = jnp.max(asked, axis=(1, 2))

    table = key_value_tables(store, gain, w_key, w_value)
    picked = picked_passages(asked, table.reshape(passages, PLEN, 2 * width))
    got = lax.all_to_all(picked, ST, split_axis=0, concat_axis=0, tiled=True)

    both = jnp.concatenate([w_key, w_value], axis=1)
    near_weights = [both, shifted(both, 1), shifted(both, 3)]
    far_weight = shifted(both, 2)

    grad_queries, outgoing = attention(owner_turned, queries, gate_pre, cotangent, got)
    back = lax.all_to_all(outgoing, ST, split_axis=0, concat_axis=0, tiled=True)
    late_store, _ = lax.optimization_barrier((store, outgoing))
    turned = turned_normed(late_store, gain)
    back, turned = lax.optimization_barrier((back, turned))

    values, mine, other = value_sums(asked, place, back, turned, passages, st_size)
    terms = mine + lax.ppermute(other, "st_2", [(0, 1), (1, 0)])
    terms = lax.all_to_all(terms, CHIPS, split_axis=0, concat_axis=0, tiled=True)
    grad_w_value = jnp.sum(terms.astype(jnp.float32), axis=0)

    own, first, second, third = key_sums(asked, place, back, values, passages)
    near = near_products([own, shifted(first, 1), shifted(third, 3)], near_weights)
    grad_store = store_gradient(place, store, gain, near, shifted(second, 2), far_weight)
    return (grad_queries, grad_store, grad_w_value)


def solution(mesh):
    torus = Mesh(mesh.devices.reshape(8, 4, 2, mesh.shape["tp"]), ("st_0", "st_1", "st_2", "tp"))
    return jax.shard_map(
        local,
        mesh=torus,
        in_specs=(
            P(ST, "tp"),
            P(ST, "tp"),
            P(ST, "tp"),
            P(ST, None),
            P(),
            P(None, "tp"),
            P(None, "tp"),
            P(ST, None),
            P(ST, None),
        ),
        out_specs=(P(ST, "tp"), P(ST_TP, None), P(ST, "tp")),
        check_vma=False,
    )
```

```python
import jax
import jax.numpy as jnp
from jax import lax
from jax.experimental import pallas as pl
from jax.experimental.pallas import tpu as pltpu
from jax.sharding import Mesh
from jax.sharding import PartitionSpec as P

HD = 128
PLEN = 64
EPS = 1e-06
ST = ("st_0", "st_1", "st_2")
CHIPS = ("st_0", "st_1")
ST_TP = ("st_0", "st_1", "st_2", "tp")
MIB = 1024 * 1024


def params(mib):
    return pltpu.CompilerParams(
        dimension_semantics=("arbitrary",), vmem_limit_bytes=mib * MIB
    )


def in_hbm(value):
    return pltpu.with_memory_space_constraint(value, pltpu.HBM)


def dot_nn(a, b):
    return lax.dot_general(a, b, (((1,), (0,)), ((), ())), preferred_element_type=jnp.float32)


def dot_nt(a, b):
    return lax.dot_general(a, b, (((1,), (1,)), ((), ())), preferred_element_type=jnp.float32)


def dot_tn(a, b):
    return lax.dot_general(a, b, (((0,), (0,)), ((), ())), preferred_element_type=jnp.float32)


def normed_rows(x, gain):
    inverse = lax.rsqrt(jnp.mean(x * x, axis=-1, keepdims=True) + EPS)
    return (x * inverse * gain).astype(jnp.bfloat16)


def tables_kernel(store_ref, gain_ref, wk_hbm, wv_hbm, table_ref, wk_ref, wv_ref, sems):
    first = pl.program_id(0) == 0
    width = wk_ref.shape[1]
    keys_in = pltpu.make_async_copy(wk_hbm, wk_ref, sems.at[0])
    values_in = pltpu.make_async_copy(wv_hbm, wv_ref, sems.at[1])

    @pl.when(first)
    def _():
        keys_in.start()
        values_in.start()

    normed = normed_rows(store_ref[...].astype(jnp.float32), gain_ref[...])

    @pl.when(first)
    def _():
        keys_in.wait()
        values_in.wait()

    table_ref[:, :width] = dot_nn(normed, wk_ref[...]).astype(jnp.bfloat16)
    table_ref[:, width:] = dot_nn(normed, wv_ref[...]).astype(jnp.bfloat16)


def key_value_tables(store, gain, w_key, w_value):
    rows, model = store.shape
    width = w_key.shape[1]
    step = 256
    return pl.pallas_call(
        tables_kernel,
        grid=(rows // step,),
        in_specs=[
            pl.BlockSpec((step, model), lambda i: (i, 0)),
            pl.BlockSpec((1, model), lambda i: (0, 0)),
            pl.BlockSpec(memory_space=pltpu.HBM),
            pl.BlockSpec(memory_space=pltpu.HBM),
        ],
        out_specs=pl.BlockSpec((step, 2 * width), lambda i: (i, 0)),
        out_shape=jax.ShapeDtypeStruct((rows, 2 * width), jnp.bfloat16),
        scratch_shapes=[
            pltpu.VMEM((model, width), jnp.bfloat16),
            pltpu.VMEM((model, width), jnp.bfloat16),
            pltpu.SemaphoreType.DMA((2,)),
        ],
        compiler_params=params(16),
        cost_estimate=pl.CostEstimate(
            flops=4 * rows * model * width, bytes_accessed=2 * rows * model, transcendentals=rows
        ),
        name="tables",
    )(in_hbm(store), in_hbm(gain), in_hbm(w_key), in_hbm(w_value))


def turned_kernel(store_ref, gain_ref, out_ref):
    normed = normed_rows(store_ref[...].astype(jnp.float32), gain_ref[...])
    out_ref[...] = normed.T


def turned_normed(store, gain):
    rows, model = store.shape
    step = 256
    return pl.pallas_call(
        turned_kernel,
        grid=(rows // step,),
        in_specs=[
            pl.BlockSpec((step, model), lambda i: (i, 0)),
            pl.BlockSpec((1, model), lambda i: (0, 0)),
        ],
        out_specs=pl.BlockSpec((model, step), lambda i: (0, i)),
        out_shape=pltpu.HBM((model, rows), jnp.bfloat16),
        compiler_params=params(16),
        cost_estimate=pl.CostEstimate(
            flops=16 * rows * model, bytes_accessed=4 * rows * model, transcendentals=rows
        ),
        name="turned_normed",
    )(in_hbm(store), in_hbm(gain))


def gather_kernel(asked_ref, table_ref, out_hbm, sems):
    copies = []
    for i in range(out_hbm.shape[0]):
        asked = jnp.maximum(asked_ref[i], 0)
        copies.append(pltpu.make_async_copy(table_ref.at[asked], out_hbm.at[i], sems.at[i]))
        copies[-1].start()
    for copy in copies:
        copy.wait()


def picked_passages(asked, table):
    _, length, width = table.shape
    slots = asked.shape[0]
    return pl.pallas_call(
        gather_kernel,
        in_specs=[
            pl.BlockSpec(memory_space=pltpu.SMEM),
            pl.BlockSpec(memory_space=pltpu.VMEM),
        ],
        out_specs=pl.BlockSpec(memory_space=pltpu.HBM),
        out_shape=pltpu.HBM((slots, length, width), jnp.bfloat16),
        scratch_shapes=[pltpu.SemaphoreType.DMA((slots,))],
        compiler_params=pltpu.CompilerParams(vmem_limit_bytes=8 * MIB),
        name="picked",
    )(asked, table)


def slot_copies(owner_ref, scratch, out_hbm, sems, at, parity):
    per_block = owner_ref.shape[0]
    each = scratch.shape[1] // per_block
    return [
        pltpu.make_async_copy(
            scratch.at[parity, b * per_block + j],
            out_hbm.at[owner_ref[j, at * each + b]],
            sems.at[parity, b * per_block + j],
        )
        for b in range(each)
        for j in range(per_block)
    ]


def wait_slots(owner_ref, scratch, out_hbm, sems):
    step = pl.program_id(0)

    @pl.when(step >= 2)
    def _():
        for copy in slot_copies(owner_ref, scratch, out_hbm, sems, step - 2, lax.rem(step, 2)):
            copy.wait()


def send_slots(owner_ref, scratch, out_hbm, sems):
    step, steps = pl.program_id(0), pl.num_programs(0)
    slot = lax.rem(step, 2)
    for copy in slot_copies(owner_ref, scratch, out_hbm, sems, step, slot):
        copy.start()

    @pl.when(step == steps - 1)
    def _():
        for copy in slot_copies(owner_ref, scratch, out_hbm, sems, step - 1, 1 - slot):
            copy.wait()
        for copy in slot_copies(owner_ref, scratch, out_hbm, sems, step, slot):
            copy.wait()


def block_units(owner_ref, q_ref, g_ref, c_ref, pieces):
    width = q_ref.shape[1]
    per_block = owner_ref.shape[0]
    each = len(pieces) // per_block
    length = q_ref.shape[0] // each
    gate = jax.nn.sigmoid(g_ref[...].astype(jnp.float32))
    grad_in = (gate * c_ref[...].astype(jnp.float32)).astype(jnp.bfloat16)
    units = []
    for b in range(each):
        for h in range(width // HD):
            rows = slice(b * length, (b + 1) * length)
            cols = slice(h * HD, (h + 1) * HD)
            own = pieces[b * per_block : (b + 1) * per_block]
            keys = jnp.concatenate([p[0, :, cols] for p in own], axis=0)
            units.append((b, rows, cols, own, q_ref[rows, cols], grad_in[rows, cols], keys))
    scores = [dot_nt(u[4], u[6]) * HD ** (-0.5) for u in units]
    weights = [jnp.exp(x - jnp.max(x, axis=-1, keepdims=True)) for x in scores]
    weights = [x / jnp.sum(x, axis=-1, keepdims=True) for x in weights]
    return units, weights


def value_slots_kernel(owner_ref, q_ref, g_ref, c_ref, *refs):
    pieces, (out_hbm, scratch, sems) = refs[:-3], refs[-3:]
    per_block = owner_ref.shape[0]
    slot = lax.rem(pl.program_id(0), 2)
    units, weights = block_units(owner_ref, q_ref, g_ref, c_ref, pieces)
    wait_slots(owner_ref, scratch, out_hbm, sems)
    for (b, _, cols, _, _, gin, _), weight in zip(units, weights):
        grad_values = dot_tn(weight.astype(jnp.bfloat16), gin).astype(jnp.bfloat16)
        for j in range(per_block):
            part = slice(j * PLEN, (j + 1) * PLEN)
            scratch[slot, b * per_block + j, :, cols] = grad_values[part]
    send_slots(owner_ref, scratch, out_hbm, sems)


def key_slots_kernel(owner_ref, q_ref, g_ref, c_ref, *refs):
    pieces, (gq_ref, out_hbm, scratch, sems) = refs[:-4], refs[-4:]
    per_block = owner_ref.shape[0]
    width = q_ref.shape[1]
    slot = lax.rem(pl.program_id(0), 2)
    units, weights = block_units(owner_ref, q_ref, g_ref, c_ref, pieces)
    grad_weights = []
    for _, _, cols, own, _, gin, _ in units:
        vcols = slice(width + cols.start, width + cols.stop)
        values = jnp.concatenate([p[0, :, vcols] for p in own], axis=0)
        grad_weights.append(dot_nt(gin, values))
    delta = [
        jnp.sum(w.astype(jnp.bfloat16).astype(jnp.float32) * g, axis=-1, keepdims=True)
        for w, g in zip(weights, grad_weights)
    ]
    halves = [(w * (g - d)).astype(jnp.bfloat16) for w, g, d in zip(weights, grad_weights, delta)]
    wait_slots(owner_ref, scratch, out_hbm, sems)
    for (b, rows, cols, _, q, _, keys), half in zip(units, halves):
        gq_ref[rows, cols] = dot_nn(half, keys) * HD ** (-0.5)
        grad_keys = (dot_tn(half, q) * HD ** (-0.5)).astype(jnp.bfloat16)
        for j in range(per_block):
            part = slice(j * PLEN, (j + 1) * PLEN)
            scratch[slot, b * per_block + j, :, cols] = grad_keys[part]
    send_slots(owner_ref, scratch, out_hbm, sems)


def attention(owner_turned, queries, gate_pre, cotangent, got, keys_only):
    rows, width = queries.shape
    per_block, blocks = owner_turned.shape
    slots, length, both = got.shape
    each = 2
    steps = blocks // each
    tokens = pl.BlockSpec((rows // steps, width), lambda i, o: (i, 0))
    read = width if keys_only else both

    def piece(b, j):
        return pl.BlockSpec((1, length, read), lambda i, o: (o[j, i * each + b], 0, 0))

    pieces = [piece(b, j) for b in range(each) for j in range(per_block)]
    keys = PLEN * per_block
    out = pltpu.HBM((slots, length, width), jnp.bfloat16)
    hbm = pl.BlockSpec(memory_space=pltpu.HBM)
    return pl.pallas_call(
        value_slots_kernel if keys_only else key_slots_kernel,
        grid_spec=pltpu.PrefetchScalarGridSpec(
            num_scalar_prefetch=1,
            grid=(steps,),
            in_specs=[tokens, tokens, tokens] + pieces,
            out_specs=[hbm] if keys_only else [tokens, hbm],
            scratch_shapes=[
                pltpu.VMEM((2, len(pieces), length, width), jnp.bfloat16),
                pltpu.SemaphoreType.DMA((2, len(pieces))),
            ],
        ),
        out_shape=[out] if keys_only else [jax.ShapeDtypeStruct((rows, width), jnp.float32), out],
        compiler_params=params(20),
        cost_estimate=pl.CostEstimate(
            flops=(4 if keys_only else 8) * rows * width * keys,
            bytes_accessed=10 * rows * width + 2 * got.size,
            transcendentals=rows * width * keys // HD,
        ),
        name="value_slots" if keys_only else "key_slots",
    )(
        owner_turned,
        in_hbm(queries),
        in_hbm(gate_pre),
        in_hbm(cotangent),
        *([in_hbm(got)] * len(pieces)),
    )


def add_asked(asked_ref, back_ref, total):
    step = pl.program_id(0)
    each = back_ref.shape[0]

    @pl.when(step == 0)
    def _():
        total[...] = jnp.zeros_like(total)

    for i in range(each):
        asked = asked_ref[step * each + i]

        @pl.when(asked >= 0)
        def _():
            total[asked] += back_ref[i].astype(jnp.float32)


def write_quarters(place_ref, total, parts):
    passages, length, _ = total.shape
    share = passages // 4
    for turn, out in enumerate(parts):
        first = lax.rem(place_ref[0] + turn, 4) * share
        for p in range(share):
            out[p * length : (p + 1) * length, :] = total[first + p].astype(jnp.bfloat16)


def value_kernel(asked_ref, place_ref, back_ref, turned_hbm, *refs):
    parts, (mine_ref, other_ref, total, terms, turned_ref, sem) = refs[:4], refs[4:]
    turned_in = pltpu.make_async_copy(turned_hbm, turned_ref, sem)

    @pl.when(pl.program_id(0) == 0)
    def _():
        turned_in.start()

    add_asked(asked_ref, back_ref, total)

    @pl.when(pl.program_id(0) == pl.num_programs(0) - 1)
    def _():
        write_quarters(place_ref, total, parts)
        passages, length, width = total.shape
        values = total[...].astype(jnp.bfloat16).reshape(passages * length, width)
        pieces, piece, _ = terms.shape
        turned_in.wait()
        made = dot_nn(turned_ref[...], values).astype(jnp.bfloat16)
        for p in range(pieces):
            terms[p] = made[p * piece : (p + 1) * piece]
        for p in range(pieces // 2):
            turn = p % 8 * 8 + p // 8 * 2
            mine_ref[p] = terms[place_ref[1] ^ turn]
            other_ref[p] = terms[place_ref[1] ^ (turn + 1)]


def value_sums(asked, place, back, turned, passages, devices):
    slots, length, width = back.shape
    model, rows = turned.shape
    each = 16
    quarter = jax.ShapeDtypeStruct((rows // 4, width), jnp.bfloat16)
    half = jax.ShapeDtypeStruct((devices // 2, model // devices, width), jnp.bfloat16)
    return pl.pallas_call(
        value_kernel,
        grid_spec=pltpu.PrefetchScalarGridSpec(
            num_scalar_prefetch=2,
            grid=(slots // each,),
            in_specs=[
                pl.BlockSpec((each, length, width), lambda i, a, t: (i, 0, 0)),
                pl.BlockSpec(memory_space=pltpu.HBM),
            ],
            out_specs=[pl.BlockSpec(quarter.shape, lambda i, a, t: (0, 0))] * 4
            + [pl.BlockSpec(half.shape, lambda i, a, t: (0, 0, 0))] * 2,
            scratch_shapes=[
                pltpu.VMEM((passages, length, width), jnp.float32),
                pltpu.VMEM((devices, model // devices, width), jnp.bfloat16),
                pltpu.VMEM((model, rows), jnp.bfloat16),
                pltpu.SemaphoreType.DMA,
            ],
        ),
        out_shape=[quarter] * 4 + [half] * 2,
        compiler_params=params(24),
        cost_estimate=pl.CostEstimate(
            flops=2 * model * rows * width, bytes_accessed=2 * model * rows, transcendentals=0
        ),
        name="value_sums",
    )(asked, place, back, in_hbm(turned))


def key_kernel(asked_ref, place_ref, back_ref, *refs):
    parts, total = refs[:4], refs[4]
    add_asked(asked_ref, back_ref, total)

    @pl.when(pl.program_id(0) == pl.num_programs(0) - 1)
    def _():
        write_quarters(place_ref, total, parts)


def key_sums(asked, place, back, passages):
    slots, length, width = back.shape
    each = 16
    quarter = jax.ShapeDtypeStruct((passages * length // 4, width), jnp.bfloat16)
    return pl.pallas_call(
        key_kernel,
        grid_spec=pltpu.PrefetchScalarGridSpec(
            num_scalar_prefetch=2,
            grid=(slots // each,),
            in_specs=[pl.BlockSpec((each, length, width), lambda i, a, t: (i, 0, 0))],
            out_specs=[pl.BlockSpec(quarter.shape, lambda i, a, t: (0, 0))] * 4,
            scratch_shapes=[pltpu.VMEM((passages, length, width), jnp.float32)],
        ),
        out_shape=[quarter] * 4,
        compiler_params=params(12),
        cost_estimate=pl.CostEstimate(
            flops=4 * back.size, bytes_accessed=2 * back.size, transcendentals=0
        ),
        name="key_sums",
    )(asked, place, back)


def near_kernel(*refs):
    count = 4
    parts, weights, out_ref = refs[:count], refs[count : 2 * count], refs[2 * count]
    held, sems = refs[2 * count + 1 : -1], refs[-1]
    width = parts[0].shape[1]
    arrivals = [
        pltpu.make_async_copy(w.at[:, width:], h, sems.at[i])
        for i, (w, h) in enumerate(zip(weights, held))
    ]
    for copy in arrivals:
        copy.start()
    made = []
    for part, arrival, h in zip(parts, arrivals, held):
        arrival.wait()
        made.append(dot_nt(part[...], h[...]))
    out_ref[...] = sum(made)


def near_products(parts, weights):
    quarter, width = parts[0].shape
    model = weights[0].shape[0]
    count = len(parts)
    vmem = pl.BlockSpec(memory_space=pltpu.VMEM)
    hbm = pl.BlockSpec(memory_space=pltpu.HBM)
    return pl.pallas_call(
        near_kernel,
        in_specs=[vmem] * count + [hbm] * count,
        out_specs=vmem,
        out_shape=jax.ShapeDtypeStruct((quarter, model), jnp.float32),
        scratch_shapes=[pltpu.VMEM((model, width), jnp.bfloat16)] * count
        + [pltpu.SemaphoreType.DMA((count,))],
        compiler_params=pltpu.CompilerParams(vmem_limit_bytes=16 * MIB),
        cost_estimate=pl.CostEstimate(
            flops=2 * count * quarter * model * width,
            bytes_accessed=2 * count * model * width,
            transcendentals=0,
        ),
        name="near_products",
    )(*parts, *[in_hbm(w) for w in weights])


def own_kernel(place_ref, part_ref, near_ref, *refs):
    count = 4
    weights, store_hbm = refs[:count], refs[count]
    out_ref, rows_ref, *keys_refs = refs[count + 1 : 2 * count + 2]
    held, sems = refs[2 * count + 2], refs[-1]
    quarter, width = part_ref.shape
    first = pl.multiple_of(place_ref[0] * quarter, quarter)
    copies = [
        pltpu.make_async_copy(w.at[:, :width], k, sems.at[i])
        for i, (w, k) in enumerate(zip(weights, [held] + keys_refs))
    ]
    copies.append(
        pltpu.make_async_copy(store_hbm.at[pl.ds(first, quarter)], rows_ref, sems.at[count])
    )
    for copy in copies:
        copy.start()
    copies[0].wait()
    out_ref[...] = near_ref[...] + dot_nt(part_ref[...], held[...])
    for copy in copies[1:]:
        copy.wait()


def own_product(place, part, near, weights, store):
    quarter, width = part.shape
    model = weights[0].shape[0]
    count = len(weights)
    vmem = pl.BlockSpec(memory_space=pltpu.VMEM)
    hbm = pl.BlockSpec(memory_space=pltpu.HBM)
    return pl.pallas_call(
        own_kernel,
        in_specs=[pl.BlockSpec(memory_space=pltpu.SMEM), vmem, vmem] + [hbm] * (count + 1),
        out_specs=[vmem] * (count + 1),
        out_shape=[
            pltpu.VMEM((quarter, model), jnp.float32),
            pltpu.VMEM((quarter, model), jnp.bfloat16),
        ]
        + [pltpu.VMEM((model, width), jnp.bfloat16)] * (count - 1),
        scratch_shapes=[
            pltpu.VMEM((model, width), jnp.bfloat16),
            pltpu.SemaphoreType.DMA((count + 1,)),
        ],
        compiler_params=pltpu.CompilerParams(vmem_limit_bytes=16 * MIB),
        cost_estimate=pl.CostEstimate(
            flops=2 * quarter * model * width,
            bytes_accessed=4 * count * model * width,
            transcendentals=0,
        ),
        name="own_product",
    )(place, part, near, *[in_hbm(w) for w in weights], in_hbm(store))


def final_kernel(rows_ref, gain_ref, near_ref, *refs):
    parts, weights, (out_hbm, out_ref, sems) = refs[:3], refs[3:6], refs[6:]
    made = near_ref[...]
    for part, weight in zip(parts, weights):
        made += dot_nt(part[...], weight[...])
    step = 64
    sent = []
    for i in range(out_ref.shape[0] // step):
        at = slice(i * step, (i + 1) * step)
        rows = rows_ref[at].astype(jnp.float32)
        inverse = lax.rsqrt(jnp.mean(rows * rows, axis=-1, keepdims=True) + EPS)
        unit = rows * inverse
        grad_unit = made[at] * gain_ref[...]
        mean = jnp.mean(grad_unit * unit, axis=-1, keepdims=True)
        out_ref[at] = inverse * (grad_unit - unit * mean)
        sent.append(pltpu.make_async_copy(out_ref.at[at], out_hbm.at[at], sems.at[i]))
        sent[-1].start()
    for copy in sent:
        copy.wait()


def store_gradient(rows, gain, near, parts, weights):
    quarter, model = rows.shape
    width = parts[0].shape[1]
    vmem = pl.BlockSpec(memory_space=pltpu.VMEM)
    return pl.pallas_call(
        final_kernel,
        in_specs=[vmem] * (3 + 2 * len(parts)),
        out_specs=pl.BlockSpec(memory_space=pltpu.HBM),
        out_shape=jax.ShapeDtypeStruct((quarter, model), jnp.float32),
        scratch_shapes=[
            pltpu.VMEM((quarter, model), jnp.float32),
            pltpu.SemaphoreType.DMA((quarter // 64,)),
        ],
        compiler_params=pltpu.CompilerParams(vmem_limit_bytes=16 * MIB),
        cost_estimate=pl.CostEstimate(
            flops=6 * quarter * model * width,
            bytes_accessed=4 * quarter * model,
            transcendentals=quarter,
        ),
        name="store_gradient",
    )(rows, gain, near, *parts, *weights)


def shifted(value, turn):
    return lax.ppermute(value, "tp", [(i, (i + turn) % 4) for i in range(4)])


def halved(value, axis, distance, kind):
    size = lax.axis_size(axis)
    half = value.shape[0] // 2
    pairs = [(i, i ^ distance) for i in range(size)]
    came = lax.ppermute(value[half:].astype(kind), axis, pairs)
    return value[:half] + came.astype(jnp.float32)


def local(queries, gate_pre, cotangent, store, store_gain, w_key, w_value, owners, slots):
    st_size = lax.axis_size(ST)
    width = queries.shape[1]
    rows_dev, model = store.shape
    passages = rows_dev // PLEN
    place = jnp.stack([lax.axis_index("tp"), lax.axis_index(ST)]).astype(jnp.int32)
    gain = store_gain.reshape(1, model)

    owner_turned = owners.T
    hits = owner_turned[None] == jnp.arange(st_size, dtype=jnp.int32)[:, None, None]
    requests = jnp.where(hits, slots.T[None], -1)
    asked = lax.all_to_all(requests, ST, split_axis=0, concat_axis=0, tiled=True)
    asked = jnp.max(asked, axis=(1, 2))

    table = key_value_tables(store, gain, w_key, w_value)
    picked = picked_passages(asked, table.reshape(passages, PLEN, 2 * width))
    got = lax.all_to_all(picked, ST, split_axis=0, concat_axis=0, tiled=True)

    late_key, late_value, _ = lax.optimization_barrier((w_key, w_value, picked))
    both = jnp.concatenate([late_key, late_value], axis=1)
    weights = [both] + [shifted(both, turn) for turn in (1, 3, 2)]
    got, *weights = lax.optimization_barrier((got, *weights))

    (outgoing,) = attention(owner_turned, queries, gate_pre, cotangent, got, True)
    back_values = lax.all_to_all(outgoing, ST, split_axis=0, concat_axis=0, tiled=True)
    late_store, late_got, _ = lax.optimization_barrier((store, got, outgoing))
    grad_queries, outgoing = attention(
        owner_turned, queries, gate_pre, cotangent, late_got, False
    )
    turned = turned_normed(late_store, gain)
    outgoing, turned = lax.optimization_barrier((outgoing, turned))
    back_keys = lax.all_to_all(outgoing, ST, split_axis=0, concat_axis=0, tiled=True)
    back_values, turned, _ = lax.optimization_barrier((back_values, turned, grad_queries))

    own, first, second, third, mine, other = value_sums(
        asked, place, back_values, turned, passages, st_size
    )
    parts = [own, shifted(first, 1), shifted(third, 3), shifted(second, 2)]
    near = near_products(parts, weights)
    came = lax.ppermute(other, "st_2", [(0, 1), (1, 0)])
    terms = mine.astype(jnp.float32) + came.astype(jnp.float32)
    terms = halved(terms, "st_1", 2, jnp.bfloat16)
    terms = halved(terms, "st_1", 1, jnp.bfloat16)
    back_keys, near, terms = lax.optimization_barrier((back_keys, near, terms))

    own, first, second, third = key_sums(asked, place, back_keys, passages)
    parts = [shifted(first, 1), shifted(third, 3), shifted(second, 2)]
    near, own_rows, *key_weights = own_product(place, own, near, weights, store)
    for distance in (4, 2, 1):
        terms = halved(terms, "st_0", distance, jnp.float32)
    grad_w_value = terms.reshape(terms.shape[1:])
    grad_store = store_gradient(own_rows, gain, near, parts, key_weights)
    return (grad_queries, grad_store, grad_w_value)


def solution(mesh):
    torus = Mesh(mesh.devices.reshape(8, 4, 2, mesh.shape["tp"]), ("st_0", "st_1", "st_2", "tp"))
    return jax.shard_map(
        local,
        mesh=torus,
        in_specs=(
            P(ST, "tp"),
            P(ST, "tp"),
            P(ST, "tp"),
            P(ST, None),
            P(),
            P(None, "tp"),
            P(None, "tp"),
            P(ST, None),
            P(ST, None),
        ),
        out_specs=(P(ST, "tp"), P(ST_TP, None), P(ST, "tp")),
        check_vma=False,
    )
```

```python
import jax
import jax.numpy as jnp
from jax import lax
from jax.experimental import pallas as pl
from jax.experimental.pallas import tpu as pltpu
from jax.sharding import Mesh
from jax.sharding import PartitionSpec as P


HD = 128
PLEN = 64
EPS = 1e-06
ST = ("st_0", "st_1", "st_2")
ST_TP = ("st_0", "st_1", "st_2", "tp")
MIB = 1024 * 1024


def params(mib):
    return pltpu.CompilerParams(
        dimension_semantics=("arbitrary",), vmem_limit_bytes=mib * MIB
    )


def in_hbm(value):
    return pltpu.with_memory_space_constraint(value, pltpu.HBM)


def dot_nn(a, b):
    return lax.dot_general(a, b, (((1,), (0,)), ((), ())), preferred_element_type=jnp.float32)


def dot_nt(a, b):
    return lax.dot_general(a, b, (((1,), (1,)), ((), ())), preferred_element_type=jnp.float32)


def dot_tn(a, b):
    return lax.dot_general(a, b, (((0,), (0,)), ((), ())), preferred_element_type=jnp.float32)


def normed_rows(x, gain):
    inverse = lax.rsqrt(jnp.mean(x * x, axis=-1, keepdims=True) + EPS)
    return (x * inverse * gain).astype(jnp.bfloat16)


def tables_kernel(store_ref, gain_ref, wk_hbm, wv_hbm, table_ref, wk_ref, wv_ref, sems):
    first = pl.program_id(0) == 0
    width = wk_ref.shape[1]
    keys_in = pltpu.make_async_copy(wk_hbm, wk_ref, sems.at[0])
    values_in = pltpu.make_async_copy(wv_hbm, wv_ref, sems.at[1])

    @pl.when(first)
    def _():
        keys_in.start()
        values_in.start()

    normed = normed_rows(store_ref[...].astype(jnp.float32), gain_ref[...])

    @pl.when(first)
    def _():
        keys_in.wait()
        values_in.wait()

    table_ref[:, :width] = dot_nn(normed, wk_ref[...]).astype(jnp.bfloat16)
    table_ref[:, width:] = dot_nn(normed, wv_ref[...]).astype(jnp.bfloat16)


def key_value_tables(store, gain, w_key, w_value):
    rows, model = store.shape
    width = w_key.shape[1]
    step = 256
    return pl.pallas_call(
        tables_kernel,
        grid=(rows // step,),
        in_specs=[
            pl.BlockSpec((step, model), lambda i: (i, 0)),
            pl.BlockSpec((1, model), lambda i: (0, 0)),
            pl.BlockSpec(memory_space=pltpu.HBM),
            pl.BlockSpec(memory_space=pltpu.HBM),
        ],
        out_specs=pl.BlockSpec((step, 2 * width), lambda i: (i, 0)),
        out_shape=jax.ShapeDtypeStruct((rows, 2 * width), jnp.bfloat16),
        scratch_shapes=[
            pltpu.VMEM((model, width), jnp.bfloat16),
            pltpu.VMEM((model, width), jnp.bfloat16),
            pltpu.SemaphoreType.DMA((2,)),
        ],
        compiler_params=params(16),
        cost_estimate=pl.CostEstimate(
            flops=4 * rows * model * width, bytes_accessed=2 * rows * model, transcendentals=rows
        ),
        name="tables",
    )(in_hbm(store), in_hbm(gain), in_hbm(w_key), in_hbm(w_value))


def turned_kernel(store_ref, gain_ref, out_ref):
    normed = normed_rows(store_ref[...].astype(jnp.float32), gain_ref[...])
    out_ref[...] = normed.T


def turned_normed(store, gain):
    rows, model = store.shape
    step = 256
    return pl.pallas_call(
        turned_kernel,
        grid=(rows // step,),
        in_specs=[
            pl.BlockSpec((step, model), lambda i: (i, 0)),
            pl.BlockSpec((1, model), lambda i: (0, 0)),
        ],
        out_specs=pl.BlockSpec((model, step), lambda i: (0, i)),
        out_shape=pltpu.HBM((model, rows), jnp.bfloat16),
        compiler_params=params(16),
        cost_estimate=pl.CostEstimate(
            flops=16 * rows * model, bytes_accessed=4 * rows * model, transcendentals=rows
        ),
        name="turned_normed",
    )(in_hbm(store), in_hbm(gain))


def gather_kernel(asked_ref, table_ref, out_hbm, sems):
    copies = []
    for i in range(out_hbm.shape[0]):
        asked = jnp.maximum(asked_ref[i], 0)
        copies.append(pltpu.make_async_copy(table_ref.at[asked], out_hbm.at[i], sems.at[i]))
        copies[-1].start()
    for copy in copies:
        copy.wait()


def picked_passages(asked, table):
    _, length, width = table.shape
    slots = asked.shape[0]
    return pl.pallas_call(
        gather_kernel,
        in_specs=[
            pl.BlockSpec(memory_space=pltpu.SMEM),
            pl.BlockSpec(memory_space=pltpu.VMEM),
        ],
        out_specs=pl.BlockSpec(memory_space=pltpu.HBM),
        out_shape=pltpu.HBM((slots, length, width), jnp.bfloat16),
        scratch_shapes=[pltpu.SemaphoreType.DMA((slots,))],
        compiler_params=pltpu.CompilerParams(vmem_limit_bytes=8 * MIB),
        name="picked",
    )(asked, table)


def slot_copies(owner_ref, scratch, out_hbm, sems, at, parity):
    per_block = owner_ref.shape[0]
    each = scratch.shape[1] // per_block
    return [
        pltpu.make_async_copy(
            scratch.at[parity, b * per_block + j],
            out_hbm.at[owner_ref[j, at * each + b]],
            sems.at[parity, b * per_block + j],
        )
        for b in range(each)
        for j in range(per_block)
    ]


def wait_slots(owner_ref, scratch, out_hbm, sems):
    step = pl.program_id(0)

    @pl.when(step >= 2)
    def _():
        for copy in slot_copies(owner_ref, scratch, out_hbm, sems, step - 2, lax.rem(step, 2)):
            copy.wait()


def send_slots(owner_ref, scratch, out_hbm, sems):
    step, steps = pl.program_id(0), pl.num_programs(0)
    slot = lax.rem(step, 2)
    for copy in slot_copies(owner_ref, scratch, out_hbm, sems, step, slot):
        copy.start()

    @pl.when(step == steps - 1)
    def _():
        for copy in slot_copies(owner_ref, scratch, out_hbm, sems, step - 1, 1 - slot):
            copy.wait()
        for copy in slot_copies(owner_ref, scratch, out_hbm, sems, step, slot):
            copy.wait()


def block_units(owner_ref, q_ref, g_ref, c_ref, pieces):
    width = q_ref.shape[1]
    per_block = owner_ref.shape[0]
    each = len(pieces) // per_block
    length = q_ref.shape[0] // each
    gate = jax.nn.sigmoid(g_ref[...].astype(jnp.float32))
    grad_in = (gate * c_ref[...].astype(jnp.float32)).astype(jnp.bfloat16)
    units = []
    for b in range(each):
        for h in range(width // HD):
            rows = slice(b * length, (b + 1) * length)
            cols = slice(h * HD, (h + 1) * HD)
            own = pieces[b * per_block : (b + 1) * per_block]
            keys = jnp.concatenate([p[0, :, cols] for p in own], axis=0)
            units.append((b, rows, cols, own, q_ref[rows, cols], grad_in[rows, cols], keys))
    scores = [dot_nt(u[4], u[6]) * HD ** (-0.5) for u in units]
    weights = [jnp.exp(x - jnp.max(x, axis=-1, keepdims=True)) for x in scores]
    weights = [x / jnp.sum(x, axis=-1, keepdims=True) for x in weights]
    return units, weights


def value_slots_kernel(owner_ref, q_ref, g_ref, c_ref, *refs):
    pieces, (out_hbm, scratch, sems) = refs[:-3], refs[-3:]
    per_block = owner_ref.shape[0]
    slot = lax.rem(pl.program_id(0), 2)
    units, weights = block_units(owner_ref, q_ref, g_ref, c_ref, pieces)
    wait_slots(owner_ref, scratch, out_hbm, sems)
    for (b, _, cols, _, _, gin, _), weight in zip(units, weights):
        grad_values = dot_tn(weight.astype(jnp.bfloat16), gin).astype(jnp.bfloat16)
        for j in range(per_block):
            part = slice(j * PLEN, (j + 1) * PLEN)
            scratch[slot, b * per_block + j, :, cols] = grad_values[part]
    send_slots(owner_ref, scratch, out_hbm, sems)


def key_slots_kernel(owner_ref, q_ref, g_ref, c_ref, *refs):
    pieces, (gq_ref, out_hbm, scratch, sems) = refs[:-4], refs[-4:]
    per_block = owner_ref.shape[0]
    width = q_ref.shape[1]
    slot = lax.rem(pl.program_id(0), 2)
    units, weights = block_units(owner_ref, q_ref, g_ref, c_ref, pieces)
    grad_weights = []
    for _, _, cols, own, _, gin, _ in units:
        vcols = slice(width + cols.start, width + cols.stop)
        values = jnp.concatenate([p[0, :, vcols] for p in own], axis=0)
        grad_weights.append(dot_nt(gin, values))
    delta = [
        jnp.sum(w.astype(jnp.bfloat16).astype(jnp.float32) * g, axis=-1, keepdims=True)
        for w, g in zip(weights, grad_weights)
    ]
    halves = [(w * (g - d)).astype(jnp.bfloat16) for w, g, d in zip(weights, grad_weights, delta)]
    wait_slots(owner_ref, scratch, out_hbm, sems)
    for (b, rows, cols, _, q, _, keys), half in zip(units, halves):
        gq_ref[rows, cols] = dot_nn(half, keys) * HD ** (-0.5)
        grad_keys = (dot_tn(half, q) * HD ** (-0.5)).astype(jnp.bfloat16)
        for j in range(per_block):
            part = slice(j * PLEN, (j + 1) * PLEN)
            scratch[slot, b * per_block + j, :, cols] = grad_keys[part]
    send_slots(owner_ref, scratch, out_hbm, sems)


def attention(owner_turned, queries, gate_pre, cotangent, got, keys_only):
    rows, width = queries.shape
    per_block, blocks = owner_turned.shape
    slots, length, both = got.shape
    each = 2
    steps = blocks // each
    tokens = pl.BlockSpec((rows // steps, width), lambda i, o: (i, 0))
    read = width if keys_only else both

    def piece(b, j):
        return pl.BlockSpec((1, length, read), lambda i, o: (o[j, i * each + b], 0, 0))

    pieces = [piece(b, j) for b in range(each) for j in range(per_block)]
    keys = PLEN * per_block
    out = pltpu.HBM((slots, length, width), jnp.bfloat16)
    hbm = pl.BlockSpec(memory_space=pltpu.HBM)
    return pl.pallas_call(
        value_slots_kernel if keys_only else key_slots_kernel,
        grid_spec=pltpu.PrefetchScalarGridSpec(
            num_scalar_prefetch=1,
            grid=(steps,),
            in_specs=[tokens, tokens, tokens] + pieces,
            out_specs=[hbm] if keys_only else [tokens, hbm],
            scratch_shapes=[
                pltpu.VMEM((2, len(pieces), length, width), jnp.bfloat16),
                pltpu.SemaphoreType.DMA((2, len(pieces))),
            ],
        ),
        out_shape=[out] if keys_only else [jax.ShapeDtypeStruct((rows, width), jnp.float32), out],
        compiler_params=params(20),
        cost_estimate=pl.CostEstimate(
            flops=(4 if keys_only else 8) * rows * width * keys,
            bytes_accessed=10 * rows * width + 2 * got.size,
            transcendentals=rows * width * keys // HD,
        ),
        name="value_slots" if keys_only else "key_slots",
    )(
        owner_turned,
        in_hbm(queries),
        in_hbm(gate_pre),
        in_hbm(cotangent),
        *([in_hbm(got)] * len(pieces)),
    )


def add_asked(asked_ref, back_ref, total):
    step = pl.program_id(0)
    each = back_ref.shape[0]

    @pl.when(step == 0)
    def _():
        total[...] = jnp.zeros_like(total)

    for i in range(each):
        asked = asked_ref[step * each + i]

        @pl.when(asked >= 0)
        def _():
            total[asked] += back_ref[i].astype(jnp.float32)


def write_quarters(place_ref, total, parts):
    passages, length, _ = total.shape
    share = passages // 4
    for turn, out in enumerate(parts):
        first = lax.rem(place_ref[0] + turn, 4) * share
        for p in range(share):
            out[p * length : (p + 1) * length, :] = total[first + p].astype(jnp.bfloat16)


def value_kernel(asked_ref, place_ref, back_ref, turned_hbm, *refs):
    parts, (mine_ref, other_ref, total, terms, turned_ref, sem) = refs[:4], refs[4:]
    turned_in = pltpu.make_async_copy(turned_hbm, turned_ref, sem)

    @pl.when(pl.program_id(0) == 0)
    def _():
        turned_in.start()

    add_asked(asked_ref, back_ref, total)

    @pl.when(pl.program_id(0) == pl.num_programs(0) - 1)
    def _():
        write_quarters(place_ref, total, parts)
        passages, length, width = total.shape
        values = total[...].astype(jnp.bfloat16).reshape(passages * length, width)
        pieces, piece, _ = terms.shape
        turned_in.wait()
        made = dot_nn(turned_ref[...], values).astype(jnp.bfloat16)
        for p in range(pieces):
            terms[p] = made[p * piece : (p + 1) * piece]
        for p in range(pieces // 2):
            turn = p % 8 * 8 + p // 8 * 2
            mine_ref[p] = terms[place_ref[1] ^ turn]
            other_ref[p] = terms[place_ref[1] ^ (turn + 1)]


def value_sums(asked, place, back, turned, passages, devices):
    slots, length, width = back.shape
    model, rows = turned.shape
    each = 16
    quarter = jax.ShapeDtypeStruct((rows // 4, width), jnp.bfloat16)
    half = jax.ShapeDtypeStruct((devices // 2, model // devices, width), jnp.bfloat16)
    return pl.pallas_call(
        value_kernel,
        grid_spec=pltpu.PrefetchScalarGridSpec(
            num_scalar_prefetch=2,
            grid=(slots // each,),
            in_specs=[
                pl.BlockSpec((each, length, width), lambda i, a, t: (i, 0, 0)),
                pl.BlockSpec(memory_space=pltpu.HBM),
            ],
            out_specs=[pl.BlockSpec(quarter.shape, lambda i, a, t: (0, 0))] * 4
            + [pl.BlockSpec(half.shape, lambda i, a, t: (0, 0, 0))] * 2,
            scratch_shapes=[
                pltpu.VMEM((passages, length, width), jnp.float32),
                pltpu.VMEM((devices, model // devices, width), jnp.bfloat16),
                pltpu.VMEM((model, rows), jnp.bfloat16),
                pltpu.SemaphoreType.DMA,
            ],
        ),
        out_shape=[quarter] * 4 + [half] * 2,
        compiler_params=params(24),
        cost_estimate=pl.CostEstimate(
            flops=2 * model * rows * width, bytes_accessed=2 * model * rows, transcendentals=0
        ),
        name="value_sums",
    )(asked, place, back, in_hbm(turned))


def key_kernel(asked_ref, place_ref, back_ref, *refs):
    parts, total = refs[:4], refs[4]
    add_asked(asked_ref, back_ref, total)

    @pl.when(pl.program_id(0) == pl.num_programs(0) - 1)
    def _():
        write_quarters(place_ref, total, parts)


def key_sums(asked, place, back, passages):
    slots, length, width = back.shape
    each = 16
    quarter = jax.ShapeDtypeStruct((passages * length // 4, width), jnp.bfloat16)
    return pl.pallas_call(
        key_kernel,
        grid_spec=pltpu.PrefetchScalarGridSpec(
            num_scalar_prefetch=2,
            grid=(slots // each,),
            in_specs=[pl.BlockSpec((each, length, width), lambda i, a, t: (i, 0, 0))],
            out_specs=[pl.BlockSpec(quarter.shape, lambda i, a, t: (0, 0))] * 4,
            scratch_shapes=[pltpu.VMEM((passages, length, width), jnp.float32)],
        ),
        out_shape=[quarter] * 4,
        compiler_params=params(12),
        cost_estimate=pl.CostEstimate(
            flops=4 * back.size, bytes_accessed=2 * back.size, transcendentals=0
        ),
        name="key_sums",
    )(asked, place, back)


def near_kernel(*refs):
    count = 4
    parts, weights, out_ref = refs[:count], refs[count : 2 * count], refs[2 * count]
    held, sems = refs[2 * count + 1 : -1], refs[-1]
    width = parts[0].shape[1]
    arrivals = [
        pltpu.make_async_copy(w.at[:, width:], h, sems.at[i])
        for i, (w, h) in enumerate(zip(weights, held))
    ]
    for copy in arrivals:
        copy.start()
    made = []
    for part, arrival, h in zip(parts, arrivals, held):
        arrival.wait()
        made.append(dot_nt(part[...], h[...]))
    out_ref[...] = sum(made)


def near_products(parts, weights):
    quarter, width = parts[0].shape
    model = weights[0].shape[0]
    count = len(parts)
    vmem = pl.BlockSpec(memory_space=pltpu.VMEM)
    hbm = pl.BlockSpec(memory_space=pltpu.HBM)
    return pl.pallas_call(
        near_kernel,
        in_specs=[vmem] * count + [hbm] * count,
        out_specs=vmem,
        out_shape=jax.ShapeDtypeStruct((quarter, model), jnp.float32),
        scratch_shapes=[pltpu.VMEM((model, width), jnp.bfloat16)] * count
        + [pltpu.SemaphoreType.DMA((count,))],
        compiler_params=pltpu.CompilerParams(vmem_limit_bytes=16 * MIB),
        cost_estimate=pl.CostEstimate(
            flops=2 * count * quarter * model * width,
            bytes_accessed=2 * count * model * width,
            transcendentals=0,
        ),
        name="near_products",
    )(*parts, *[in_hbm(w) for w in weights])


def own_kernel(place_ref, part_ref, near_ref, *refs):
    count = 4
    weights, store_hbm = refs[:count], refs[count]
    out_ref, rows_ref, *keys_refs = refs[count + 1 : 2 * count + 2]
    held, sems = refs[2 * count + 2], refs[-1]
    quarter, width = part_ref.shape
    first = pl.multiple_of(place_ref[0] * quarter, quarter)
    copies = [
        pltpu.make_async_copy(w.at[:, :width], k, sems.at[i])
        for i, (w, k) in enumerate(zip(weights, [held] + keys_refs))
    ]
    copies.append(
        pltpu.make_async_copy(store_hbm.at[pl.ds(first, quarter)], rows_ref, sems.at[count])
    )
    for copy in copies:
        copy.start()
    copies[0].wait()
    out_ref[...] = near_ref[...] + dot_nt(part_ref[...], held[...])
    for copy in copies[1:]:
        copy.wait()


def own_product(place, part, near, weights, store):
    quarter, width = part.shape
    model = weights[0].shape[0]
    count = len(weights)
    vmem = pl.BlockSpec(memory_space=pltpu.VMEM)
    hbm = pl.BlockSpec(memory_space=pltpu.HBM)
    return pl.pallas_call(
        own_kernel,
        in_specs=[pl.BlockSpec(memory_space=pltpu.SMEM), vmem, vmem] + [hbm] * (count + 1),
        out_specs=[vmem] * (count + 1),
        out_shape=[
            pltpu.VMEM((quarter, model), jnp.float32),
            pltpu.VMEM((quarter, model), jnp.bfloat16),
        ]
        + [pltpu.VMEM((model, width), jnp.bfloat16)] * (count - 1),
        scratch_shapes=[
            pltpu.VMEM((model, width), jnp.bfloat16),
            pltpu.SemaphoreType.DMA((count + 1,)),
        ],
        compiler_params=pltpu.CompilerParams(vmem_limit_bytes=16 * MIB),
        cost_estimate=pl.CostEstimate(
            flops=2 * quarter * model * width,
            bytes_accessed=4 * count * model * width,
            transcendentals=0,
        ),
        name="own_product",
    )(place, part, near, *[in_hbm(w) for w in weights], in_hbm(store))


def final_kernel(rows_ref, gain_ref, near_ref, *refs):
    parts, weights, (out_hbm, out_ref, sems) = refs[:3], refs[3:6], refs[6:]
    made = near_ref[...]
    for part, weight in zip(parts, weights):
        made += dot_nt(part[...], weight[...])
    step = 64
    sent = []
    for i in range(out_ref.shape[0] // step):
        at = slice(i * step, (i + 1) * step)
        rows = rows_ref[at].astype(jnp.float32)
        inverse = lax.rsqrt(jnp.mean(rows * rows, axis=-1, keepdims=True) + EPS)
        unit = rows * inverse
        grad_unit = made[at] * gain_ref[...]
        mean = jnp.mean(grad_unit * unit, axis=-1, keepdims=True)
        out_ref[at] = inverse * (grad_unit - unit * mean)
        sent.append(pltpu.make_async_copy(out_ref.at[at], out_hbm.at[at], sems.at[i]))
        sent[-1].start()
    for copy in sent:
        copy.wait()


def store_gradient(rows, gain, near, parts, weights):
    quarter, model = rows.shape
    width = parts[0].shape[1]
    vmem = pl.BlockSpec(memory_space=pltpu.VMEM)
    return pl.pallas_call(
        final_kernel,
        in_specs=[vmem] * (3 + 2 * len(parts)),
        out_specs=pl.BlockSpec(memory_space=pltpu.HBM),
        out_shape=jax.ShapeDtypeStruct((quarter, model), jnp.float32),
        scratch_shapes=[
            pltpu.VMEM((quarter, model), jnp.float32),
            pltpu.SemaphoreType.DMA((quarter // 64,)),
        ],
        compiler_params=pltpu.CompilerParams(vmem_limit_bytes=16 * MIB),
        cost_estimate=pl.CostEstimate(
            flops=6 * quarter * model * width,
            bytes_accessed=4 * quarter * model,
            transcendentals=quarter,
        ),
        name="store_gradient",
    )(rows, gain, near, *parts, *weights)


def shifted(value, turn):
    return lax.ppermute(value, "tp", [(i, (i + turn) % 4) for i in range(4)])


def halved(value, axis, distance, kind):
    size = lax.axis_size(axis)
    half = value.shape[0] // 2
    pairs = [(i, i ^ distance) for i in range(size)]
    came = lax.ppermute(value[half:].astype(kind), axis, pairs)
    return value[:half] + came.astype(jnp.float32)


def local(queries, gate_pre, cotangent, store, store_gain, w_key, w_value, owners, slots):
    st_size = lax.axis_size(ST)
    width = queries.shape[1]
    rows_dev, model = store.shape
    passages = rows_dev // PLEN
    place = jnp.stack([lax.axis_index("tp"), lax.axis_index(ST)]).astype(jnp.int32)
    gain = store_gain.reshape(1, model)

    owner_turned = owners.T
    hits = owner_turned[None] == jnp.arange(st_size, dtype=jnp.int32)[:, None, None]
    requests = jnp.where(hits, slots.T[None], -1)
    asked = lax.all_to_all(requests, ST, split_axis=0, concat_axis=0, tiled=True)
    asked = jnp.max(asked, axis=(1, 2))

    table = key_value_tables(store, gain, w_key, w_value)
    picked = picked_passages(asked, table.reshape(passages, PLEN, 2 * width))
    got = lax.all_to_all(picked, ST, split_axis=0, concat_axis=0, tiled=True)

    late_key, late_value, _ = lax.optimization_barrier((w_key, w_value, picked))
    both = jnp.concatenate([late_key, late_value], axis=1)
    weights = [both] + [shifted(both, turn) for turn in (1, 3, 2)]
    got, *came = lax.optimization_barrier((got, *weights[1:]))
    weights = [both] + came

    (outgoing,) = attention(owner_turned, queries, gate_pre, cotangent, got, True)
    back_values = lax.all_to_all(outgoing, ST, split_axis=0, concat_axis=0, tiled=True)
    late_store, late_got, _ = lax.optimization_barrier((store, got, outgoing))
    grad_queries, outgoing = attention(
        owner_turned, queries, gate_pre, cotangent, late_got, False
    )
    turned = turned_normed(late_store, gain)
    outgoing, turned = lax.optimization_barrier((outgoing, turned))
    back_keys = lax.all_to_all(outgoing, ST, split_axis=0, concat_axis=0, tiled=True)
    back_values, turned, _ = lax.optimization_barrier((back_values, turned, grad_queries))

    own, first, second, third, mine, other = value_sums(
        asked, place, back_values, turned, passages, st_size
    )
    parts = [own, shifted(first, 1), shifted(third, 3), shifted(second, 2)]
    near = near_products(parts, weights)
    came = lax.ppermute(other, "st_2", [(0, 1), (1, 0)])
    terms = mine.astype(jnp.float32) + came.astype(jnp.float32)
    terms = halved(terms, "st_1", 2, jnp.bfloat16)
    terms = halved(terms, "st_1", 1, jnp.bfloat16)
    back_keys, near = lax.optimization_barrier((back_keys, near))
    terms = halved(terms, "st_0", 4, jnp.float32)

    own, first, second, third = key_sums(asked, place, back_keys, passages)
    own, first, second, third, terms = lax.optimization_barrier(
        (own, first, second, third, terms)
    )
    parts = []
    for part, turn in ((first, 1), (third, 3), (second, 2)):
        parts.append(shifted(part, turn))
    near, own_rows, *key_weights = own_product(place, own, near, weights, store)
    terms = halved(terms, "st_0", 2, jnp.float32)
    terms = halved(terms, "st_0", 1, jnp.float32)
    grad_w_value = terms.reshape(terms.shape[1:])
    grad_store = store_gradient(own_rows, gain, near, parts, key_weights)
    return (grad_queries, grad_store, grad_w_value)


def solution(mesh):
    torus = Mesh(mesh.devices.reshape(8, 4, 2, mesh.shape["tp"]), ("st_0", "st_1", "st_2", "tp"))
    return jax.shard_map(
        local,
        mesh=torus,
        in_specs=(
            P(ST, "tp"),
            P(ST, "tp"),
            P(ST, "tp"),
            P(ST, None),
            P(),
            P(None, "tp"),
            P(None, "tp"),
            P(ST, None),
            P(ST, None),
        ),
        out_specs=(P(ST, "tp"), P(ST_TP, None), P(ST, "tp")),
        check_vma=False,
    )
```

```python
import jax
import jax.numpy as jnp
from jax import lax
from jax.experimental import pallas as pl
from jax.experimental.pallas import tpu as pltpu
from jax.sharding import Mesh
from jax.sharding import PartitionSpec as P


HD = 128
PLEN = 64
EPS = 1e-06
ST = ("st_0", "st_1", "st_2")
ST_TP = ("st_0", "st_1", "st_2", "tp")
MIB = 1024 * 1024


def params(mib):
    return pltpu.CompilerParams(
        dimension_semantics=("arbitrary",), vmem_limit_bytes=mib * MIB
    )


def in_hbm(value):
    return pltpu.with_memory_space_constraint(value, pltpu.HBM)


def dot_nn(a, b):
    return lax.dot_general(a, b, (((1,), (0,)), ((), ())), preferred_element_type=jnp.float32)


def dot_nt(a, b):
    return lax.dot_general(a, b, (((1,), (1,)), ((), ())), preferred_element_type=jnp.float32)


def dot_tn(a, b):
    return lax.dot_general(a, b, (((0,), (0,)), ((), ())), preferred_element_type=jnp.float32)


def normed_rows(x, gain):
    inverse = lax.rsqrt(jnp.mean(x * x, axis=-1, keepdims=True) + EPS)
    return (x * inverse * gain).astype(jnp.bfloat16)


def tables_kernel(store_ref, gain_ref, wk_hbm, wv_hbm, table_ref, both_hbm, wk_ref, wv_ref, sems):
    first = pl.program_id(0) == 0
    last = pl.program_id(0) == pl.num_programs(0) - 1
    width = wk_ref.shape[1]
    keys_out = pltpu.make_async_copy(wk_ref, both_hbm.at[:, :width], sems.at[2])
    values_out = pltpu.make_async_copy(wv_ref, both_hbm.at[:, width:], sems.at[3])
    keys_in = pltpu.make_async_copy(wk_hbm, wk_ref, sems.at[0])
    values_in = pltpu.make_async_copy(wv_hbm, wv_ref, sems.at[1])

    @pl.when(first)
    def _():
        keys_in.start()
        values_in.start()

    normed = normed_rows(store_ref[...].astype(jnp.float32), gain_ref[...])

    @pl.when(first)
    def _():
        keys_in.wait()
        values_in.wait()
        keys_out.start()
        values_out.start()

    table_ref[:, :width] = dot_nn(normed, wk_ref[...]).astype(jnp.bfloat16)
    table_ref[:, width:] = dot_nn(normed, wv_ref[...]).astype(jnp.bfloat16)

    @pl.when(last)
    def _():
        keys_out.wait()
        values_out.wait()


def key_value_tables(store, gain, w_key, w_value):
    rows, model = store.shape
    width = w_key.shape[1]
    step = 256
    return pl.pallas_call(
        tables_kernel,
        grid=(rows // step,),
        in_specs=[
            pl.BlockSpec((step, model), lambda i: (i, 0)),
            pl.BlockSpec((1, model), lambda i: (0, 0)),
            pl.BlockSpec(memory_space=pltpu.HBM),
            pl.BlockSpec(memory_space=pltpu.HBM),
        ],
        out_specs=[
            pl.BlockSpec((step, 2 * width), lambda i: (i, 0)),
            pl.BlockSpec(memory_space=pltpu.HBM),
        ],
        out_shape=[
            jax.ShapeDtypeStruct((rows, 2 * width), jnp.bfloat16),
            pltpu.HBM((model, 2 * width), jnp.bfloat16),
        ],
        scratch_shapes=[
            pltpu.VMEM((model, width), jnp.bfloat16),
            pltpu.VMEM((model, width), jnp.bfloat16),
            pltpu.SemaphoreType.DMA((4,)),
        ],
        compiler_params=params(16),
        cost_estimate=pl.CostEstimate(
            flops=4 * rows * model * width, bytes_accessed=2 * rows * model, transcendentals=rows
        ),
        name="tables",
    )(in_hbm(store), in_hbm(gain), in_hbm(w_key), in_hbm(w_value))


def turned_kernel(store_ref, gain_ref, out_ref):
    normed = normed_rows(store_ref[...].astype(jnp.float32), gain_ref[...])
    out_ref[...] = normed.T


def turned_normed(store, gain):
    rows, model = store.shape
    step = 256
    return pl.pallas_call(
        turned_kernel,
        grid=(rows // step,),
        in_specs=[
            pl.BlockSpec((step, model), lambda i: (i, 0)),
            pl.BlockSpec((1, model), lambda i: (0, 0)),
        ],
        out_specs=pl.BlockSpec((model, step), lambda i: (0, i)),
        out_shape=pltpu.HBM((model, rows), jnp.bfloat16),
        compiler_params=params(16),
        cost_estimate=pl.CostEstimate(
            flops=16 * rows * model, bytes_accessed=4 * rows * model, transcendentals=rows
        ),
        name="turned_normed",
    )(in_hbm(store), in_hbm(gain))


def gather_kernel(asked_ref, table_ref, out_hbm, sems):
    copies = []
    for i in range(out_hbm.shape[0]):
        asked = jnp.maximum(asked_ref[i], 0)
        copies.append(pltpu.make_async_copy(table_ref.at[asked], out_hbm.at[i], sems.at[i]))
        copies[-1].start()
    for copy in copies:
        copy.wait()


def picked_passages(asked, table):
    _, length, width = table.shape
    slots = asked.shape[0]
    return pl.pallas_call(
        gather_kernel,
        in_specs=[
            pl.BlockSpec(memory_space=pltpu.SMEM),
            pl.BlockSpec(memory_space=pltpu.VMEM),
        ],
        out_specs=pl.BlockSpec(memory_space=pltpu.HBM),
        out_shape=pltpu.HBM((slots, length, width), jnp.bfloat16),
        scratch_shapes=[pltpu.SemaphoreType.DMA((slots,))],
        compiler_params=pltpu.CompilerParams(vmem_limit_bytes=8 * MIB),
        name="picked",
    )(asked, table)


def slot_copies(owner_ref, scratch, out_hbm, sems, at, parity):
    per_block = owner_ref.shape[0]
    each = scratch.shape[1] // per_block
    return [
        pltpu.make_async_copy(
            scratch.at[parity, b * per_block + j],
            out_hbm.at[owner_ref[j, at * each + b]],
            sems.at[parity, b * per_block + j],
        )
        for b in range(each)
        for j in range(per_block)
    ]


def wait_slots(owner_ref, scratch, out_hbm, sems):
    step = pl.program_id(0)

    @pl.when(step >= 2)
    def _():
        for copy in slot_copies(owner_ref, scratch, out_hbm, sems, step - 2, lax.rem(step, 2)):
            copy.wait()


def send_slots(owner_ref, scratch, out_hbm, sems):
    step, steps = pl.program_id(0), pl.num_programs(0)
    slot = lax.rem(step, 2)
    for copy in slot_copies(owner_ref, scratch, out_hbm, sems, step, slot):
        copy.start()

    @pl.when(step == steps - 1)
    def _():
        for copy in slot_copies(owner_ref, scratch, out_hbm, sems, step - 1, 1 - slot):
            copy.wait()
        for copy in slot_copies(owner_ref, scratch, out_hbm, sems, step, slot):
            copy.wait()


def block_units(owner_ref, q_ref, g_ref, c_ref, pieces):
    width = q_ref.shape[1]
    per_block = owner_ref.shape[0]
    each = len(pieces) // per_block
    length = q_ref.shape[0] // each
    gate = jax.nn.sigmoid(g_ref[...].astype(jnp.float32))
    grad_in = (gate * c_ref[...].astype(jnp.float32)).astype(jnp.bfloat16)
    units = []
    for b in range(each):
        for h in range(width // HD):
            rows = slice(b * length, (b + 1) * length)
            cols = slice(h * HD, (h + 1) * HD)
            own = pieces[b * per_block : (b + 1) * per_block]
            keys = jnp.concatenate([p[0, :, cols] for p in own], axis=0)
            units.append((b, rows, cols, own, q_ref[rows, cols], grad_in[rows, cols], keys))
    scores = [dot_nt(u[6], u[4]) * HD ** (-0.5) for u in units]
    weights = [jnp.exp(x - jnp.max(x, axis=0, keepdims=True)) for x in scores]
    weights = [x * (1.0 / jnp.sum(x, axis=0, keepdims=True)) for x in weights]
    return units, weights


def value_slots_kernel(owner_ref, q_ref, g_ref, c_ref, *refs):
    pieces, (out_hbm, scratch, sems) = refs[:-3], refs[-3:]
    per_block = owner_ref.shape[0]
    slot = lax.rem(pl.program_id(0), 2)
    units, weights = block_units(owner_ref, q_ref, g_ref, c_ref, pieces)
    wait_slots(owner_ref, scratch, out_hbm, sems)
    for (b, _, cols, _, _, gin, _), weight in zip(units, weights):
        grad_values = dot_nn(weight.astype(jnp.bfloat16), gin).astype(jnp.bfloat16)
        for j in range(per_block):
            part = slice(j * PLEN, (j + 1) * PLEN)
            scratch[slot, b * per_block + j, :, cols] = grad_values[part]
    send_slots(owner_ref, scratch, out_hbm, sems)


def key_slots_kernel(owner_ref, q_ref, g_ref, c_ref, *refs):
    pieces, (gq_ref, out_hbm, scratch, sems) = refs[:-4], refs[-4:]
    per_block = owner_ref.shape[0]
    width = q_ref.shape[1]
    slot = lax.rem(pl.program_id(0), 2)
    units, weights = block_units(owner_ref, q_ref, g_ref, c_ref, pieces)
    grad_weights = []
    for _, _, cols, own, _, gin, _ in units:
        vcols = slice(width + cols.start, width + cols.stop)
        values = jnp.concatenate([p[0, :, vcols] for p in own], axis=0)
        grad_weights.append(dot_nt(values, gin))
    delta = [
        jnp.sum(w.astype(jnp.bfloat16).astype(jnp.float32) * g, axis=0, keepdims=True)
        for w, g in zip(weights, grad_weights)
    ]
    halves = [(w * (g - d)).astype(jnp.bfloat16) for w, g, d in zip(weights, grad_weights, delta)]
    wait_slots(owner_ref, scratch, out_hbm, sems)
    for (b, rows, cols, _, q, _, keys), half in zip(units, halves):
        gq_ref[rows, cols] = dot_tn(half, keys) * HD ** (-0.5)
        grad_keys = (dot_nn(half, q) * HD ** (-0.5)).astype(jnp.bfloat16)
        for j in range(per_block):
            part = slice(j * PLEN, (j + 1) * PLEN)
            scratch[slot, b * per_block + j, :, cols] = grad_keys[part]
    send_slots(owner_ref, scratch, out_hbm, sems)


def attention(owner_turned, queries, gate_pre, cotangent, got, keys_only):
    rows, width = queries.shape
    per_block, blocks = owner_turned.shape
    slots, length, both = got.shape
    each = 2
    steps = blocks // each
    tokens = pl.BlockSpec((rows // steps, width), lambda i, o: (i, 0))
    read = width if keys_only else both

    def piece(b, j):
        return pl.BlockSpec((1, length, read), lambda i, o: (o[j, i * each + b], 0, 0))

    pieces = [piece(b, j) for b in range(each) for j in range(per_block)]
    keys = PLEN * per_block
    out = pltpu.HBM((slots, length, width), jnp.bfloat16)
    hbm = pl.BlockSpec(memory_space=pltpu.HBM)
    return pl.pallas_call(
        value_slots_kernel if keys_only else key_slots_kernel,
        grid_spec=pltpu.PrefetchScalarGridSpec(
            num_scalar_prefetch=1,
            grid=(steps,),
            in_specs=[tokens, tokens, tokens] + pieces,
            out_specs=[hbm] if keys_only else [tokens, hbm],
            scratch_shapes=[
                pltpu.VMEM((2, len(pieces), length, width), jnp.bfloat16),
                pltpu.SemaphoreType.DMA((2, len(pieces))),
            ],
        ),
        out_shape=[out] if keys_only else [jax.ShapeDtypeStruct((rows, width), jnp.float32), out],
        compiler_params=params(20),
        cost_estimate=pl.CostEstimate(
            flops=(4 if keys_only else 8) * rows * width * keys,
            bytes_accessed=10 * rows * width + 2 * got.size,
            transcendentals=rows * width * keys // HD,
        ),
        name="value_slots" if keys_only else "key_slots",
    )(
        owner_turned,
        in_hbm(queries),
        in_hbm(gate_pre),
        in_hbm(cotangent),
        *([in_hbm(got)] * len(pieces)),
    )


def add_asked(asked_ref, back_ref, total):
    step = pl.program_id(0)
    each = back_ref.shape[0]

    @pl.when(step == 0)
    def _():
        total[...] = jnp.zeros_like(total)

    for i in range(each):
        asked = asked_ref[step * each + i]

        @pl.when(asked >= 0)
        def _():
            total[asked] += back_ref[i].astype(jnp.float32)


def write_quarters(place_ref, total, parts):
    passages, length, _ = total.shape
    share = passages // 4
    for turn, out in enumerate(parts):
        first = lax.rem(place_ref[0] + turn, 4) * share
        for p in range(share):
            out[p * length : (p + 1) * length, :] = total[first + p].astype(jnp.bfloat16)


def value_kernel(asked_ref, place_ref, back_ref, turned_hbm, *refs):
    parts, (mine_ref, other_ref, total, terms, turned_ref, sem) = refs[:4], refs[4:]
    turned_in = pltpu.make_async_copy(turned_hbm, turned_ref, sem)

    @pl.when(pl.program_id(0) == 0)
    def _():
        turned_in.start()

    add_asked(asked_ref, back_ref, total)

    @pl.when(pl.program_id(0) == pl.num_programs(0) - 1)
    def _():
        write_quarters(place_ref, total, parts)
        passages, length, width = total.shape
        values = total[...].astype(jnp.bfloat16).reshape(passages * length, width)
        pieces, piece, _ = terms.shape
        turned_in.wait()
        made = dot_nn(turned_ref[...], values).astype(jnp.bfloat16)
        for p in range(pieces):
            terms[p] = made[p * piece : (p + 1) * piece]
        for p in range(pieces // 2):
            turn = p % 8 * 8 + p // 8 * 2
            mine_ref[p] = terms[place_ref[1] ^ turn]
            other_ref[p] = terms[place_ref[1] ^ (turn + 1)]


def value_sums(asked, place, back, turned, passages, devices):
    slots, length, width = back.shape
    model, rows = turned.shape
    each = 16
    quarter = jax.ShapeDtypeStruct((rows // 4, width), jnp.bfloat16)
    half = jax.ShapeDtypeStruct((devices // 2, model // devices, width), jnp.bfloat16)
    return pl.pallas_call(
        value_kernel,
        grid_spec=pltpu.PrefetchScalarGridSpec(
            num_scalar_prefetch=2,
            grid=(slots // each,),
            in_specs=[
                pl.BlockSpec((each, length, width), lambda i, a, t: (i, 0, 0)),
                pl.BlockSpec(memory_space=pltpu.HBM),
            ],
            out_specs=[pl.BlockSpec(quarter.shape, lambda i, a, t: (0, 0))] * 4
            + [pl.BlockSpec(half.shape, lambda i, a, t: (0, 0, 0))] * 2,
            scratch_shapes=[
                pltpu.VMEM((passages, length, width), jnp.float32),
                pltpu.VMEM((devices, model // devices, width), jnp.bfloat16),
                pltpu.VMEM((model, rows), jnp.bfloat16),
                pltpu.SemaphoreType.DMA,
            ],
        ),
        out_shape=[quarter] * 4 + [half] * 2,
        compiler_params=params(24),
        cost_estimate=pl.CostEstimate(
            flops=2 * model * rows * width, bytes_accessed=2 * model * rows, transcendentals=0
        ),
        name="value_sums",
    )(asked, place, back, in_hbm(turned))


def key_kernel(asked_ref, place_ref, back_ref, *refs):
    parts, total = refs[:4], refs[4]
    total[...] = jnp.zeros_like(total)
    for r in range(back_ref.shape[0]):
        asked = asked_ref[r]

        @pl.when(asked >= 0)
        def _():
            total[asked] += back_ref[r].astype(jnp.float32)

    write_quarters(place_ref, total, parts)


def key_sums(asked, place, back, passages):
    _, length, width = back.shape
    quarter = jax.ShapeDtypeStruct((passages * length // 4, width), jnp.bfloat16)
    smem = pl.BlockSpec(memory_space=pltpu.SMEM)
    vmem = pl.BlockSpec(memory_space=pltpu.VMEM)
    return pl.pallas_call(
        key_kernel,
        in_specs=[smem, smem, vmem],
        out_specs=[vmem] * 4,
        out_shape=[quarter] * 4,
        scratch_shapes=[pltpu.VMEM((passages, length, width), jnp.float32)],
        compiler_params=pltpu.CompilerParams(vmem_limit_bytes=12 * MIB),
        cost_estimate=pl.CostEstimate(
            flops=4 * back.size, bytes_accessed=2 * back.size, transcendentals=0
        ),
        name="key_sums",
    )(asked, place, back)


def near_kernel(*refs):
    count = 4
    parts, weights, out_ref = refs[:count], refs[count : 2 * count], refs[2 * count]
    held, sems = refs[2 * count + 1 : -1], refs[-1]
    width = parts[0].shape[1]
    arrivals = [
        pltpu.make_async_copy(w.at[:, width:], h, sems.at[i])
        for i, (w, h) in enumerate(zip(weights, held))
    ]
    for copy in arrivals:
        copy.start()
    made = []
    for part, arrival, h in zip(parts, arrivals, held):
        arrival.wait()
        made.append(dot_nt(part[...], h[...]))
    out_ref[...] = sum(made)


def near_products(parts, weights):
    quarter, width = parts[0].shape
    model = weights[0].shape[0]
    count = len(parts)
    vmem = pl.BlockSpec(memory_space=pltpu.VMEM)
    hbm = pl.BlockSpec(memory_space=pltpu.HBM)
    return pl.pallas_call(
        near_kernel,
        in_specs=[vmem] * count + [hbm] * count,
        out_specs=vmem,
        out_shape=jax.ShapeDtypeStruct((quarter, model), jnp.float32),
        scratch_shapes=[pltpu.VMEM((model, width), jnp.bfloat16)] * count
        + [pltpu.SemaphoreType.DMA((count,))],
        compiler_params=pltpu.CompilerParams(vmem_limit_bytes=16 * MIB),
        cost_estimate=pl.CostEstimate(
            flops=2 * count * quarter * model * width,
            bytes_accessed=2 * count * model * width,
            transcendentals=0,
        ),
        name="near_products",
    )(*parts, *[in_hbm(w) for w in weights])


def own_kernel(place_ref, part_ref, near_ref, *refs):
    count = 4
    weights, store_hbm = refs[:count], refs[count]
    out_ref, rows_ref, *keys_refs = refs[count + 1 : 2 * count + 2]
    held, sems = refs[2 * count + 2], refs[-1]
    quarter, width = part_ref.shape
    first = pl.multiple_of(place_ref[0] * quarter, quarter)
    copies = [
        pltpu.make_async_copy(w.at[:, :width], k, sems.at[i])
        for i, (w, k) in enumerate(zip(weights, [held] + keys_refs))
    ]
    copies.append(
        pltpu.make_async_copy(store_hbm.at[pl.ds(first, quarter)], rows_ref, sems.at[count])
    )
    for copy in copies:
        copy.start()
    copies[0].wait()
    out_ref[...] = near_ref[...] + dot_nt(part_ref[...], held[...])
    for copy in copies[1:]:
        copy.wait()


def own_product(place, part, near, weights, store):
    quarter, width = part.shape
    model = weights[0].shape[0]
    count = len(weights)
    vmem = pl.BlockSpec(memory_space=pltpu.VMEM)
    hbm = pl.BlockSpec(memory_space=pltpu.HBM)
    return pl.pallas_call(
        own_kernel,
        in_specs=[pl.BlockSpec(memory_space=pltpu.SMEM), vmem, vmem] + [hbm] * (count + 1),
        out_specs=[vmem] * (count + 1),
        out_shape=[
            pltpu.VMEM((quarter, model), jnp.float32),
            pltpu.VMEM((quarter, model), jnp.bfloat16),
        ]
        + [pltpu.VMEM((model, width), jnp.bfloat16)] * (count - 1),
        scratch_shapes=[
            pltpu.VMEM((model, width), jnp.bfloat16),
            pltpu.SemaphoreType.DMA((count + 1,)),
        ],
        compiler_params=pltpu.CompilerParams(vmem_limit_bytes=16 * MIB),
        cost_estimate=pl.CostEstimate(
            flops=2 * quarter * model * width,
            bytes_accessed=4 * count * model * width,
            transcendentals=0,
        ),
        name="own_product",
    )(place, part, near, *[in_hbm(w) for w in weights], in_hbm(store))


def final_kernel(rows_ref, gain_ref, near_ref, *refs):
    parts, weights, (out_hbm, out_ref, sems) = refs[:3], refs[3:6], refs[6:]
    made = near_ref[...]
    for part, weight in zip(parts, weights):
        made += dot_nt(part[...], weight[...])
    step = 64
    sent = []
    for i in range(out_ref.shape[0] // step):
        at = slice(i * step, (i + 1) * step)
        rows = rows_ref[at].astype(jnp.float32)
        inverse = lax.rsqrt(jnp.mean(rows * rows, axis=-1, keepdims=True) + EPS)
        unit = rows * inverse
        grad_unit = made[at] * gain_ref[...]
        mean = jnp.mean(grad_unit * unit, axis=-1, keepdims=True)
        out_ref[at] = inverse * (grad_unit - unit * mean)
        sent.append(pltpu.make_async_copy(out_ref.at[at], out_hbm.at[at], sems.at[i]))
        sent[-1].start()
    for copy in sent:
        copy.wait()


def store_gradient(rows, gain, near, parts, weights):
    quarter, model = rows.shape
    width = parts[0].shape[1]
    vmem = pl.BlockSpec(memory_space=pltpu.VMEM)
    return pl.pallas_call(
        final_kernel,
        in_specs=[vmem] * (3 + 2 * len(parts)),
        out_specs=pl.BlockSpec(memory_space=pltpu.HBM),
        out_shape=jax.ShapeDtypeStruct((quarter, model), jnp.float32),
        scratch_shapes=[
            pltpu.VMEM((quarter, model), jnp.float32),
            pltpu.SemaphoreType.DMA((quarter // 64,)),
        ],
        compiler_params=pltpu.CompilerParams(vmem_limit_bytes=16 * MIB),
        cost_estimate=pl.CostEstimate(
            flops=6 * quarter * model * width,
            bytes_accessed=4 * quarter * model,
            transcendentals=quarter,
        ),
        name="store_gradient",
    )(rows, gain, near, *parts, *weights)


def shifted(value, turn):
    return lax.ppermute(value, "tp", [(i, (i + turn) % 4) for i in range(4)])


def halved(value, axis, distance, kind):
    size = lax.axis_size(axis)
    half = value.shape[0] // 2
    pairs = [(i, i ^ distance) for i in range(size)]
    came = lax.ppermute(value[half:].astype(kind), axis, pairs)
    return value[:half] + came.astype(jnp.float32)


def local(queries, gate_pre, cotangent, store, store_gain, w_key, w_value, owners, slots):
    st_size = lax.axis_size(ST)
    width = queries.shape[1]
    rows_dev, model = store.shape
    passages = rows_dev // PLEN
    place = jnp.stack([lax.axis_index("tp"), lax.axis_index(ST)]).astype(jnp.int32)
    gain = store_gain.reshape(1, model)

    owner_turned = owners.T
    hits = owner_turned[None] == jnp.arange(st_size, dtype=jnp.int32)[:, None, None]
    requests = jnp.where(hits, slots.T[None], -1)
    asked = lax.all_to_all(requests, ST, split_axis=0, concat_axis=0, tiled=True)
    asked = jnp.max(asked, axis=(1, 2))

    table, both = key_value_tables(store, gain, w_key, w_value)
    picked = picked_passages(asked, table.reshape(passages, PLEN, 2 * width))
    got = lax.all_to_all(picked, ST, split_axis=0, concat_axis=0, tiled=True)

    both, _ = lax.optimization_barrier((both, picked))
    weights = [both] + [shifted(both, turn) for turn in (1, 3, 2)]
    got, *came = lax.optimization_barrier((got, *weights[1:]))
    weights = [both] + came

    (outgoing,) = attention(owner_turned, queries, gate_pre, cotangent, got, True)
    back_values = lax.all_to_all(outgoing, ST, split_axis=0, concat_axis=0, tiled=True)
    late_store, late_got, _ = lax.optimization_barrier((store, got, outgoing))
    grad_queries, outgoing = attention(
        owner_turned, queries, gate_pre, cotangent, late_got, False
    )
    turned = turned_normed(late_store, gain)
    outgoing, turned = lax.optimization_barrier((outgoing, turned))
    back_keys = lax.all_to_all(outgoing, ST, split_axis=0, concat_axis=0, tiled=True)
    back_values, turned, _ = lax.optimization_barrier((back_values, turned, grad_queries))

    own, first, second, third, mine, other = value_sums(
        asked, place, back_values, turned, passages, st_size
    )
    parts = [own, shifted(first, 1), shifted(third, 3), shifted(second, 2)]
    near = near_products(parts, weights)
    came = lax.ppermute(other, "st_2", [(0, 1), (1, 0)])
    terms = mine.astype(jnp.float32) + came.astype(jnp.float32)
    terms = halved(terms, "st_1", 2, jnp.bfloat16)
    terms = halved(terms, "st_1", 1, jnp.bfloat16)
    back_keys, near = lax.optimization_barrier((back_keys, near))
    terms = halved(terms, "st_0", 4, jnp.float32)

    own, first, second, third = key_sums(asked, place, back_keys, passages)
    own, first, second, third, terms = lax.optimization_barrier(
        (own, first, second, third, terms)
    )
    parts = []
    for part, turn in ((first, 1), (third, 3), (second, 2)):
        parts.append(shifted(part, turn))
    near, own_rows, *key_weights = own_product(place, own, near, weights, store)
    terms = halved(terms, "st_0", 2, jnp.float32)
    terms = halved(terms, "st_0", 1, jnp.float32)
    grad_w_value = terms.reshape(terms.shape[1:])
    grad_store = store_gradient(own_rows, gain, near, parts, key_weights)
    return (grad_queries, grad_store, grad_w_value)


def solution(mesh):
    torus = Mesh(mesh.devices.reshape(8, 4, 2, mesh.shape["tp"]), ("st_0", "st_1", "st_2", "tp"))
    return jax.shard_map(
        local,
        mesh=torus,
        in_specs=(
            P(ST, "tp"),
            P(ST, "tp"),
            P(ST, "tp"),
            P(ST, None),
            P(),
            P(None, "tp"),
            P(None, "tp"),
            P(ST, None),
            P(ST, None),
        ),
        out_specs=(P(ST, "tp"), P(ST_TP, None), P(ST, "tp")),
        check_vma=False,
    )
```

```python
import jax
import jax.numpy as jnp
from jax import lax
from jax.experimental import pallas as pl
from jax.experimental.pallas import tpu as pltpu
from jax.sharding import Mesh
from jax.sharding import PartitionSpec as P


HD = 128
PLEN = 64
EPS = 1e-06
ST = ("st_0", "st_1", "st_2")
ST_TP = ("st_0", "st_1", "st_2", "tp")
MIB = 1024 * 1024


def params(mib):
    return pltpu.CompilerParams(
        dimension_semantics=("arbitrary",), vmem_limit_bytes=mib * MIB
    )


def in_hbm(value):
    return pltpu.with_memory_space_constraint(value, pltpu.HBM)


def dot_nn(a, b):
    return lax.dot_general(a, b, (((1,), (0,)), ((), ())), preferred_element_type=jnp.float32)


def dot_nt(a, b):
    return lax.dot_general(a, b, (((1,), (1,)), ((), ())), preferred_element_type=jnp.float32)


def dot_tn(a, b):
    return lax.dot_general(a, b, (((0,), (0,)), ((), ())), preferred_element_type=jnp.float32)


def normed_rows(x, gain):
    inverse = lax.rsqrt(jnp.mean(x * x, axis=-1, keepdims=True) + EPS)
    return (x * inverse * gain).astype(jnp.bfloat16)


def tables_kernel(store_ref, gain_ref, wk_hbm, wv_hbm, table_ref, both_hbm, wk_ref, wv_ref, sems):
    first = pl.program_id(0) == 0
    last = pl.program_id(0) == pl.num_programs(0) - 1
    width = wk_ref.shape[1]
    keys_out = pltpu.make_async_copy(wk_ref, both_hbm.at[:, :width], sems.at[2])
    values_out = pltpu.make_async_copy(wv_ref, both_hbm.at[:, width:], sems.at[3])
    keys_in = pltpu.make_async_copy(wk_hbm, wk_ref, sems.at[0])
    values_in = pltpu.make_async_copy(wv_hbm, wv_ref, sems.at[1])

    @pl.when(first)
    def _():
        keys_in.start()
        values_in.start()

    normed = normed_rows(store_ref[...].astype(jnp.float32), gain_ref[...])

    @pl.when(first)
    def _():
        keys_in.wait()
        values_in.wait()
        keys_out.start()
        values_out.start()

    table_ref[:, :width] = dot_nn(normed, wk_ref[...]).astype(jnp.bfloat16)
    table_ref[:, width:] = dot_nn(normed, wv_ref[...]).astype(jnp.bfloat16)

    @pl.when(last)
    def _():
        keys_out.wait()
        values_out.wait()


def key_value_tables(store, gain, w_key, w_value):
    rows, model = store.shape
    width = w_key.shape[1]
    step = 256
    return pl.pallas_call(
        tables_kernel,
        grid=(rows // step,),
        in_specs=[
            pl.BlockSpec((step, model), lambda i: (i, 0)),
            pl.BlockSpec((1, model), lambda i: (0, 0)),
            pl.BlockSpec(memory_space=pltpu.HBM),
            pl.BlockSpec(memory_space=pltpu.HBM),
        ],
        out_specs=[
            pl.BlockSpec((step, 2 * width), lambda i: (i, 0)),
            pl.BlockSpec(memory_space=pltpu.HBM),
        ],
        out_shape=[
            jax.ShapeDtypeStruct((rows, 2 * width), jnp.bfloat16),
            pltpu.HBM((model, 2 * width), jnp.bfloat16),
        ],
        scratch_shapes=[
            pltpu.VMEM((model, width), jnp.bfloat16),
            pltpu.VMEM((model, width), jnp.bfloat16),
            pltpu.SemaphoreType.DMA((4,)),
        ],
        compiler_params=params(16),
        cost_estimate=pl.CostEstimate(
            flops=4 * rows * model * width, bytes_accessed=2 * rows * model, transcendentals=rows
        ),
        name="tables",
    )(in_hbm(store), in_hbm(gain), in_hbm(w_key), in_hbm(w_value))


def turned_kernel(store_ref, gain_ref, out_ref):
    normed = normed_rows(store_ref[...].astype(jnp.float32), gain_ref[...])
    out_ref[...] = normed.T


def turned_normed(store, gain):
    rows, model = store.shape
    step = 256
    return pl.pallas_call(
        turned_kernel,
        grid=(rows // step,),
        in_specs=[
            pl.BlockSpec((step, model), lambda i: (i, 0)),
            pl.BlockSpec((1, model), lambda i: (0, 0)),
        ],
        out_specs=pl.BlockSpec((model, step), lambda i: (0, i)),
        out_shape=pltpu.HBM((model, rows), jnp.bfloat16),
        compiler_params=params(16),
        cost_estimate=pl.CostEstimate(
            flops=16 * rows * model, bytes_accessed=4 * rows * model, transcendentals=rows
        ),
        name="turned_normed",
    )(in_hbm(store), in_hbm(gain))


def gather_kernel(asked_ref, table_ref, out_hbm, sems):
    copies = []
    for i in range(out_hbm.shape[0]):
        asked = jnp.maximum(asked_ref[i], 0)
        copies.append(pltpu.make_async_copy(table_ref.at[asked], out_hbm.at[i], sems.at[i]))
        copies[-1].start()
    for copy in copies:
        copy.wait()


def picked_passages(asked, table):
    _, length, width = table.shape
    slots = asked.shape[0]
    return pl.pallas_call(
        gather_kernel,
        in_specs=[
            pl.BlockSpec(memory_space=pltpu.SMEM),
            pl.BlockSpec(memory_space=pltpu.VMEM),
        ],
        out_specs=pl.BlockSpec(memory_space=pltpu.HBM),
        out_shape=pltpu.HBM((slots, length, width), jnp.bfloat16),
        scratch_shapes=[pltpu.SemaphoreType.DMA((slots,))],
        compiler_params=pltpu.CompilerParams(vmem_limit_bytes=8 * MIB),
        name="picked",
    )(asked, table)


def slot_copies(owner_ref, scratch, out_hbm, sems, at, parity):
    per_block = owner_ref.shape[0]
    each = scratch.shape[1] // per_block
    return [
        pltpu.make_async_copy(
            scratch.at[parity, b * per_block + j],
            out_hbm.at[owner_ref[j, at * each + b]],
            sems.at[parity, b * per_block + j],
        )
        for b in range(each)
        for j in range(per_block)
    ]


def wait_slots(owner_ref, scratch, out_hbm, sems):
    step = pl.program_id(0)

    @pl.when(step >= 2)
    def _():
        for copy in slot_copies(owner_ref, scratch, out_hbm, sems, step - 2, lax.rem(step, 2)):
            copy.wait()


def send_slots(owner_ref, scratch, out_hbm, sems):
    step, steps = pl.program_id(0), pl.num_programs(0)
    slot = lax.rem(step, 2)
    for copy in slot_copies(owner_ref, scratch, out_hbm, sems, step, slot):
        copy.start()

    @pl.when(step == steps - 1)
    def _():
        for copy in slot_copies(owner_ref, scratch, out_hbm, sems, step - 1, 1 - slot):
            copy.wait()
        for copy in slot_copies(owner_ref, scratch, out_hbm, sems, step, slot):
            copy.wait()


def block_units(owner_ref, q_ref, g_ref, c_ref, pieces):
    width = q_ref.shape[1]
    per_block = owner_ref.shape[0]
    each = len(pieces) // per_block
    length = q_ref.shape[0] // each
    gate = jax.nn.sigmoid(g_ref[...].astype(jnp.float32))
    grad_in = (gate * c_ref[...].astype(jnp.float32)).astype(jnp.bfloat16)
    units = []
    for b in range(each):
        for h in range(width // HD):
            rows = slice(b * length, (b + 1) * length)
            cols = slice(h * HD, (h + 1) * HD)
            own = pieces[b * per_block : (b + 1) * per_block]
            keys = jnp.concatenate([p[0, :, cols] for p in own], axis=0)
            units.append((b, rows, cols, own, q_ref[rows, cols], grad_in[rows, cols], keys))
    scores = [dot_nt(u[6], u[4]) * HD ** (-0.5) for u in units]
    weights = [jnp.exp(x - jnp.max(x, axis=0, keepdims=True)) for x in scores]
    weights = [x * (1.0 / jnp.sum(x, axis=0, keepdims=True)) for x in weights]
    return units, weights


def value_slots_kernel(owner_ref, q_ref, g_ref, c_ref, *refs):
    pieces, (out_hbm, scratch, sems) = refs[:-3], refs[-3:]
    per_block = owner_ref.shape[0]
    slot = lax.rem(pl.program_id(0), 2)
    units, weights = block_units(owner_ref, q_ref, g_ref, c_ref, pieces)
    wait_slots(owner_ref, scratch, out_hbm, sems)
    for (b, _, cols, _, _, gin, _), weight in zip(units, weights):
        grad_values = dot_nn(weight.astype(jnp.bfloat16), gin).astype(jnp.bfloat16)
        for j in range(per_block):
            part = slice(j * PLEN, (j + 1) * PLEN)
            scratch[slot, b * per_block + j, :, cols] = grad_values[part]
    send_slots(owner_ref, scratch, out_hbm, sems)


def key_slots_kernel(owner_ref, q_ref, g_ref, c_ref, *refs):
    pieces, (gq_ref, out_hbm, scratch, sems) = refs[:-4], refs[-4:]
    per_block = owner_ref.shape[0]
    width = q_ref.shape[1]
    slot = lax.rem(pl.program_id(0), 2)
    units, weights = block_units(owner_ref, q_ref, g_ref, c_ref, pieces)
    grad_weights = []
    for _, _, cols, own, _, gin, _ in units:
        vcols = slice(width + cols.start, width + cols.stop)
        values = jnp.concatenate([p[0, :, vcols] for p in own], axis=0)
        grad_weights.append(dot_nt(values, gin))
    delta = [
        jnp.sum(w.astype(jnp.bfloat16).astype(jnp.float32) * g, axis=0, keepdims=True)
        for w, g in zip(weights, grad_weights)
    ]
    halves = [(w * (g - d)).astype(jnp.bfloat16) for w, g, d in zip(weights, grad_weights, delta)]
    wait_slots(owner_ref, scratch, out_hbm, sems)
    for (b, rows, cols, _, q, _, keys), half in zip(units, halves):
        gq_ref[rows, cols] = dot_tn(half, keys) * HD ** (-0.5)
        grad_keys = (dot_nn(half, q) * HD ** (-0.5)).astype(jnp.bfloat16)
        for j in range(per_block):
            part = slice(j * PLEN, (j + 1) * PLEN)
            scratch[slot, b * per_block + j, :, cols] = grad_keys[part]
    send_slots(owner_ref, scratch, out_hbm, sems)


def attention(owner_turned, queries, gate_pre, cotangent, got, keys_only):
    rows, width = queries.shape
    per_block, blocks = owner_turned.shape
    slots, length, both = got.shape
    each = 2
    steps = blocks // each
    tokens = pl.BlockSpec((rows // steps, width), lambda i, o: (i, 0))
    read = width if keys_only else both

    def piece(b, j):
        return pl.BlockSpec((1, length, read), lambda i, o: (o[j, i * each + b], 0, 0))

    pieces = [piece(b, j) for b in range(each) for j in range(per_block)]
    keys = PLEN * per_block
    out = pltpu.HBM((slots, length, width), jnp.bfloat16)
    hbm = pl.BlockSpec(memory_space=pltpu.HBM)
    return pl.pallas_call(
        value_slots_kernel if keys_only else key_slots_kernel,
        grid_spec=pltpu.PrefetchScalarGridSpec(
            num_scalar_prefetch=1,
            grid=(steps,),
            in_specs=[tokens, tokens, tokens] + pieces,
            out_specs=[hbm] if keys_only else [tokens, hbm],
            scratch_shapes=[
                pltpu.VMEM((2, len(pieces), length, width), jnp.bfloat16),
                pltpu.SemaphoreType.DMA((2, len(pieces))),
            ],
        ),
        out_shape=[out] if keys_only else [jax.ShapeDtypeStruct((rows, width), jnp.float32), out],
        compiler_params=params(20),
        cost_estimate=pl.CostEstimate(
            flops=(4 if keys_only else 8) * rows * width * keys,
            bytes_accessed=10 * rows * width + 2 * got.size,
            transcendentals=rows * width * keys // HD,
        ),
        name="value_slots" if keys_only else "key_slots",
    )(
        owner_turned,
        in_hbm(queries),
        in_hbm(gate_pre),
        in_hbm(cotangent),
        *([in_hbm(got)] * len(pieces)),
    )


def add_asked(asked_ref, back_ref, total):
    step = pl.program_id(0)
    each = back_ref.shape[0]

    @pl.when(step == 0)
    def _():
        total[...] = jnp.zeros_like(total)

    for i in range(each):
        asked = asked_ref[step * each + i]

        @pl.when(asked >= 0)
        def _():
            total[asked] += back_ref[i].astype(jnp.float32)


def write_quarters(place_ref, total, parts):
    passages, length, _ = total.shape
    share = passages // 4
    for turn, out in enumerate(parts):
        first = lax.rem(place_ref[0] + turn, 4) * share
        for p in range(share):
            out[p * length : (p + 1) * length, :] = total[first + p].astype(jnp.bfloat16)


def value_kernel(asked_ref, place_ref, back_ref, turned_hbm, *refs):
    parts, (mine_ref, other_ref, total, terms, turned_ref, sem) = refs[:4], refs[4:]
    turned_in = pltpu.make_async_copy(turned_hbm, turned_ref, sem)

    @pl.when(pl.program_id(0) == 0)
    def _():
        turned_in.start()

    add_asked(asked_ref, back_ref, total)

    @pl.when(pl.program_id(0) == pl.num_programs(0) - 1)
    def _():
        write_quarters(place_ref, total, parts)
        passages, length, width = total.shape
        values = total[...].astype(jnp.bfloat16).reshape(passages * length, width)
        pieces, piece, _ = terms.shape
        turned_in.wait()
        made = dot_nn(turned_ref[...], values).astype(jnp.bfloat16)
        for p in range(pieces):
            terms[p] = made[p * piece : (p + 1) * piece]
        for p in range(pieces // 2):
            turn = p % 8 * 8 + p // 8 * 2
            mine_ref[p] = terms[place_ref[1] ^ turn]
            other_ref[p] = terms[place_ref[1] ^ (turn + 1)]


def value_sums(asked, place, back, turned, passages, devices):
    slots, length, width = back.shape
    model, rows = turned.shape
    each = 16
    quarter = jax.ShapeDtypeStruct((rows // 4, width), jnp.bfloat16)
    half = jax.ShapeDtypeStruct((devices // 2, model // devices, width), jnp.bfloat16)
    return pl.pallas_call(
        value_kernel,
        grid_spec=pltpu.PrefetchScalarGridSpec(
            num_scalar_prefetch=2,
            grid=(slots // each,),
            in_specs=[
                pl.BlockSpec((each, length, width), lambda i, a, t: (i, 0, 0)),
                pl.BlockSpec(memory_space=pltpu.HBM),
            ],
            out_specs=[pl.BlockSpec(quarter.shape, lambda i, a, t: (0, 0))] * 4
            + [pl.BlockSpec(half.shape, lambda i, a, t: (0, 0, 0))] * 2,
            scratch_shapes=[
                pltpu.VMEM((passages, length, width), jnp.float32),
                pltpu.VMEM((devices, model // devices, width), jnp.bfloat16),
                pltpu.VMEM((model, rows), jnp.bfloat16),
                pltpu.SemaphoreType.DMA,
            ],
        ),
        out_shape=[quarter] * 4 + [half] * 2,
        compiler_params=params(24),
        cost_estimate=pl.CostEstimate(
            flops=2 * model * rows * width, bytes_accessed=2 * model * rows, transcendentals=0
        ),
        name="value_sums",
    )(asked, place, back, in_hbm(turned))


def key_kernel(asked_ref, place_ref, back_ref, *refs):
    parts, total = refs[:4], refs[4]
    total[...] = jnp.zeros_like(total)
    for r in range(back_ref.shape[0]):
        asked = asked_ref[r]

        @pl.when(asked >= 0)
        def _():
            total[asked] += back_ref[r].astype(jnp.float32)

    write_quarters(place_ref, total, parts)


def key_sums(asked, place, back, passages):
    _, length, width = back.shape
    quarter = jax.ShapeDtypeStruct((passages * length // 4, width), jnp.bfloat16)
    smem = pl.BlockSpec(memory_space=pltpu.SMEM)
    vmem = pl.BlockSpec(memory_space=pltpu.VMEM)
    return pl.pallas_call(
        key_kernel,
        in_specs=[smem, smem, vmem],
        out_specs=[vmem] * 4,
        out_shape=[quarter] * 4,
        scratch_shapes=[pltpu.VMEM((passages, length, width), jnp.float32)],
        compiler_params=pltpu.CompilerParams(vmem_limit_bytes=12 * MIB),
        cost_estimate=pl.CostEstimate(
            flops=4 * back.size, bytes_accessed=2 * back.size, transcendentals=0
        ),
        name="key_sums",
    )(asked, place, back)


def near_kernel(*refs):
    count = 4
    parts, weights, out_ref = refs[:count], refs[count : 2 * count], refs[2 * count]
    held, sems = refs[2 * count + 1 : -1], refs[-1]
    width = parts[0].shape[1]
    arrivals = [
        pltpu.make_async_copy(w.at[:, width:], h, sems.at[i])
        for i, (w, h) in enumerate(zip(weights, held))
    ]
    for copy in arrivals:
        copy.start()
    made = []
    for part, arrival, h in zip(parts, arrivals, held):
        arrival.wait()
        made.append(dot_nt(part[...], h[...]))
    out_ref[...] = sum(made)


def near_products(parts, weights):
    quarter, width = parts[0].shape
    model = weights[0].shape[0]
    count = len(parts)
    vmem = pl.BlockSpec(memory_space=pltpu.VMEM)
    hbm = pl.BlockSpec(memory_space=pltpu.HBM)
    return pl.pallas_call(
        near_kernel,
        in_specs=[vmem] * count + [hbm] * count,
        out_specs=vmem,
        out_shape=jax.ShapeDtypeStruct((quarter, model), jnp.float32),
        scratch_shapes=[pltpu.VMEM((model, width), jnp.bfloat16)] * count
        + [pltpu.SemaphoreType.DMA((count,))],
        compiler_params=pltpu.CompilerParams(vmem_limit_bytes=16 * MIB),
        cost_estimate=pl.CostEstimate(
            flops=2 * count * quarter * model * width,
            bytes_accessed=2 * count * model * width,
            transcendentals=0,
        ),
        name="near_products",
    )(*parts, *[in_hbm(w) for w in weights])


def own_kernel(place_ref, part_ref, near_ref, *refs):
    count = 4
    weights, store_hbm = refs[:count], refs[count]
    out_ref, rows_ref, *keys_refs = refs[count + 1 : 2 * count + 2]
    held, sems = refs[2 * count + 2], refs[-1]
    quarter, width = part_ref.shape
    first = pl.multiple_of(place_ref[0] * quarter, quarter)
    copies = [
        pltpu.make_async_copy(w.at[:, :width], k, sems.at[i])
        for i, (w, k) in enumerate(zip(weights, [held] + keys_refs))
    ]
    copies.append(
        pltpu.make_async_copy(store_hbm.at[pl.ds(first, quarter)], rows_ref, sems.at[count])
    )
    for copy in copies:
        copy.start()
    copies[0].wait()
    out_ref[...] = near_ref[...] + dot_nt(part_ref[...], held[...])
    for copy in copies[1:]:
        copy.wait()


def own_product(place, part, near, weights, store):
    quarter, width = part.shape
    model = weights[0].shape[0]
    count = len(weights)
    vmem = pl.BlockSpec(memory_space=pltpu.VMEM)
    hbm = pl.BlockSpec(memory_space=pltpu.HBM)
    return pl.pallas_call(
        own_kernel,
        in_specs=[pl.BlockSpec(memory_space=pltpu.SMEM), vmem, vmem] + [hbm] * (count + 1),
        out_specs=[vmem] * (count + 1),
        out_shape=[
            pltpu.VMEM((quarter, model), jnp.float32),
            pltpu.VMEM((quarter, model), jnp.bfloat16),
        ]
        + [pltpu.VMEM((model, width), jnp.bfloat16)] * (count - 1),
        scratch_shapes=[
            pltpu.VMEM((model, width), jnp.bfloat16),
            pltpu.SemaphoreType.DMA((count + 1,)),
        ],
        compiler_params=pltpu.CompilerParams(vmem_limit_bytes=16 * MIB),
        cost_estimate=pl.CostEstimate(
            flops=2 * quarter * model * width,
            bytes_accessed=4 * count * model * width,
            transcendentals=0,
        ),
        name="own_product",
    )(place, part, near, *[in_hbm(w) for w in weights], in_hbm(store))


def final_kernel(rows_ref, gain_ref, near_ref, *refs):
    parts, weights, (out_hbm, out_ref, sems) = refs[:3], refs[3:6], refs[6:]
    made = near_ref[...]
    for part, weight in zip(parts, weights):
        made += dot_nt(part[...], weight[...])
    step = 64
    sent = []
    for i in range(out_ref.shape[0] // step):
        at = slice(i * step, (i + 1) * step)
        rows = rows_ref[at].astype(jnp.float32)
        inverse = lax.rsqrt(jnp.mean(rows * rows, axis=-1, keepdims=True) + EPS)
        unit = rows * inverse
        grad_unit = made[at] * gain_ref[...]
        mean = jnp.mean(grad_unit * unit, axis=-1, keepdims=True)
        out_ref[at] = inverse * (grad_unit - unit * mean)
        sent.append(pltpu.make_async_copy(out_ref.at[at], out_hbm.at[at], sems.at[i]))
        sent[-1].start()
    for copy in sent:
        copy.wait()


def store_gradient(rows, gain, near, parts, weights):
    quarter, model = rows.shape
    width = parts[0].shape[1]
    vmem = pl.BlockSpec(memory_space=pltpu.VMEM)
    return pl.pallas_call(
        final_kernel,
        in_specs=[vmem] * (3 + 2 * len(parts)),
        out_specs=pl.BlockSpec(memory_space=pltpu.HBM),
        out_shape=jax.ShapeDtypeStruct((quarter, model), jnp.float32),
        scratch_shapes=[
            pltpu.VMEM((quarter, model), jnp.float32),
            pltpu.SemaphoreType.DMA((quarter // 64,)),
        ],
        compiler_params=pltpu.CompilerParams(vmem_limit_bytes=16 * MIB),
        cost_estimate=pl.CostEstimate(
            flops=6 * quarter * model * width,
            bytes_accessed=4 * quarter * model,
            transcendentals=quarter,
        ),
        name="store_gradient",
    )(rows, gain, near, *parts, *weights)


def shifted(value, turn):
    return lax.ppermute(value, "tp", [(i, (i + turn) % 4) for i in range(4)])


def halved(value, axis, distance, kind):
    size = lax.axis_size(axis)
    half = value.shape[0] // 2
    pairs = [(i, i ^ distance) for i in range(size)]
    came = lax.ppermute(value[half:].astype(kind), axis, pairs)
    return value[:half] + came.astype(jnp.float32)


def local(queries, gate_pre, cotangent, store, store_gain, w_key, w_value, owners, slots):
    st_size = lax.axis_size(ST)
    width = queries.shape[1]
    rows_dev, model = store.shape
    passages = rows_dev // PLEN
    place = jnp.stack([lax.axis_index("tp"), lax.axis_index(ST)]).astype(jnp.int32)
    gain = store_gain.reshape(1, model)

    owner_turned = owners.T
    hits = owner_turned[None] == jnp.arange(st_size, dtype=jnp.int32)[:, None, None]
    requests = jnp.where(hits, slots.T[None], -1)
    asked = lax.all_to_all(requests, ST, split_axis=0, concat_axis=0, tiled=True)
    asked = jnp.max(asked, axis=(1, 2))

    table, both = key_value_tables(store, gain, w_key, w_value)
    picked = picked_passages(asked, table.reshape(passages, PLEN, 2 * width))
    got = lax.all_to_all(picked, ST, split_axis=0, concat_axis=0, tiled=True)

    both, _ = lax.optimization_barrier((both, picked))
    weights = [both]
    for turn in (1, 3, 2):
        weights.append(shifted(both, turn))

    (outgoing,) = attention(owner_turned, queries, gate_pre, cotangent, got, True)
    back_values = lax.all_to_all(outgoing, ST, split_axis=0, concat_axis=0, tiled=True)
    late_got, _ = lax.optimization_barrier((got, outgoing))
    grad_queries, outgoing = attention(
        owner_turned, queries, gate_pre, cotangent, late_got, False
    )
    turned = turned_normed(store, gain)
    outgoing, turned = lax.optimization_barrier((outgoing, turned))
    back_keys = lax.all_to_all(outgoing, ST, split_axis=0, concat_axis=0, tiled=True)
    back_values, turned, *near_weights = lax.optimization_barrier(
        (back_values, turned, *weights[1:])
    )
    weights[1:] = near_weights

    own, first, second, third, mine, other = value_sums(
        asked, place, back_values, turned, passages, st_size
    )
    parts = [own, shifted(first, 1), shifted(third, 3), shifted(second, 2)]
    near = near_products(parts, weights)
    came = lax.ppermute(other, "st_2", [(0, 1), (1, 0)])
    terms = mine.astype(jnp.float32) + came.astype(jnp.float32)
    terms = halved(terms, "st_1", 2, jnp.bfloat16)
    terms = halved(terms, "st_1", 1, jnp.bfloat16)
    back_keys, near = lax.optimization_barrier((back_keys, near))
    spread = [terms[0]]
    for distance in range(1, terms.shape[0]):
        pairs = [(i, i ^ distance) for i in range(terms.shape[0])]
        spread.append(lax.ppermute(terms[distance], "st_0", pairs))

    own, first, second, third = key_sums(asked, place, back_keys, passages)
    parts = []
    for part, turn in ((first, 1), (third, 3), (second, 2)):
        parts.append(shifted(part, turn))
    near, own_rows, *key_weights = own_product(place, own, near, weights, store)
    grad_w_value = sum(spread)
    grad_store = store_gradient(own_rows, gain, near, parts, key_weights)
    return (grad_queries, grad_store, grad_w_value)


def solution(mesh):
    torus = Mesh(mesh.devices.reshape(8, 4, 2, mesh.shape["tp"]), ("st_0", "st_1", "st_2", "tp"))
    return jax.shard_map(
        local,
        mesh=torus,
        in_specs=(
            P(ST, "tp"),
            P(ST, "tp"),
            P(ST, "tp"),
            P(ST, None),
            P(),
            P(None, "tp"),
            P(None, "tp"),
            P(ST, None),
            P(ST, None),
        ),
        out_specs=(P(ST, "tp"), P(ST_TP, None), P(ST, "tp")),
        check_vma=False,
    )
```

```python
import jax
import jax.numpy as jnp
from jax import lax
from jax.experimental import pallas as pl
from jax.experimental.pallas import tpu as pltpu
from jax.sharding import Mesh
from jax.sharding import PartitionSpec as P


HD = 128
PLEN = 64
EPS = 1e-06
ST = ("st_0", "st_1", "st_2")
ST_TP = ("st_0", "st_1", "st_2", "tp")
MIB = 1024 * 1024


def params(mib):
    return pltpu.CompilerParams(
        dimension_semantics=("arbitrary",), vmem_limit_bytes=mib * MIB
    )


def in_hbm(value):
    return pltpu.with_memory_space_constraint(value, pltpu.HBM)


def dot_nn(a, b):
    return lax.dot_general(a, b, (((1,), (0,)), ((), ())), preferred_element_type=jnp.float32)


def dot_nt(a, b):
    return lax.dot_general(a, b, (((1,), (1,)), ((), ())), preferred_element_type=jnp.float32)


def dot_tn(a, b):
    return lax.dot_general(a, b, (((0,), (0,)), ((), ())), preferred_element_type=jnp.float32)


def normed_rows(x, gain):
    inverse = lax.rsqrt(jnp.mean(x * x, axis=-1, keepdims=True) + EPS)
    return (x * inverse * gain).astype(jnp.bfloat16)


def tables_kernel(store_ref, gain_ref, wk_hbm, wv_hbm, table_ref, both_hbm, wk_ref, wv_ref, sems):
    first = pl.program_id(0) == 0
    last = pl.program_id(0) == pl.num_programs(0) - 1
    width = wk_ref.shape[1]
    keys_out = pltpu.make_async_copy(wk_ref, both_hbm.at[:, :width], sems.at[2])
    values_out = pltpu.make_async_copy(wv_ref, both_hbm.at[:, width:], sems.at[3])
    keys_in = pltpu.make_async_copy(wk_hbm, wk_ref, sems.at[0])
    values_in = pltpu.make_async_copy(wv_hbm, wv_ref, sems.at[1])

    @pl.when(first)
    def _():
        keys_in.start()
        values_in.start()

    normed = normed_rows(store_ref[...].astype(jnp.float32), gain_ref[...])

    @pl.when(first)
    def _():
        keys_in.wait()
        values_in.wait()
        keys_out.start()
        values_out.start()

    table_ref[:, :width] = dot_nn(normed, wk_ref[...]).astype(jnp.bfloat16)
    table_ref[:, width:] = dot_nn(normed, wv_ref[...]).astype(jnp.bfloat16)

    @pl.when(last)
    def _():
        keys_out.wait()
        values_out.wait()


def key_value_tables(store, gain, w_key, w_value):
    rows, model = store.shape
    width = w_key.shape[1]
    step = 256
    return pl.pallas_call(
        tables_kernel,
        grid=(rows // step,),
        in_specs=[
            pl.BlockSpec((step, model), lambda i: (i, 0)),
            pl.BlockSpec((1, model), lambda i: (0, 0)),
            pl.BlockSpec(memory_space=pltpu.HBM),
            pl.BlockSpec(memory_space=pltpu.HBM),
        ],
        out_specs=[
            pl.BlockSpec((step, 2 * width), lambda i: (i, 0)),
            pl.BlockSpec(memory_space=pltpu.HBM),
        ],
        out_shape=[
            jax.ShapeDtypeStruct((rows, 2 * width), jnp.bfloat16),
            pltpu.HBM((model, 2 * width), jnp.bfloat16),
        ],
        scratch_shapes=[
            pltpu.VMEM((model, width), jnp.bfloat16),
            pltpu.VMEM((model, width), jnp.bfloat16),
            pltpu.SemaphoreType.DMA((4,)),
        ],
        compiler_params=params(16),
        cost_estimate=pl.CostEstimate(
            flops=4 * rows * model * width, bytes_accessed=2 * rows * model, transcendentals=rows
        ),
        name="tables",
    )(in_hbm(store), in_hbm(gain), in_hbm(w_key), in_hbm(w_value))


def turned_kernel(store_ref, gain_ref, out_ref):
    normed = normed_rows(store_ref[...].astype(jnp.float32), gain_ref[...])
    out_ref[...] = normed.T


def turned_normed(store, gain):
    rows, model = store.shape
    step = 256
    return pl.pallas_call(
        turned_kernel,
        grid=(rows // step,),
        in_specs=[
            pl.BlockSpec((step, model), lambda i: (i, 0)),
            pl.BlockSpec((1, model), lambda i: (0, 0)),
        ],
        out_specs=pl.BlockSpec((model, step), lambda i: (0, i)),
        out_shape=pltpu.HBM((model, rows), jnp.bfloat16),
        compiler_params=params(16),
        cost_estimate=pl.CostEstimate(
            flops=16 * rows * model, bytes_accessed=4 * rows * model, transcendentals=rows
        ),
        name="turned_normed",
    )(in_hbm(store), in_hbm(gain))


def gather_kernel(asked_ref, table_ref, out_hbm, sems):
    copies = []
    for i in range(out_hbm.shape[0]):
        asked = jnp.maximum(asked_ref[i], 0)
        copies.append(pltpu.make_async_copy(table_ref.at[asked], out_hbm.at[i], sems.at[i]))
        copies[-1].start()
    for copy in copies:
        copy.wait()


def picked_passages(asked, table):
    _, length, width = table.shape
    slots = asked.shape[0]
    return pl.pallas_call(
        gather_kernel,
        in_specs=[
            pl.BlockSpec(memory_space=pltpu.SMEM),
            pl.BlockSpec(memory_space=pltpu.VMEM),
        ],
        out_specs=pl.BlockSpec(memory_space=pltpu.HBM),
        out_shape=pltpu.HBM((slots, length, width), jnp.bfloat16),
        scratch_shapes=[pltpu.SemaphoreType.DMA((slots,))],
        compiler_params=pltpu.CompilerParams(vmem_limit_bytes=8 * MIB),
        name="picked",
    )(asked, table)


def gated_kernel(g_ref, c_ref, out_ref):
    gate = jax.nn.sigmoid(g_ref[...].astype(jnp.float32))
    out_ref[...] = (gate * c_ref[...].astype(jnp.float32)).astype(jnp.bfloat16)


def gated(gate_pre, cotangent):
    rows, width = gate_pre.shape
    step = pl.BlockSpec((rows // 4, width), lambda i: (i, 0))
    return pl.pallas_call(
        gated_kernel,
        grid=(4,),
        in_specs=[step, step],
        out_specs=step,
        out_shape=jax.ShapeDtypeStruct((rows, width), jnp.bfloat16),
        compiler_params=params(8),
        cost_estimate=pl.CostEstimate(
            flops=8 * rows * width, bytes_accessed=6 * rows * width, transcendentals=rows * width
        ),
        name="gated",
    )(in_hbm(gate_pre), in_hbm(cotangent))


def slot_copies(owner_ref, scratch, out_hbm, sems, at, parity):
    per_block = owner_ref.shape[0]
    each = scratch.shape[1] // per_block
    return [
        pltpu.make_async_copy(
            scratch.at[parity, b * per_block + j],
            out_hbm.at[owner_ref[j, at * each + b]],
            sems.at[parity, b * per_block + j],
        )
        for b in range(each)
        for j in range(per_block)
    ]


def wait_slots(owner_ref, scratch, out_hbm, sems):
    step = pl.program_id(0)

    @pl.when(step >= 2)
    def _():
        for copy in slot_copies(owner_ref, scratch, out_hbm, sems, step - 2, lax.rem(step, 2)):
            copy.wait()


def send_slots(owner_ref, scratch, out_hbm, sems):
    step, steps = pl.program_id(0), pl.num_programs(0)
    slot = lax.rem(step, 2)
    for copy in slot_copies(owner_ref, scratch, out_hbm, sems, step, slot):
        copy.start()

    @pl.when(step == steps - 1)
    def _():
        for copy in slot_copies(owner_ref, scratch, out_hbm, sems, step - 1, 1 - slot):
            copy.wait()
        for copy in slot_copies(owner_ref, scratch, out_hbm, sems, step, slot):
            copy.wait()


def softmax_turned(keys, q):
    scores = dot_nt(keys, q) * HD ** (-0.5)
    weights = jnp.exp(scores - jnp.max(scores, axis=0, keepdims=True))
    return weights * (1.0 / jnp.sum(weights, axis=0, keepdims=True))


def value_slots_kernel(owner_ref, q_ref, gin_ref, got_hbm, out_hbm, keys_ref, made_ref, sems):
    per_block, blocks = owner_ref.shape
    length = q_ref.shape[0] // blocks
    width = q_ref.shape[1]
    places = [(b, j) for b in range(blocks) for j in range(per_block)]
    arrivals, sent = [], []
    for i, (b, j) in enumerate(places):
        piece = got_hbm.at[owner_ref[j, b], :, :width]
        arrivals.append(pltpu.make_async_copy(piece, keys_ref.at[i], sems.at[i]))
        arrivals[-1].start()
    for b in range(blocks):
        first = b * per_block
        rows = slice(b * length, (b + 1) * length)
        for arrival in arrivals[first : first + per_block]:
            arrival.wait()
        for h in range(width // HD):
            cols = slice(h * HD, (h + 1) * HD)
            keys = keys_ref[first : first + per_block, :, cols].reshape(per_block * PLEN, HD)
            weights = softmax_turned(keys, q_ref[rows, cols]).astype(jnp.bfloat16)
            values = dot_nn(weights, gin_ref[rows, cols]).astype(jnp.bfloat16)
            made_ref[first : first + per_block, :, cols] = values.reshape(per_block, PLEN, HD)
        for i in range(first, first + per_block):
            place = out_hbm.at[owner_ref[i - first, b]]
            sent.append(pltpu.make_async_copy(made_ref.at[i], place, sems.at[len(places) + i]))
            sent[-1].start()
    for copy in sent:
        copy.wait()


def value_slots(owner_turned, queries, grad_in, got):
    slots, length, _ = got.shape
    count = owner_turned.shape[0] * owner_turned.shape[1]
    width = queries.shape[1]
    smem = pl.BlockSpec(memory_space=pltpu.SMEM)
    vmem = pl.BlockSpec(memory_space=pltpu.VMEM)
    hbm = pl.BlockSpec(memory_space=pltpu.HBM)
    pieces = pltpu.VMEM((count, length, width), jnp.bfloat16)
    return pl.pallas_call(
        value_slots_kernel,
        in_specs=[smem, vmem, vmem, hbm],
        out_specs=hbm,
        out_shape=pltpu.HBM((slots, length, width), jnp.bfloat16),
        scratch_shapes=[pieces, pieces, pltpu.SemaphoreType.DMA((2 * count,))],
        compiler_params=pltpu.CompilerParams(vmem_limit_bytes=12 * MIB),
        cost_estimate=pl.CostEstimate(
            flops=4 * queries.size * PLEN * owner_turned.shape[0],
            bytes_accessed=2 * got.size,
            transcendentals=queries.size * PLEN * owner_turned.shape[0] // HD,
        ),
        name="value_slots",
    )(owner_turned, queries, grad_in, in_hbm(got))


def key_slots_kernel(owner_ref, q_ref, gin_ref, *refs):
    pieces, (gq_ref, out_hbm, scratch, sems) = refs[:-4], refs[-4:]
    per_block = owner_ref.shape[0]
    width = q_ref.shape[1]
    each = len(pieces) // per_block
    length = q_ref.shape[0] // each
    slot = lax.rem(pl.program_id(0), 2)
    units = []
    for b in range(each):
        for h in range(width // HD):
            rows = slice(b * length, (b + 1) * length)
            cols = slice(h * HD, (h + 1) * HD)
            vcols = slice(width + h * HD, width + (h + 1) * HD)
            own = pieces[b * per_block : (b + 1) * per_block]
            keys = jnp.concatenate([p[0, :, cols] for p in own], axis=0)
            values = jnp.concatenate([p[0, :, vcols] for p in own], axis=0)
            q = q_ref[rows, cols]
            weights = softmax_turned(keys, q)
            grad_weights = dot_nt(values, gin_ref[rows, cols])
            kept = weights.astype(jnp.bfloat16).astype(jnp.float32)
            delta = jnp.sum(kept * grad_weights, axis=0, keepdims=True)
            half = (weights * (grad_weights - delta)).astype(jnp.bfloat16)
            units.append((b, rows, cols, q, keys, half))
    wait_slots(owner_ref, scratch, out_hbm, sems)
    for b, rows, cols, q, keys, half in units:
        gq_ref[rows, cols] = dot_tn(half, keys) * HD ** (-0.5)
        grad_keys = (dot_nn(half, q) * HD ** (-0.5)).astype(jnp.bfloat16)
        for j in range(per_block):
            part = slice(j * PLEN, (j + 1) * PLEN)
            scratch[slot, b * per_block + j, :, cols] = grad_keys[part]
    send_slots(owner_ref, scratch, out_hbm, sems)


def key_slots(owner_turned, queries, grad_in, got):
    rows, width = queries.shape
    per_block, blocks = owner_turned.shape
    slots, length, both = got.shape
    each = 2
    steps = blocks // each
    tokens = pl.BlockSpec((rows // steps, width), lambda i, o: (i, 0))

    def piece(b, j):
        return pl.BlockSpec((1, length, both), lambda i, o: (o[j, i * each + b], 0, 0))

    pieces = [piece(b, j) for b in range(each) for j in range(per_block)]
    keys = PLEN * per_block
    return pl.pallas_call(
        key_slots_kernel,
        grid_spec=pltpu.PrefetchScalarGridSpec(
            num_scalar_prefetch=1,
            grid=(steps,),
            in_specs=[tokens, tokens] + pieces,
            out_specs=[tokens, pl.BlockSpec(memory_space=pltpu.HBM)],
            scratch_shapes=[
                pltpu.VMEM((2, len(pieces), length, width), jnp.bfloat16),
                pltpu.SemaphoreType.DMA((2, len(pieces))),
            ],
        ),
        out_shape=[
            jax.ShapeDtypeStruct((rows, width), jnp.float32),
            pltpu.HBM((slots, length, width), jnp.bfloat16),
        ],
        compiler_params=params(20),
        cost_estimate=pl.CostEstimate(
            flops=8 * rows * width * keys,
            bytes_accessed=10 * rows * width + 2 * got.size,
            transcendentals=rows * width * keys // HD,
        ),
        name="key_slots",
    )(owner_turned, queries, grad_in, *([in_hbm(got)] * len(pieces)))


def add_asked(asked_ref, back_ref, total):
    step = pl.program_id(0)
    each = back_ref.shape[0]

    @pl.when(step == 0)
    def _():
        total[...] = jnp.zeros_like(total)

    for i in range(each):
        asked = asked_ref[step * each + i]

        @pl.when(asked >= 0)
        def _():
            total[asked] += back_ref[i].astype(jnp.float32)


def write_quarters(place_ref, total, parts):
    passages, length, _ = total.shape
    share = passages // 4
    for turn, out in enumerate(parts):
        first = lax.rem(place_ref[0] + turn, 4) * share
        for p in range(share):
            out[p * length : (p + 1) * length, :] = total[first + p].astype(jnp.bfloat16)


def value_kernel(asked_ref, place_ref, back_ref, turned_hbm, *refs):
    parts, (mine_ref, other_ref, total, terms, turned_ref, sem) = refs[:4], refs[4:]
    turned_in = pltpu.make_async_copy(turned_hbm, turned_ref, sem)

    @pl.when(pl.program_id(0) == 0)
    def _():
        turned_in.start()

    add_asked(asked_ref, back_ref, total)

    @pl.when(pl.program_id(0) == pl.num_programs(0) - 1)
    def _():
        write_quarters(place_ref, total, parts)
        passages, length, width = total.shape
        values = total[...].astype(jnp.bfloat16).reshape(passages * length, width)
        pieces, piece, _ = terms.shape
        turned_in.wait()
        made = dot_nn(turned_ref[...], values).astype(jnp.bfloat16)
        for p in range(pieces):
            terms[p] = made[p * piece : (p + 1) * piece]
        for p in range(pieces // 2):
            turn = p % 8 * 8 + p // 8 * 2
            mine_ref[p] = terms[place_ref[1] ^ turn]
            other_ref[p] = terms[place_ref[1] ^ (turn + 1)]


def value_sums(asked, place, back, turned, passages, devices):
    slots, length, width = back.shape
    model, rows = turned.shape
    each = 16
    quarter = jax.ShapeDtypeStruct((rows // 4, width), jnp.bfloat16)
    half = jax.ShapeDtypeStruct((devices // 2, model // devices, width), jnp.bfloat16)
    return pl.pallas_call(
        value_kernel,
        grid_spec=pltpu.PrefetchScalarGridSpec(
            num_scalar_prefetch=2,
            grid=(slots // each,),
            in_specs=[
                pl.BlockSpec((each, length, width), lambda i, a, t: (i, 0, 0)),
                pl.BlockSpec(memory_space=pltpu.HBM),
            ],
            out_specs=[pl.BlockSpec(quarter.shape, lambda i, a, t: (0, 0))] * 4
            + [pl.BlockSpec(half.shape, lambda i, a, t: (0, 0, 0))] * 2,
            scratch_shapes=[
                pltpu.VMEM((passages, length, width), jnp.float32),
                pltpu.VMEM((devices, model // devices, width), jnp.bfloat16),
                pltpu.VMEM((model, rows), jnp.bfloat16),
                pltpu.SemaphoreType.DMA,
            ],
        ),
        out_shape=[quarter] * 4 + [half] * 2,
        compiler_params=params(24),
        cost_estimate=pl.CostEstimate(
            flops=2 * model * rows * width, bytes_accessed=2 * model * rows, transcendentals=0
        ),
        name="value_sums",
    )(asked, place, back, in_hbm(turned))


def key_kernel(asked_ref, place_ref, back_ref, *refs):
    parts, total = refs[:4], refs[4]
    total[...] = jnp.zeros_like(total)
    for r in range(back_ref.shape[0]):
        asked = asked_ref[r]

        @pl.when(asked >= 0)
        def _():
            total[asked] += back_ref[r].astype(jnp.float32)

    write_quarters(place_ref, total, parts)


def key_sums(asked, place, back, passages):
    _, length, width = back.shape
    quarter = jax.ShapeDtypeStruct((passages * length // 4, width), jnp.bfloat16)
    smem = pl.BlockSpec(memory_space=pltpu.SMEM)
    vmem = pl.BlockSpec(memory_space=pltpu.VMEM)
    return pl.pallas_call(
        key_kernel,
        in_specs=[smem, smem, vmem],
        out_specs=[vmem] * 4,
        out_shape=[quarter] * 4,
        scratch_shapes=[pltpu.VMEM((passages, length, width), jnp.float32)],
        compiler_params=pltpu.CompilerParams(vmem_limit_bytes=12 * MIB),
        cost_estimate=pl.CostEstimate(
            flops=4 * back.size, bytes_accessed=2 * back.size, transcendentals=0
        ),
        name="key_sums",
    )(asked, place, back)


def near_kernel(*refs):
    count = 4
    parts, weights, out_ref = refs[:count], refs[count : 2 * count], refs[2 * count]
    held, sems = refs[2 * count + 1 : -1], refs[-1]
    width = parts[0].shape[1]
    arrivals = [
        pltpu.make_async_copy(w.at[:, width:], h, sems.at[i])
        for i, (w, h) in enumerate(zip(weights, held))
    ]
    for copy in arrivals:
        copy.start()
    made = []
    for part, arrival, h in zip(parts, arrivals, held):
        arrival.wait()
        made.append(dot_nt(part[...], h[...]))
    out_ref[...] = sum(made)


def near_products(parts, weights):
    quarter, width = parts[0].shape
    model = weights[0].shape[0]
    count = len(parts)
    vmem = pl.BlockSpec(memory_space=pltpu.VMEM)
    hbm = pl.BlockSpec(memory_space=pltpu.HBM)
    return pl.pallas_call(
        near_kernel,
        in_specs=[vmem] * count + [hbm] * count,
        out_specs=vmem,
        out_shape=jax.ShapeDtypeStruct((quarter, model), jnp.float32),
        scratch_shapes=[pltpu.VMEM((model, width), jnp.bfloat16)] * count
        + [pltpu.SemaphoreType.DMA((count,))],
        compiler_params=pltpu.CompilerParams(vmem_limit_bytes=16 * MIB),
        cost_estimate=pl.CostEstimate(
            flops=2 * count * quarter * model * width,
            bytes_accessed=2 * count * model * width,
            transcendentals=0,
        ),
        name="near_products",
    )(*parts, *[in_hbm(w) for w in weights])


def own_kernel(place_ref, part_ref, near_ref, *refs):
    count = 4
    weights, store_hbm = refs[:count], refs[count]
    out_ref, rows_ref, *keys_refs = refs[count + 1 : 2 * count + 2]
    held, sems = refs[2 * count + 2], refs[-1]
    quarter, width = part_ref.shape
    first = pl.multiple_of(place_ref[0] * quarter, quarter)
    copies = [
        pltpu.make_async_copy(w.at[:, :width], k, sems.at[i])
        for i, (w, k) in enumerate(zip(weights, [held] + keys_refs))
    ]
    copies.append(
        pltpu.make_async_copy(store_hbm.at[pl.ds(first, quarter)], rows_ref, sems.at[count])
    )
    for copy in copies:
        copy.start()
    copies[0].wait()
    out_ref[...] = near_ref[...] + dot_nt(part_ref[...], held[...])
    for copy in copies[1:]:
        copy.wait()


def own_product(place, part, near, weights, store):
    quarter, width = part.shape
    model = weights[0].shape[0]
    count = len(weights)
    vmem = pl.BlockSpec(memory_space=pltpu.VMEM)
    hbm = pl.BlockSpec(memory_space=pltpu.HBM)
    return pl.pallas_call(
        own_kernel,
        in_specs=[pl.BlockSpec(memory_space=pltpu.SMEM), vmem, vmem] + [hbm] * (count + 1),
        out_specs=[vmem] * (count + 1),
        out_shape=[
            pltpu.VMEM((quarter, model), jnp.float32),
            pltpu.VMEM((quarter, model), jnp.bfloat16),
        ]
        + [pltpu.VMEM((model, width), jnp.bfloat16)] * (count - 1),
        scratch_shapes=[
            pltpu.VMEM((model, width), jnp.bfloat16),
            pltpu.SemaphoreType.DMA((count + 1,)),
        ],
        compiler_params=pltpu.CompilerParams(vmem_limit_bytes=16 * MIB),
        cost_estimate=pl.CostEstimate(
            flops=2 * quarter * model * width,
            bytes_accessed=4 * count * model * width,
            transcendentals=0,
        ),
        name="own_product",
    )(place, part, near, *[in_hbm(w) for w in weights], in_hbm(store))


def final_kernel(rows_ref, gain_ref, near_ref, *refs):
    parts, weights, (out_hbm, out_ref, sems) = refs[:3], refs[3:6], refs[6:]
    made = near_ref[...]
    for part, weight in zip(parts, weights):
        made += dot_nt(part[...], weight[...])
    step = 64
    sent = []
    for i in range(out_ref.shape[0] // step):
        at = slice(i * step, (i + 1) * step)
        rows = rows_ref[at].astype(jnp.float32)
        inverse = lax.rsqrt(jnp.mean(rows * rows, axis=-1, keepdims=True) + EPS)
        unit = rows * inverse
        grad_unit = made[at] * gain_ref[...]
        mean = jnp.mean(grad_unit * unit, axis=-1, keepdims=True)
        out_ref[at] = inverse * (grad_unit - unit * mean)
        sent.append(pltpu.make_async_copy(out_ref.at[at], out_hbm.at[at], sems.at[i]))
        sent[-1].start()
    for copy in sent:
        copy.wait()


def store_gradient(rows, gain, near, parts, weights):
    quarter, model = rows.shape
    width = parts[0].shape[1]
    vmem = pl.BlockSpec(memory_space=pltpu.VMEM)
    return pl.pallas_call(
        final_kernel,
        in_specs=[vmem] * (3 + 2 * len(parts)),
        out_specs=pl.BlockSpec(memory_space=pltpu.HBM),
        out_shape=jax.ShapeDtypeStruct((quarter, model), jnp.float32),
        scratch_shapes=[
            pltpu.VMEM((quarter, model), jnp.float32),
            pltpu.SemaphoreType.DMA((quarter // 64,)),
        ],
        compiler_params=pltpu.CompilerParams(vmem_limit_bytes=16 * MIB),
        cost_estimate=pl.CostEstimate(
            flops=6 * quarter * model * width,
            bytes_accessed=4 * quarter * model,
            transcendentals=quarter,
        ),
        name="store_gradient",
    )(rows, gain, near, *parts, *weights)


def shifted(value, turn):
    return lax.ppermute(value, "tp", [(i, (i + turn) % 4) for i in range(4)])


def local(queries, gate_pre, cotangent, store, store_gain, w_key, w_value, owners, slots):
    st_size = lax.axis_size(ST)
    width = queries.shape[1]
    rows_dev, model = store.shape
    passages = rows_dev // PLEN
    place = jnp.stack([lax.axis_index("tp"), lax.axis_index(ST)]).astype(jnp.int32)
    gain = store_gain.reshape(1, model)

    owner_turned = owners.T
    hits = owner_turned[None] == jnp.arange(st_size, dtype=jnp.int32)[:, None, None]
    requests = jnp.where(hits, slots.T[None], -1)
    asked = lax.all_to_all(requests, ST, split_axis=0, concat_axis=0, tiled=True)
    asked = jnp.max(asked, axis=(1, 2))

    table, both = key_value_tables(store, gain, w_key, w_value)
    picked = picked_passages(asked, table.reshape(passages, PLEN, 2 * width))
    got = lax.all_to_all(picked, ST, split_axis=0, concat_axis=0, tiled=True)

    both, _ = lax.optimization_barrier((both, picked))
    weights = [both]
    for turn in (1, 3, 2):
        weights.append(shifted(both, turn))

    grad_in = gated(gate_pre, cotangent)
    outgoing = value_slots(owner_turned, queries, grad_in, got)
    back_values = lax.all_to_all(outgoing, ST, split_axis=0, concat_axis=0, tiled=True)
    late_got, _ = lax.optimization_barrier((got, outgoing))
    grad_queries, outgoing = key_slots(owner_turned, queries, grad_in, late_got)
    turned = turned_normed(store, gain)
    outgoing, turned = lax.optimization_barrier((outgoing, turned))
    back_keys = lax.all_to_all(outgoing, ST, split_axis=0, concat_axis=0, tiled=True)
    back_values, turned, *near_weights = lax.optimization_barrier(
        (back_values, turned, *weights[1:])
    )
    weights[1:] = near_weights

    own, first, second, third, mine, other = value_sums(
        asked, place, back_values, turned, passages, st_size
    )
    parts = [own, shifted(first, 1), shifted(third, 3), shifted(second, 2)]
    near = near_products(parts, weights)
    came = lax.ppermute(other, "st_2", [(0, 1), (1, 0)])
    terms = mine.astype(jnp.float32) + came.astype(jnp.float32)
    terms = terms.reshape((4, terms.shape[0] // 4) + terms.shape[1:])
    near_terms = [terms[0]]
    for distance in (2, 1, 3):
        pairs = [(i, i ^ distance) for i in range(4)]
        came = lax.ppermute(terms[distance].astype(jnp.bfloat16), "st_1", pairs)
        near_terms.append(came.astype(jnp.float32))
    terms = sum(near_terms)
    back_keys, near = lax.optimization_barrier((back_keys, near))
    spread = [terms[0]]
    for distance in range(1, terms.shape[0]):
        pairs = [(i, i ^ distance) for i in range(terms.shape[0])]
        spread.append(lax.ppermute(terms[distance], "st_0", pairs))

    own, first, second, third = key_sums(asked, place, back_keys, passages)
    parts = []
    for part, turn in ((first, 1), (third, 3), (second, 2)):
        parts.append(shifted(part, turn))
    near, own_rows, *key_weights = own_product(place, own, near, weights, store)
    grad_w_value = sum(spread)
    grad_store = store_gradient(own_rows, gain, near, parts, key_weights)
    return (grad_queries, grad_store, grad_w_value)


def solution(mesh):
    torus = Mesh(mesh.devices.reshape(8, 4, 2, mesh.shape["tp"]), ("st_0", "st_1", "st_2", "tp"))
    return jax.shard_map(
        local,
        mesh=torus,
        in_specs=(
            P(ST, "tp"),
            P(ST, "tp"),
            P(ST, "tp"),
            P(ST, None),
            P(),
            P(None, "tp"),
            P(None, "tp"),
            P(ST, None),
            P(ST, None),
        ),
        out_specs=(P(ST, "tp"), P(ST_TP, None), P(ST, "tp")),
        check_vma=False,
    )
```

```python
import jax
import jax.numpy as jnp
from jax import lax
from jax.experimental import pallas as pl
from jax.experimental.pallas import tpu as pltpu
from jax.sharding import Mesh
from jax.sharding import PartitionSpec as P


HD = 128
PLEN = 64
EPS = 1e-06
ST = ("st_0", "st_1", "st_2")
ST_TP = ("st_0", "st_1", "st_2", "tp")
MIB = 1024 * 1024


def params(mib):
    return pltpu.CompilerParams(
        dimension_semantics=("arbitrary",), vmem_limit_bytes=mib * MIB
    )


def in_hbm(value):
    return pltpu.with_memory_space_constraint(value, pltpu.HBM)


def dot_nn(a, b):
    return lax.dot_general(a, b, (((1,), (0,)), ((), ())), preferred_element_type=jnp.float32)


def dot_nt(a, b):
    return lax.dot_general(a, b, (((1,), (1,)), ((), ())), preferred_element_type=jnp.float32)


def dot_tn(a, b):
    return lax.dot_general(a, b, (((0,), (0,)), ((), ())), preferred_element_type=jnp.float32)


def normed_rows(x, gain):
    inverse = lax.rsqrt(jnp.mean(x * x, axis=-1, keepdims=True) + EPS)
    return (x * inverse * gain).astype(jnp.bfloat16)


def tables_kernel(store_ref, gain_ref, wk_hbm, wv_hbm, table_ref, both_hbm, wk_ref, wv_ref, sems):
    first = pl.program_id(0) == 0
    last = pl.program_id(0) == pl.num_programs(0) - 1
    width = wk_ref.shape[1]
    keys_out = pltpu.make_async_copy(wk_ref, both_hbm.at[:, :width], sems.at[2])
    values_out = pltpu.make_async_copy(wv_ref, both_hbm.at[:, width:], sems.at[3])
    keys_in = pltpu.make_async_copy(wk_hbm, wk_ref, sems.at[0])
    values_in = pltpu.make_async_copy(wv_hbm, wv_ref, sems.at[1])

    @pl.when(first)
    def _():
        keys_in.start()
        values_in.start()

    normed = normed_rows(store_ref[...].astype(jnp.float32), gain_ref[...])

    @pl.when(first)
    def _():
        keys_in.wait()
        values_in.wait()
        keys_out.start()
        values_out.start()

    table_ref[:, :width] = dot_nn(normed, wk_ref[...]).astype(jnp.bfloat16)
    table_ref[:, width:] = dot_nn(normed, wv_ref[...]).astype(jnp.bfloat16)

    @pl.when(last)
    def _():
        keys_out.wait()
        values_out.wait()


def key_value_tables(store, gain, w_key, w_value):
    rows, model = store.shape
    width = w_key.shape[1]
    step = 256
    return pl.pallas_call(
        tables_kernel,
        grid=(rows // step,),
        in_specs=[
            pl.BlockSpec((step, model), lambda i: (i, 0)),
            pl.BlockSpec((1, model), lambda i: (0, 0)),
            pl.BlockSpec(memory_space=pltpu.HBM),
            pl.BlockSpec(memory_space=pltpu.HBM),
        ],
        out_specs=[
            pl.BlockSpec((step, 2 * width), lambda i: (i, 0)),
            pl.BlockSpec(memory_space=pltpu.HBM),
        ],
        out_shape=[
            jax.ShapeDtypeStruct((rows, 2 * width), jnp.bfloat16),
            pltpu.HBM((model, 2 * width), jnp.bfloat16),
        ],
        scratch_shapes=[
            pltpu.VMEM((model, width), jnp.bfloat16),
            pltpu.VMEM((model, width), jnp.bfloat16),
            pltpu.SemaphoreType.DMA((4,)),
        ],
        compiler_params=params(16),
        cost_estimate=pl.CostEstimate(
            flops=4 * rows * model * width, bytes_accessed=2 * rows * model, transcendentals=rows
        ),
        name="tables",
    )(in_hbm(store), in_hbm(gain), in_hbm(w_key), in_hbm(w_value))


def turned_kernel(store_ref, gain_ref, out_ref):
    normed = normed_rows(store_ref[...].astype(jnp.float32), gain_ref[...])
    out_ref[...] = normed.T


def turned_normed(store, gain):
    rows, model = store.shape
    step = 256
    return pl.pallas_call(
        turned_kernel,
        grid=(rows // step,),
        in_specs=[
            pl.BlockSpec((step, model), lambda i: (i, 0)),
            pl.BlockSpec((1, model), lambda i: (0, 0)),
        ],
        out_specs=pl.BlockSpec((model, step), lambda i: (0, i)),
        out_shape=pltpu.HBM((model, rows), jnp.bfloat16),
        compiler_params=params(16),
        cost_estimate=pl.CostEstimate(
            flops=16 * rows * model, bytes_accessed=4 * rows * model, transcendentals=rows
        ),
        name="turned_normed",
    )(in_hbm(store), in_hbm(gain))


def gather_kernel(asked_ref, table_ref, out_hbm, sems):
    copies = []
    for i in range(out_hbm.shape[0]):
        asked = jnp.maximum(asked_ref[i], 0)
        copies.append(pltpu.make_async_copy(table_ref.at[asked], out_hbm.at[i], sems.at[i]))
        copies[-1].start()
    for copy in copies:
        copy.wait()


def picked_passages(asked, table):
    _, length, width = table.shape
    slots = asked.shape[0]
    return pl.pallas_call(
        gather_kernel,
        in_specs=[
            pl.BlockSpec(memory_space=pltpu.SMEM),
            pl.BlockSpec(memory_space=pltpu.VMEM),
        ],
        out_specs=pl.BlockSpec(memory_space=pltpu.HBM),
        out_shape=pltpu.HBM((slots, length, width), jnp.bfloat16),
        scratch_shapes=[pltpu.SemaphoreType.DMA((slots,))],
        compiler_params=pltpu.CompilerParams(vmem_limit_bytes=8 * MIB),
        name="picked",
    )(asked, table)


def gated_kernel(g_ref, c_ref, out_ref):
    gate = jax.nn.sigmoid(g_ref[...].astype(jnp.float32))
    out_ref[...] = (gate * c_ref[...].astype(jnp.float32)).astype(jnp.bfloat16)


def gated(gate_pre, cotangent):
    rows, width = gate_pre.shape
    step = pl.BlockSpec((rows // 4, width), lambda i: (i, 0))
    return pl.pallas_call(
        gated_kernel,
        grid=(4,),
        in_specs=[step, step],
        out_specs=step,
        out_shape=jax.ShapeDtypeStruct((rows, width), jnp.bfloat16),
        compiler_params=params(8),
        cost_estimate=pl.CostEstimate(
            flops=8 * rows * width, bytes_accessed=6 * rows * width, transcendentals=rows * width
        ),
        name="gated",
    )(in_hbm(gate_pre), in_hbm(cotangent))


def slot_copies(owner_ref, scratch, out_hbm, sems, at, parity):
    per_block = owner_ref.shape[0]
    each = scratch.shape[1] // per_block
    return [
        pltpu.make_async_copy(
            scratch.at[parity, b * per_block + j],
            out_hbm.at[owner_ref[j, at * each + b]],
            sems.at[parity, b * per_block + j],
        )
        for b in range(each)
        for j in range(per_block)
    ]


def wait_slots(owner_ref, scratch, out_hbm, sems):
    step = pl.program_id(0)

    @pl.when(step >= 2)
    def _():
        for copy in slot_copies(owner_ref, scratch, out_hbm, sems, step - 2, lax.rem(step, 2)):
            copy.wait()


def send_slots(owner_ref, scratch, out_hbm, sems):
    step, steps = pl.program_id(0), pl.num_programs(0)
    slot = lax.rem(step, 2)
    for copy in slot_copies(owner_ref, scratch, out_hbm, sems, step, slot):
        copy.start()

    @pl.when(step == steps - 1)
    def _():
        for copy in slot_copies(owner_ref, scratch, out_hbm, sems, step - 1, 1 - slot):
            copy.wait()
        for copy in slot_copies(owner_ref, scratch, out_hbm, sems, step, slot):
            copy.wait()


def softmax_turned(keys, q):
    scores = dot_nt(keys, q) * HD ** (-0.5)
    weights = jnp.exp(scores - jnp.max(scores, axis=0, keepdims=True))
    return weights * (1.0 / jnp.sum(weights, axis=0, keepdims=True))


def value_slots_kernel(owner_ref, q_ref, gin_ref, *refs):
    pieces, (out_hbm, scratch, sems) = refs[:-3], refs[-3:]
    step = pl.program_id(0)
    per_block = owner_ref.shape[0]
    width = q_ref.shape[1]
    each = len(pieces) // per_block
    length = q_ref.shape[0] // owner_ref.shape[1]
    slot = lax.rem(step, 2)
    units = []
    for b in range(each):
        rows = pl.ds(pl.multiple_of((step * each + b) * length, length), length)
        own = pieces[b * per_block : (b + 1) * per_block]
        for h in range(width // HD):
            cols = slice(h * HD, (h + 1) * HD)
            keys = jnp.concatenate([p[0, :, cols] for p in own], axis=0)
            units.append((b, cols, keys, q_ref[rows, cols], gin_ref[rows, cols]))
    scores = [dot_nt(u[2], u[3]) * HD ** (-0.5) for u in units]
    weights = [jnp.exp(x - jnp.max(x, axis=0, keepdims=True)) for x in scores]
    weights = [x * (1.0 / jnp.sum(x, axis=0, keepdims=True)) for x in weights]
    wait_slots(owner_ref, scratch, out_hbm, sems)
    for (b, cols, _, _, gin), weight in zip(units, weights):
        grad_values = dot_nn(weight.astype(jnp.bfloat16), gin).astype(jnp.bfloat16)
        for j in range(per_block):
            part = slice(j * PLEN, (j + 1) * PLEN)
            scratch[slot, b * per_block + j, :, cols] = grad_values[part]
    send_slots(owner_ref, scratch, out_hbm, sems)


def value_slots(owner_turned, queries, grad_in, got):
    rows, width = queries.shape
    per_block, blocks = owner_turned.shape
    slots, length, _ = got.shape
    each = 4

    def piece(b, j):
        return pl.BlockSpec((1, length, width), lambda i, o: (o[j, i * each + b], 0, 0))

    pieces = [piece(b, j) for b in range(each) for j in range(per_block)]
    keys = PLEN * per_block
    vmem = pl.BlockSpec(memory_space=pltpu.VMEM)
    return pl.pallas_call(
        value_slots_kernel,
        grid_spec=pltpu.PrefetchScalarGridSpec(
            num_scalar_prefetch=1,
            grid=(blocks // each,),
            in_specs=[vmem, vmem] + pieces,
            out_specs=pl.BlockSpec(memory_space=pltpu.HBM),
            scratch_shapes=[
                pltpu.VMEM((2, len(pieces), length, width), jnp.bfloat16),
                pltpu.SemaphoreType.DMA((2, len(pieces))),
            ],
        ),
        out_shape=pltpu.HBM((slots, length, width), jnp.bfloat16),
        compiler_params=params(12),
        cost_estimate=pl.CostEstimate(
            flops=4 * rows * width * keys,
            bytes_accessed=4 * rows * width + 2 * got.size,
            transcendentals=rows * width * keys // HD,
        ),
        name="value_slots",
    )(owner_turned, queries, grad_in, *([in_hbm(got)] * len(pieces)))


def key_slots_kernel(owner_ref, q_ref, gin_ref, *refs):
    pieces, (gq_ref, out_hbm, scratch, sems) = refs[:-4], refs[-4:]
    per_block = owner_ref.shape[0]
    width = q_ref.shape[1]
    each = len(pieces) // per_block
    length = q_ref.shape[0] // each
    slot = lax.rem(pl.program_id(0), 2)
    units = []
    for b in range(each):
        for h in range(width // HD):
            rows = slice(b * length, (b + 1) * length)
            cols = slice(h * HD, (h + 1) * HD)
            vcols = slice(width + h * HD, width + (h + 1) * HD)
            own = pieces[b * per_block : (b + 1) * per_block]
            keys = jnp.concatenate([p[0, :, cols] for p in own], axis=0)
            values = jnp.concatenate([p[0, :, vcols] for p in own], axis=0)
            q = q_ref[rows, cols]
            weights = softmax_turned(keys, q)
            grad_weights = dot_nt(values, gin_ref[rows, cols])
            kept = weights.astype(jnp.bfloat16).astype(jnp.float32)
            delta = jnp.sum(kept * grad_weights, axis=0, keepdims=True)
            half = (weights * (grad_weights - delta)).astype(jnp.bfloat16)
            units.append((b, rows, cols, q, keys, half))
    wait_slots(owner_ref, scratch, out_hbm, sems)
    for b, rows, cols, q, keys, half in units:
        gq_ref[rows, cols] = dot_tn(half, keys) * HD ** (-0.5)
        grad_keys = (dot_nn(half, q) * HD ** (-0.5)).astype(jnp.bfloat16)
        for j in range(per_block):
            part = slice(j * PLEN, (j + 1) * PLEN)
            scratch[slot, b * per_block + j, :, cols] = grad_keys[part]
    send_slots(owner_ref, scratch, out_hbm, sems)


def key_slots(owner_turned, queries, grad_in, got):
    rows, width = queries.shape
    per_block, blocks = owner_turned.shape
    slots, length, both = got.shape
    each = 2
    steps = blocks // each
    tokens = pl.BlockSpec((rows // steps, width), lambda i, o: (i, 0))

    def piece(b, j):
        return pl.BlockSpec((1, length, both), lambda i, o: (o[j, i * each + b], 0, 0))

    pieces = [piece(b, j) for b in range(each) for j in range(per_block)]
    keys = PLEN * per_block
    return pl.pallas_call(
        key_slots_kernel,
        grid_spec=pltpu.PrefetchScalarGridSpec(
            num_scalar_prefetch=1,
            grid=(steps,),
            in_specs=[tokens, tokens] + pieces,
            out_specs=[tokens, pl.BlockSpec(memory_space=pltpu.HBM)],
            scratch_shapes=[
                pltpu.VMEM((2, len(pieces), length, width), jnp.bfloat16),
                pltpu.SemaphoreType.DMA((2, len(pieces))),
            ],
        ),
        out_shape=[
            jax.ShapeDtypeStruct((rows, width), jnp.float32),
            pltpu.HBM((slots, length, width), jnp.bfloat16),
        ],
        compiler_params=params(20),
        cost_estimate=pl.CostEstimate(
            flops=8 * rows * width * keys,
            bytes_accessed=10 * rows * width + 2 * got.size,
            transcendentals=rows * width * keys // HD,
        ),
        name="key_slots",
    )(owner_turned, queries, grad_in, *([in_hbm(got)] * len(pieces)))


def add_asked(asked_ref, back_ref, total):
    step = pl.program_id(0)
    each = back_ref.shape[0]

    @pl.when(step == 0)
    def _():
        total[...] = jnp.zeros_like(total)

    for i in range(each):
        asked = asked_ref[step * each + i]

        @pl.when(asked >= 0)
        def _():
            total[asked] += back_ref[i].astype(jnp.float32)


def write_quarters(place_ref, total, parts):
    passages, length, _ = total.shape
    share = passages // 4
    for turn, out in enumerate(parts):
        first = lax.rem(place_ref[0] + turn, 4) * share
        for p in range(share):
            out[p * length : (p + 1) * length, :] = total[first + p].astype(jnp.bfloat16)


def value_kernel(asked_ref, place_ref, back_ref, turned_hbm, *refs):
    parts, (mine_ref, other_ref, total, terms, turned_ref, sem) = refs[:4], refs[4:]
    turned_in = pltpu.make_async_copy(turned_hbm, turned_ref, sem)

    @pl.when(pl.program_id(0) == 0)
    def _():
        turned_in.start()

    add_asked(asked_ref, back_ref, total)

    @pl.when(pl.program_id(0) == pl.num_programs(0) - 1)
    def _():
        write_quarters(place_ref, total, parts)
        passages, length, width = total.shape
        values = total[...].astype(jnp.bfloat16).reshape(passages * length, width)
        pieces, piece, _ = terms.shape
        turned_in.wait()
        made = dot_nn(turned_ref[...], values).astype(jnp.bfloat16)
        for p in range(pieces):
            terms[p] = made[p * piece : (p + 1) * piece]
        for p in range(pieces // 2):
            turn = p % 8 * 8 + p // 8 * 2
            mine_ref[p] = terms[place_ref[1] ^ turn]
            other_ref[p] = terms[place_ref[1] ^ (turn + 1)]


def value_sums(asked, place, back, turned, passages, devices):
    slots, length, width = back.shape
    model, rows = turned.shape
    each = 16
    quarter = jax.ShapeDtypeStruct((rows // 4, width), jnp.bfloat16)
    half = jax.ShapeDtypeStruct((devices // 2, model // devices, width), jnp.bfloat16)
    return pl.pallas_call(
        value_kernel,
        grid_spec=pltpu.PrefetchScalarGridSpec(
            num_scalar_prefetch=2,
            grid=(slots // each,),
            in_specs=[
                pl.BlockSpec((each, length, width), lambda i, a, t: (i, 0, 0)),
                pl.BlockSpec(memory_space=pltpu.HBM),
            ],
            out_specs=[pl.BlockSpec(quarter.shape, lambda i, a, t: (0, 0))] * 4
            + [pl.BlockSpec(half.shape, lambda i, a, t: (0, 0, 0))] * 2,
            scratch_shapes=[
                pltpu.VMEM((passages, length, width), jnp.float32),
                pltpu.VMEM((devices, model // devices, width), jnp.bfloat16),
                pltpu.VMEM((model, rows), jnp.bfloat16),
                pltpu.SemaphoreType.DMA,
            ],
        ),
        out_shape=[quarter] * 4 + [half] * 2,
        compiler_params=params(24),
        cost_estimate=pl.CostEstimate(
            flops=2 * model * rows * width, bytes_accessed=2 * model * rows, transcendentals=0
        ),
        name="value_sums",
    )(asked, place, back, in_hbm(turned))


def key_kernel(asked_ref, place_ref, back_ref, *refs):
    parts, total = refs[:4], refs[4]
    total[...] = jnp.zeros_like(total)
    for r in range(back_ref.shape[0]):
        asked = asked_ref[r]

        @pl.when(asked >= 0)
        def _():
            total[asked] += back_ref[r].astype(jnp.float32)

    write_quarters(place_ref, total, parts)


def key_sums(asked, place, back, passages):
    _, length, width = back.shape
    quarter = jax.ShapeDtypeStruct((passages * length // 4, width), jnp.bfloat16)
    smem = pl.BlockSpec(memory_space=pltpu.SMEM)
    vmem = pl.BlockSpec(memory_space=pltpu.VMEM)
    return pl.pallas_call(
        key_kernel,
        in_specs=[smem, smem, vmem],
        out_specs=[vmem] * 4,
        out_shape=[quarter] * 4,
        scratch_shapes=[pltpu.VMEM((passages, length, width), jnp.float32)],
        compiler_params=pltpu.CompilerParams(vmem_limit_bytes=12 * MIB),
        cost_estimate=pl.CostEstimate(
            flops=4 * back.size, bytes_accessed=2 * back.size, transcendentals=0
        ),
        name="key_sums",
    )(asked, place, back)


def near_kernel(*refs):
    count = 4
    parts, weights, out_ref = refs[:count], refs[count : 2 * count], refs[2 * count]
    held, sems = refs[2 * count + 1 : -1], refs[-1]
    width = parts[0].shape[1]
    arrivals = [
        pltpu.make_async_copy(w.at[:, width:], h, sems.at[i])
        for i, (w, h) in enumerate(zip(weights, held))
    ]
    for copy in arrivals:
        copy.start()
    made = []
    for part, arrival, h in zip(parts, arrivals, held):
        arrival.wait()
        made.append(dot_nt(part[...], h[...]))
    out_ref[...] = sum(made)


def near_products(parts, weights):
    quarter, width = parts[0].shape
    model = weights[0].shape[0]
    count = len(parts)
    vmem = pl.BlockSpec(memory_space=pltpu.VMEM)
    hbm = pl.BlockSpec(memory_space=pltpu.HBM)
    return pl.pallas_call(
        near_kernel,
        in_specs=[vmem] * count + [hbm] * count,
        out_specs=vmem,
        out_shape=jax.ShapeDtypeStruct((quarter, model), jnp.float32),
        scratch_shapes=[pltpu.VMEM((model, width), jnp.bfloat16)] * count
        + [pltpu.SemaphoreType.DMA((count,))],
        compiler_params=pltpu.CompilerParams(vmem_limit_bytes=16 * MIB),
        cost_estimate=pl.CostEstimate(
            flops=2 * count * quarter * model * width,
            bytes_accessed=2 * count * model * width,
            transcendentals=0,
        ),
        name="near_products",
    )(*parts, *[in_hbm(w) for w in weights])


def own_kernel(place_ref, part_ref, near_ref, *refs):
    count = 4
    weights, store_hbm = refs[:count], refs[count]
    out_ref, rows_ref, *keys_refs = refs[count + 1 : 2 * count + 2]
    held, sems = refs[2 * count + 2], refs[-1]
    quarter, width = part_ref.shape
    first = pl.multiple_of(place_ref[0] * quarter, quarter)
    copies = [
        pltpu.make_async_copy(w.at[:, :width], k, sems.at[i])
        for i, (w, k) in enumerate(zip(weights, [held] + keys_refs))
    ]
    copies.append(
        pltpu.make_async_copy(store_hbm.at[pl.ds(first, quarter)], rows_ref, sems.at[count])
    )
    for copy in copies:
        copy.start()
    copies[0].wait()
    out_ref[...] = near_ref[...] + dot_nt(part_ref[...], held[...])
    for copy in copies[1:]:
        copy.wait()


def own_product(place, part, near, weights, store):
    quarter, width = part.shape
    model = weights[0].shape[0]
    count = len(weights)
    vmem = pl.BlockSpec(memory_space=pltpu.VMEM)
    hbm = pl.BlockSpec(memory_space=pltpu.HBM)
    return pl.pallas_call(
        own_kernel,
        in_specs=[pl.BlockSpec(memory_space=pltpu.SMEM), vmem, vmem] + [hbm] * (count + 1),
        out_specs=[vmem] * (count + 1),
        out_shape=[
            pltpu.VMEM((quarter, model), jnp.float32),
            pltpu.VMEM((quarter, model), jnp.bfloat16),
        ]
        + [pltpu.VMEM((model, width), jnp.bfloat16)] * (count - 1),
        scratch_shapes=[
            pltpu.VMEM((model, width), jnp.bfloat16),
            pltpu.SemaphoreType.DMA((count + 1,)),
        ],
        compiler_params=pltpu.CompilerParams(vmem_limit_bytes=16 * MIB),
        cost_estimate=pl.CostEstimate(
            flops=2 * quarter * model * width,
            bytes_accessed=4 * count * model * width,
            transcendentals=0,
        ),
        name="own_product",
    )(place, part, near, *[in_hbm(w) for w in weights], in_hbm(store))


def final_kernel(rows_ref, gain_ref, near_ref, *refs):
    parts, weights, (out_hbm, out_ref, sems) = refs[:3], refs[3:6], refs[6:]
    made = near_ref[...]
    for part, weight in zip(parts, weights):
        made += dot_nt(part[...], weight[...])
    step = 64
    sent = []
    for i in range(out_ref.shape[0] // step):
        at = slice(i * step, (i + 1) * step)
        rows = rows_ref[at].astype(jnp.float32)
        inverse = lax.rsqrt(jnp.mean(rows * rows, axis=-1, keepdims=True) + EPS)
        unit = rows * inverse
        grad_unit = made[at] * gain_ref[...]
        mean = jnp.mean(grad_unit * unit, axis=-1, keepdims=True)
        out_ref[at] = inverse * (grad_unit - unit * mean)
        sent.append(pltpu.make_async_copy(out_ref.at[at], out_hbm.at[at], sems.at[i]))
        sent[-1].start()
    for copy in sent:
        copy.wait()


def store_gradient(rows, gain, near, parts, weights):
    quarter, model = rows.shape
    width = parts[0].shape[1]
    vmem = pl.BlockSpec(memory_space=pltpu.VMEM)
    return pl.pallas_call(
        final_kernel,
        in_specs=[vmem] * (3 + 2 * len(parts)),
        out_specs=pl.BlockSpec(memory_space=pltpu.HBM),
        out_shape=jax.ShapeDtypeStruct((quarter, model), jnp.float32),
        scratch_shapes=[
            pltpu.VMEM((quarter, model), jnp.float32),
            pltpu.SemaphoreType.DMA((quarter // 64,)),
        ],
        compiler_params=pltpu.CompilerParams(vmem_limit_bytes=16 * MIB),
        cost_estimate=pl.CostEstimate(
            flops=6 * quarter * model * width,
            bytes_accessed=4 * quarter * model,
            transcendentals=quarter,
        ),
        name="store_gradient",
    )(rows, gain, near, *parts, *weights)


def shifted(value, turn):
    return lax.ppermute(value, "tp", [(i, (i + turn) % 4) for i in range(4)])


def local(queries, gate_pre, cotangent, store, store_gain, w_key, w_value, owners, slots):
    st_size = lax.axis_size(ST)
    width = queries.shape[1]
    rows_dev, model = store.shape
    passages = rows_dev // PLEN
    place = jnp.stack([lax.axis_index("tp"), lax.axis_index(ST)]).astype(jnp.int32)
    gain = store_gain.reshape(1, model)

    owner_turned = owners.T
    hits = owner_turned[None] == jnp.arange(st_size, dtype=jnp.int32)[:, None, None]
    requests = jnp.where(hits, slots.T[None], -1)
    asked = lax.all_to_all(requests, ST, split_axis=0, concat_axis=0, tiled=True)
    asked = jnp.max(asked, axis=(1, 2))

    table, both = key_value_tables(store, gain, w_key, w_value)
    picked = picked_passages(asked, table.reshape(passages, PLEN, 2 * width))
    got = lax.all_to_all(picked, ST, split_axis=0, concat_axis=0, tiled=True)

    both, _ = lax.optimization_barrier((both, picked))
    weights = [both]
    for turn in (1, 3, 2):
        weights.append(shifted(both, turn))

    grad_in = gated(gate_pre, cotangent)
    outgoing = value_slots(owner_turned, queries, grad_in, got)
    back_values = lax.all_to_all(outgoing, ST, split_axis=0, concat_axis=0, tiled=True)
    late_got, _ = lax.optimization_barrier((got, outgoing))
    grad_queries, outgoing = key_slots(owner_turned, queries, grad_in, late_got)
    turned = turned_normed(store, gain)
    outgoing, turned = lax.optimization_barrier((outgoing, turned))
    back_keys = lax.all_to_all(outgoing, ST, split_axis=0, concat_axis=0, tiled=True)
    back_values, turned, *near_weights = lax.optimization_barrier(
        (back_values, turned, *weights[1:])
    )
    weights[1:] = near_weights

    own, first, second, third, mine, other = value_sums(
        asked, place, back_values, turned, passages, st_size
    )
    parts = [own, shifted(first, 1), shifted(third, 3), shifted(second, 2)]
    near = near_products(parts, weights)
    came = lax.ppermute(other, "st_2", [(0, 1), (1, 0)])
    terms = mine.astype(jnp.float32) + came.astype(jnp.float32)
    terms = terms.reshape((4, terms.shape[0] // 4) + terms.shape[1:])
    near_terms = [terms[0]]
    for distance in (2, 1, 3):
        pairs = [(i, i ^ distance) for i in range(4)]
        came = lax.ppermute(terms[distance].astype(jnp.bfloat16), "st_1", pairs)
        near_terms.append(came.astype(jnp.float32))
    terms = sum(near_terms)
    back_keys, near = lax.optimization_barrier((back_keys, near))
    spread = [terms[0]]
    for distance in range(1, terms.shape[0]):
        pairs = [(i, i ^ distance) for i in range(terms.shape[0])]
        spread.append(lax.ppermute(terms[distance], "st_0", pairs))

    own, first, second, third = key_sums(asked, place, back_keys, passages)
    parts = []
    for part, turn in ((first, 1), (third, 3), (second, 2)):
        parts.append(shifted(part, turn))
    near, own_rows, *key_weights = own_product(place, own, near, weights, store)
    grad_w_value = sum(spread)
    grad_store = store_gradient(own_rows, gain, near, parts, key_weights)
    return (grad_queries, grad_store, grad_w_value)


def solution(mesh):
    torus = Mesh(mesh.devices.reshape(8, 4, 2, mesh.shape["tp"]), ("st_0", "st_1", "st_2", "tp"))
    return jax.shard_map(
        local,
        mesh=torus,
        in_specs=(
            P(ST, "tp"),
            P(ST, "tp"),
            P(ST, "tp"),
            P(ST, None),
            P(),
            P(None, "tp"),
            P(None, "tp"),
            P(ST, None),
            P(ST, None),
        ),
        out_specs=(P(ST, "tp"), P(ST_TP, None), P(ST, "tp")),
        check_vma=False,
    )
```
